128 devices in a mesh: ep: 32 (over z, y, core), tp: 4 (over x).
Axes of the slice: x: 4, y: 4, z: 4, core: 2. Of those that a mesh axis runs over, the one named last changes fastest.
Arguments:
- mix_input: bfloat16 [16384, 4096], P(('ep', 'tp')), may hold values from -30 to 30
- moe_input: bfloat16 [16384, 4096], P(('ep', 'tp')), may hold values from -6 to 6
- norm_mix: float32 [4096], replicated, may hold values from 0.1 to 1.9
- query_weight: bfloat16 [4096, 2048], P(None, 'tp'), may hold values from -0.09375 to 0.09375
- forget_weight: bfloat16 [4096, 2048], P(None, 'tp'), may hold values from -0.09375 to 0.09375
- value_weight: bfloat16 [4096, 2048], P(None, 'tp'), may hold values from -0.09375 to 0.09375
- forget_gap: float32 [2048], P('tp'), may hold values from 1e-05 to 0.06
- norm_out: float32 [2048], P('tp'), may hold values from 0.1 to 1.9
- norm_moe: float32 [4096], replicated, may hold values from 0.1 to 1.9
- router_weight: bfloat16 [4096, 32], replicated, may hold values from -0.09375 to 0.09375
- expert_gate: bfloat16 [32, 4096, 1024], P('ep', None, 'tp'), may hold values from -2 to 2, as said below
- expert_up: bfloat16 [32, 4096, 1024], P('ep', None, 'tp'), may hold values from -2 to 2, as said below
- expert_down: bfloat16 [32, 1024, 4096], P('ep', None, 'tp'), may hold values from -0.1875 to 0.1875
- routes: int32 [16384, 2], P('ep'), may hold values from 0 to 31, all different within a row; in each aligned block of 128 rows (0 to 127, 128 to 255, ...) at most 16 rows name the same one
Outputs:
- mixer_out: bfloat16 [16384, 2048], P('ep', 'tp')
- expert_out: bfloat16 [16384, 4096], P('ep', 'tp')
The draws below stay inside these ranges and needn't reach their ends.
Inputs may be any that keep to these rules, and one draw needn't show every extreme that they name: `routes`: each row names 2 different experts; in each aligned block of 128 rows no expert is named by more than 16 rows. `expert_gate`: independent entries, scaled by the fan-in 4096. `expert_up`: independent entries, scaled by the fan-in 4096.
All inputs are finite; a program needn't handle non-finite values.
Results may differ from the reference program's by a relative error of at most 0.012.
The reference program's roundings to bfloat16 on the way count: a program that leaves them out, or rounds other values in their place, can miss the bound.
Values may be sent and summed in bfloat16 or wider, within the bound.
No kernel may reach another device: no remote copies, remote signals or barrier semaphores. Data moves between devices by JAX's collectives and lax.ppermute only.
A program may use at most 192 MiB of HBM per device.

```python
import math
import jax
import jax.numpy as jnp
import numpy as np
from jax import lax

D = 4096
HEADS = 16
HEAD_DIM = 128
HW = 2048
FF = 1024
EXPERTS = 32
TOPK = 2
BLOCK = 64
TOK_DEV = 128
TOKENS = 16384
CAP = 16


def draw_mix_input(key, part):
    noise_key, level_key, direction_key, scale_key = jax.random.split(jax.random.fold_in(key, 11), 4)
    block_total = TOKENS // TOK_DEV
    noise = jax.random.truncated_normal(noise_key, -6.0, 6.0, (TOKENS, D), jnp.float32)
    scale = jnp.ones((TOKENS, 1), jnp.float32)
    levels = jax.random.uniform(level_key, (block_total, 1), jnp.float32, -2.0, 2.0)
    direction = jax.random.truncated_normal(direction_key, -4.0, 4.0, (1, D), jnp.float32)
    row_values = noise + jnp.repeat(levels, TOK_DEV, axis=0) * direction
    return (row_values * scale).astype(jnp.bfloat16)


def draw_forget_gap(key, part):
    pick_key, slow_key, fast_key = jax.random.split(jax.random.fold_in(key, 23), 3)
    ordering = jax.random.permutation(pick_key, HEADS)
    slow_count = HEADS // 2
    slow = (ordering < slow_count)[:, None]
    slow_gap = jnp.exp(jax.random.uniform(slow_key, (HEADS, HEAD_DIM), jnp.float32, math.log(1e-05), math.log(0.0001)))
    fast_gap = jnp.exp(jax.random.uniform(fast_key, (HEADS, HEAD_DIM), jnp.float32, math.log(0.02), math.log(0.06)))
    return jnp.where(slow, slow_gap, fast_gap).reshape(HEADS * HEAD_DIM).astype(jnp.float32)


def expert_matrix(key):
    spread = 1.0
    entries = jax.random.truncated_normal(key, -6.0, 6.0, (EXPERTS, D, FF), jnp.float32)
    return (entries * (spread / math.sqrt(D))).astype(jnp.bfloat16)


def draw_expert_gate(key, part):
    return expert_matrix(jax.random.fold_in(key, 31))


def draw_expert_up(key, part):
    return expert_matrix(jax.random.fold_in(key, 37))


def block_scale(stream_key, shape, pieces, smallest, largest):
    loudness = 1.0
    for dim, shards_of in pieces:
        draws = jax.random.uniform(jax.random.fold_in(jax.random.fold_in(stream_key, 6), dim), (shards_of,), jnp.float32, smallest / len(pieces), largest / len(pieces))
        loudness = loudness * jnp.repeat(jnp.exp(draws), shape[dim] // shards_of).reshape((-1,) + (1,) * (len(shape) - 1 - dim))
    return loudness


def shared_out(stream_key, own, number, rows, amount, top, limit, slope):
    sequence = jax.random.permutation(stream_key, amount)
    crowded, ordinary = shares(amount, rows * top, limit, slope, True), shares(amount, rows * top, limit, slope, False)
    places = jnp.arange(amount)

    def named(lengths, offset_by):
        used = int((lengths > 0).sum())
        fixed = max(1, used // 4)
        moved = fixed + (places - fixed + offset_by * (used - fixed)) % max(1, amount - fixed)
        return jnp.zeros((amount,), jnp.int32).at[sequence[jnp.where(places < fixed, places, moved)]].set(jnp.asarray(lengths, jnp.int32))

    lengths = jnp.where(number % 4 == 0, named(crowded, number // 4), named(ordinary, number - number // 4 - 1))
    mixed = jax.random.permutation(jax.random.fold_in(own, 3), amount)
    giver, taker = mixed[0:amount // 2 * 2:2], mixed[1:amount // 2 * 2:2]
    room = jnp.minimum(lengths[giver] - 1, limit - lengths[taker]) // 2
    room = jnp.where((giver == sequence[0]) | (taker == sequence[0]) | (lengths[taker] == 0), 0, jnp.maximum(room, 0))
    moved = jax.random.randint(jax.random.fold_in(own, 4), (amount // 2,), 0, 1 << 20) % (room + 1)
    lengths = lengths.at[giver].add(-moved).at[taker].add(moved)
    items = jnp.searchsorted(jnp.cumsum(lengths), jnp.arange(rows * top), side="right").astype(jnp.int32)
    table = items.reshape(top, rows).T
    table = table[jax.random.permutation(jax.random.fold_in(own, 1), rows)]
    offset_by = jax.random.randint(jax.random.fold_in(own, 2), (rows, 1), 0, top)
    return jnp.take_along_axis(table, (jnp.arange(top)[None, :] + offset_by) % top, axis=1)


def shares(count, total, most, lean, full):
    weights = [(1 << 20) // math.isqrt(grade ** lean) + 1 for grade in range(1, count + 1)]
    largest = most if full else min(most, max(-(-total // count), total * weights[0] // sum(weights)))
    least = 1 if total - largest >= count - 1 else 0
    holding, surplus = [largest] + [least] * (count - 1), total - largest - least * (count - 1)
    while surplus > 0:
        free = [i for i in range(1, count) if holding[i] < largest] or [i for i in range(1, count) if holding[i] < most]
        whole, budget = sum([weights[i] for i in free]), surplus
        for i in free:
            addition = min(most - holding[i], max(1, budget * weights[i] // whole), surplus)
            holding[i] = holding[i] + addition
            surplus = surplus - addition
    return np.array(holding)


def bell_draw(key, dims, scale, reach, cuts=(), held_as=jnp.bfloat16):
    array = scale * jax.random.normal(key, dims, jnp.float32)
    if cuts:
        array = array * block_scale(key, dims, cuts, -0.22, 0.18)
    return jnp.clip(array, -reach, reach).astype(held_as)


def setup_inputs(seed: int = 0) -> dict:
    key_list = jax.random.split(jax.random.key(seed), 15)
    mix_input = draw_mix_input(jax.random.fold_in(key_list[14], 71), 0)
    moe_input = bell_draw(key_list[1], (TOKENS, D), 1.0, 6.0, ((0, 128),))
    norm_mix = jnp.clip(1.0 + 0.18 * jax.random.normal(key_list[2], (D,), jnp.float32), 0.1, 1.9)
    query_weight = bell_draw(key_list[3], (D, HW), D ** -0.5, 0.09375, ((1, 4),))
    forget_weight = bell_draw(key_list[4], (D, HW), D ** -0.5, 0.09375, ((1, 4),))
    value_weight = bell_draw(key_list[5], (D, HW), D ** -0.5, 0.09375, ((1, 4),))
    forget_gap = draw_forget_gap(jax.random.fold_in(key_list[14], 71), 0)
    norm_out = jnp.clip(1.0 + 0.18 * jax.random.normal(key_list[7], (HW,), jnp.float32), 0.1, 1.9)
    norm_moe = jnp.clip(1.0 + 0.18 * jax.random.normal(key_list[8], (D,), jnp.float32), 0.1, 1.9)
    router_weight = bell_draw(key_list[9], (D, EXPERTS), D ** -0.5, 0.09375)
    expert_gate = draw_expert_gate(jax.random.fold_in(key_list[14], 71), 0)
    expert_up = draw_expert_up(jax.random.fold_in(key_list[14], 71), 0)
    expert_down = bell_draw(key_list[12], (EXPERTS, FF, D), FF ** -0.5, 0.1875, ((0, 32), (2, 4)))
    routes_keys = jax.random.split(jax.random.fold_in(key_list[13], 1), TOKENS // TOK_DEV)
    routes_turns = jax.random.permutation(jax.random.fold_in(key_list[13], 3), TOKENS // TOK_DEV)
    routes = jax.vmap(lambda own, number: shared_out(jax.random.fold_in(key_list[13], 2), own, number, TOK_DEV, EXPERTS, TOPK, CAP, 1))(routes_keys, routes_turns).reshape((TOKENS, TOPK))
    return dict(mix_input=mix_input, moe_input=moe_input, norm_mix=norm_mix, query_weight=query_weight, forget_weight=forget_weight, value_weight=value_weight, forget_gap=forget_gap, norm_out=norm_out, norm_moe=norm_moe, router_weight=router_weight, expert_gate=expert_gate, expert_up=expert_up, expert_down=expert_down, routes=routes)


EPSILON = 1e-06
CLAMP_LIMIT = 7.0
SWISH_SLOPE = 1.702
MAXIMAL_ACCURACY = lax.Precision.HIGHEST

def normed(row_data, gain_vec):
    as_float = row_data.astype(jnp.float32)
    scale = lax.rsqrt(lax.optimization_barrier(jnp.mean(as_float * as_float, axis=-1, keepdims=True)) + EPSILON)
    return as_float * scale * gain_vec

def head_blocks(matrix, head_count):
    row_count = matrix.shape[0]
    return matrix.reshape(row_count // BLOCK, BLOCK, head_count, HEAD_DIM).transpose(0, 2, 1, 3)

def block_pass(running_state, inputs):
    query_rows, key_matrix_rows, value_rows, log_forget = inputs
    prefix_log_decay = jnp.cumsum(log_forget, axis=1)
    places = jnp.arange(BLOCK, dtype=jnp.int32)
    causal = (places[:, None] >= places[None, :])[None, :, :, None]
    spread = prefix_log_decay[:, :, None, :] - prefix_log_decay[:, None, :, :]
    decays = jnp.exp(jnp.where(causal, spread, -jnp.inf))
    scores = jnp.einsum('htk,hsk,htsk->hts', query_rows, key_matrix_rows, decays, precision=MAXIMAL_ACCURACY)
    inside = jnp.einsum('hts,hsv->htv', scores, value_rows, precision=MAXIMAL_ACCURACY)
    carried_state_block = jnp.einsum('faq,fqp->fap', query_rows * jnp.exp(prefix_log_decay), running_state, precision=MAXIMAL_ACCURACY)
    final_log_sum = prefix_log_decay[:, -1:, :]
    state_update = jnp.einsum('fge,fga->fea', key_matrix_rows * jnp.exp(final_log_sum - prefix_log_decay), value_rows, precision=MAXIMAL_ACCURACY)
    running_state = jnp.exp(final_log_sum[:, 0, :, None]) * running_state + state_update
    return (running_state, (inside + carried_state_block, prefix_log_decay))

def head_readout(block_out, gain_vec, head_count):
    block_total = block_out.shape[0]
    row_values = block_out.transpose(0, 2, 1, 3).reshape(block_total * BLOCK, head_count, HEAD_DIM)
    scale = lax.rsqrt(lax.optimization_barrier(jnp.mean(row_values * row_values, axis=-1, keepdims=True)) + EPSILON)
    shaped = row_values * scale * gain_vec.reshape(head_count, HEAD_DIM)
    return shaped.reshape(block_total * BLOCK, head_count * HEAD_DIM).astype(jnp.bfloat16)

def slot_places(routes, block_rows, expert_count, capacity):
    row_count = routes.shape[0]
    picks = routes.shape[1]
    flat_ids = routes.reshape(-1)
    onehot = (flat_ids[:, None] == jnp.arange(expert_count, dtype=jnp.int32)[None, :]).astype(jnp.int32)
    per_block = onehot.reshape(row_count // block_rows, block_rows * picks, expert_count)
    before = jnp.cumsum(per_block, axis=1) - per_block
    slot_rank = lax.optimization_barrier(jnp.sum(before * per_block, axis=2)).reshape(-1)
    anchor = jnp.arange(row_count * picks, dtype=jnp.int32) // (block_rows * picks)
    return (flat_ids * (row_count // block_rows) + anchor) * capacity + slot_rank

def route_weights(logits, routes):
    expert_count = logits.shape[1]
    chosen = routes[:, :, None] == jnp.arange(expert_count, dtype=jnp.int32)[None, None, :]
    picked = lax.optimization_barrier(jnp.sum(jnp.where(chosen, logits.astype(jnp.float32)[:, None, :], 0.0), axis=2))
    differences = picked[:, None, :] - picked[:, :, None]
    return 1.0 / lax.optimization_barrier(jnp.sum(jnp.exp(differences), axis=2))

def expert_rows(row_data, gate_mat, up_mat, down_mat):
    gate_pre = jnp.dot(row_data, gate_mat, preferred_element_type=jnp.float32)
    up_pre = jnp.dot(row_data, up_mat, preferred_element_type=jnp.float32)
    gated = jnp.minimum(gate_pre, CLAMP_LIMIT)
    opened = jnp.clip(up_pre, -CLAMP_LIMIT, CLAMP_LIMIT)
    hidden = ((opened + 1.0) * gated * jax.nn.sigmoid(SWISH_SLOPE * gated)).astype(jnp.bfloat16)
    return jnp.dot(hidden, down_mat, preferred_element_type=jnp.float32).astype(jnp.bfloat16)

def reference(mix_input, moe_input, norm_mix, query_weight, forget_weight, value_weight, forget_gap, norm_out, norm_moe, router_weight, expert_gate, expert_up, expert_down, routes):
    rows_a = normed(mix_input, norm_mix).astype(jnp.bfloat16)
    query_rows = jnp.dot(rows_a, query_weight, preferred_element_type=jnp.float32)
    forget_pre = jnp.dot(rows_a, forget_weight, preferred_element_type=jnp.float32)
    value_rows = jnp.dot(rows_a, value_weight, preferred_element_type=jnp.float32)
    shut = forget_gap * jax.nn.sigmoid(-forget_pre)
    log_forget = jnp.log1p(-shut)
    zero_state = jnp.zeros((HEADS, HEAD_DIM, HEAD_DIM), jnp.float32)
    end_state, (outputs, log_sums) = lax.scan(block_pass, zero_state, (head_blocks(query_rows, HEADS), head_blocks(shut, HEADS), head_blocks(value_rows, HEADS), head_blocks(log_forget, HEADS)))
    mixer_out = head_readout(outputs, norm_out, HEADS)
    rows_b = normed(moe_input, norm_moe).astype(jnp.bfloat16)
    logits = jnp.dot(rows_b, router_weight, preferred_element_type=jnp.float32).astype(jnp.bfloat16)
    weights = route_weights(logits, routes)
    block_total = TOKENS // TOK_DEV
    dest = slot_places(routes, TOK_DEV, EXPERTS, CAP)
    source = jnp.full((EXPERTS * block_total * CAP,), TOKENS, jnp.int32).at[dest].set(jnp.arange(TOKENS * TOPK, dtype=jnp.int32) // TOPK)
    padded = jnp.concatenate([rows_b, jnp.zeros((1, D), jnp.bfloat16)], axis=0)

    def one_expert(inputs):
        index_rows, gate_mat, up_mat, down_mat = inputs
        return expert_rows(padded[index_rows], gate_mat, up_mat, down_mat)
    results = lax.map(one_expert, (source.reshape(EXPERTS, block_total * CAP), expert_gate, expert_up, expert_down))
    flat_results = results.reshape(EXPERTS * block_total * CAP, D)
    dest_rows = dest.reshape(TOKENS, TOPK)
    total = jnp.zeros((TOKENS, D), jnp.float32)
    for slot_index in range(TOPK):
        total = total + weights[:, slot_index:slot_index + 1] * flat_results[dest_rows[:, slot_index]].astype(jnp.float32)
    expert_out = total.astype(jnp.bfloat16)
    return (mixer_out, expert_out)
```

```python
import jax
import jax.numpy as jnp
from jax import lax
from jax.experimental import pallas as pl
from jax.experimental.pallas import tpu as pltpu
from jax.sharding import Mesh
from jax.sharding import PartitionSpec as P

HEAD_DIM = 128
CAP = 16
EP = ("ep_0", "ep_1", "ep_2")
EP_TP = ("ep_0", "ep_1", "ep_2", "tp")

EPSILON = 1e-06
CLAMP_LIMIT = 7.0
SWISH_SLOPE = 1.702
EXACT = lax.Precision.HIGHEST
F32 = jnp.float32
BF16 = jnp.bfloat16


def mm(a, b, contract=((1,), (0,)), precision=None):
    return lax.dot_general(
        a, b, (contract, ((), ())), precision=precision, preferred_element_type=F32
    )


def params(mib=56, axes=("arbitrary",)):
    return pltpu.CompilerParams(vmem_limit_bytes=mib << 20, dimension_semantics=axes)


def normed(row_data, gain_vec):
    as_float = row_data.astype(F32)
    scale = lax.rsqrt(jnp.mean(as_float * as_float, axis=-1, keepdims=True) + EPSILON)
    return as_float * scale * gain_vec


def chosen(routes, experts):
    toks = routes.shape[1]
    ids = lax.broadcasted_iota(jnp.int32, (experts, toks), 0)
    first = routes[0:1, :] == ids
    second = routes[1:2, :] == ids
    count = jnp.where(first | second, 1.0, 0.0)
    earlier = (
        lax.broadcasted_iota(jnp.int32, (toks, toks), 0)
        < lax.broadcasted_iota(jnp.int32, (toks, toks), 1)
    )
    before = mm(count.astype(BF16), jnp.where(earlier, 1.0, 0.0).astype(BF16))
    return first, second, count, before


def slot_matrix(weight, before, count):
    experts, toks = weight.shape
    place = lax.broadcasted_iota(jnp.int32, (experts, CAP, toks), 1).astype(F32)
    here = (before[:, None, :] == place) & (count[:, None, :] > 0.5)
    return jnp.where(here, weight[:, None, :], 0.0).reshape(experts * CAP, toks)


def front_kernel(which, x_ref, gain_ref, router_ref, routes_ref, rows_ref, logits_ref, buf_ref, *, group):
    step = pl.program_id(0)

    @pl.when(step == 0)
    def _():
        rows_ref[...] = normed(x_ref[...], gain_ref[...]).astype(BF16)
        logits_ref[...] = mm(rows_ref[...], router_ref[...]).astype(BF16)

    fill(step, routes_ref, rows_ref, buf_ref, group)


def fill(step, routes_ref, rows_ref, buf_ref, group):
    experts = buf_ref.shape[0]
    routes = routes_ref[0] - step * group
    _, _, count, before = chosen(routes, experts)
    pick = slot_matrix(count, before, count).astype(BF16)
    buf_ref[...] = mm(pick, rows_ref[...]).astype(BF16).reshape(buf_ref.shape)


def fill_kernel(which, rows_ref, routes_ref, buf_ref, *, group):
    fill(pl.program_id(0), routes_ref, rows_ref, buf_ref, group)


def front(which, x, gain, router, routes, experts):
    toks, width = x.shape
    group = 8
    whole = lambda i, w: (0, 0)
    import functools

    return pl.pallas_call(
        functools.partial(front_kernel, group=group),
        grid_spec=pltpu.PrefetchScalarGridSpec(
            num_scalar_prefetch=1,
            grid=(experts // group,),
            in_specs=[
                pl.BlockSpec((toks, width), whole),
                pl.BlockSpec((1, width), whole),
                pl.BlockSpec(router.shape, whole),
                pl.BlockSpec((1, 2, toks), lambda i, w: (w[0], 0, 0)),
            ],
            out_specs=[
                pl.BlockSpec((toks, width), whole),
                pl.BlockSpec((toks, experts), whole),
                pl.BlockSpec((group, CAP, width), lambda i, w: (i, 0, 0)),
            ],
        ),
        out_shape=[
            jax.ShapeDtypeStruct((toks, width), BF16),
            jax.ShapeDtypeStruct((toks, experts), BF16),
            jax.ShapeDtypeStruct((experts, CAP, width), BF16),
        ],
        compiler_params=params(),
        name="front",
    )(which, x, gain, router, routes)


def refill(which, rows, routes, experts):
    toks, width = rows.shape
    group = 8
    import functools

    return pl.pallas_call(
        functools.partial(fill_kernel, group=group),
        grid_spec=pltpu.PrefetchScalarGridSpec(
            num_scalar_prefetch=1,
            grid=(experts // group,),
            in_specs=[
                pl.BlockSpec((toks, width), lambda i, w: (0, 0)),
                pl.BlockSpec((1, 2, toks), lambda i, w: (w[0], 0, 0)),
            ],
            out_specs=pl.BlockSpec((group, CAP, width), lambda i, w: (i, 0, 0)),
        ),
        out_shape=jax.ShapeDtypeStruct((experts, CAP, width), BF16),
        compiler_params=params(),
        name="refill",
    )(which, rows, routes)


def mixer_kernel(a_ref, q_ref, f_ref, v_ref, gap_ref, inside_ref, query_ref, packed_ref, qa, fa, va):
    step = pl.program_id(0)

    @pl.when(step == 0)
    def _():
        qa[...] = jnp.zeros_like(qa)
        fa[...] = jnp.zeros_like(fa)
        va[...] = jnp.zeros_like(va)

    a = a_ref[...]
    qa[...] += mm(a, q_ref[...])
    fa[...] += mm(a, f_ref[...])
    va[...] += mm(a, v_ref[...])

    @pl.when(step == pl.num_programs(0) - 1)
    def _():
        rows = a.shape[0]
        causal = (
            lax.broadcasted_iota(jnp.int32, (rows, rows), 0)
            >= lax.broadcasted_iota(jnp.int32, (rows, rows), 1)
        )
        ones = jnp.where(causal, 1.0, 0.0)
        heads = packed_ref.shape[0]
        for h in range(heads):
            at = slice(h * HEAD_DIM, (h + 1) * HEAD_DIM)
            shut = gap_ref[:, at] * jax.nn.sigmoid(-fa[:, at])
            sums = mm(ones, jnp.log1p(-shut), precision=EXACT)
            last = sums[rows - 1 :, :]
            value = va[:, at]
            query = qa[:, at] * jnp.exp(sums)
            scores = mm(query, shut * jnp.exp(-sums), ((1,), (1,)), EXACT)
            scores = jnp.where(causal, scores, 0.0)
            inside_ref[:, at] = mm(scores, value, precision=EXACT)
            query_ref[:, at] = query
            packed_ref[h, :HEAD_DIM, :] = mm(
                value, shut * jnp.exp(last - sums), ((0,), (0,)), EXACT
            )
            packed_ref[h, HEAD_DIM:, :] = jnp.broadcast_to(last, (8, HEAD_DIM))


def mixer(a, wq, wf, wv, gap):
    rows, width = a.shape
    cols = wq.shape[1]
    heads = cols // HEAD_DIM
    kb = 512
    fixed = lambda i: (0, 0)
    weight = pl.BlockSpec((kb, cols), lambda i: (i, 0))
    return pl.pallas_call(
        mixer_kernel,
        grid=(width // kb,),
        in_specs=[
            pl.BlockSpec((rows, kb), lambda i: (0, i)),
            weight,
            weight,
            weight,
            pl.BlockSpec((1, cols), fixed),
        ],
        out_specs=[
            pl.BlockSpec((rows, cols), fixed),
            pl.BlockSpec((rows, cols), fixed),
            pl.BlockSpec((heads, HEAD_DIM + 8, HEAD_DIM), lambda i: (0, 0, 0)),
        ],
        out_shape=[
            jax.ShapeDtypeStruct((rows, cols), F32),
            jax.ShapeDtypeStruct((rows, cols), F32),
            jax.ShapeDtypeStruct((heads, HEAD_DIM + 8, HEAD_DIM), F32),
        ],
        scratch_shapes=[pltpu.VMEM((rows, cols), F32)] * 3,
        compiler_params=params(),
        name="mixer",
    )(a, wq, wf, wv, gap)


def readout_kernel(inside_ref, query_ref, state_ref, gain_ref, out_ref):
    total = inside_ref[...] + mm(query_ref[...], state_ref[0], ((1,), (1,)), EXACT)
    out_ref[...] = normed(total, gain_ref[...]).astype(BF16)


def readout(inside, query, state, gain):
    rows, cols = inside.shape
    block = pl.BlockSpec((rows, HEAD_DIM), lambda h: (0, h))
    return pl.pallas_call(
        readout_kernel,
        grid=(cols // HEAD_DIM,),
        in_specs=[
            block,
            block,
            pl.BlockSpec((1, HEAD_DIM, HEAD_DIM), lambda h: (h, 0, 0)),
            pl.BlockSpec((1, HEAD_DIM), lambda h: (0, h)),
        ],
        out_specs=block,
        out_shape=jax.ShapeDtypeStruct((rows, cols), BF16),
        compiler_params=params(),
        name="readout",
    )(inside, query, state, gain)


def pieces(packed):
    return packed[:, HEAD_DIM : HEAD_DIM + 1, :], packed[:, :HEAD_DIM, :]


def link(earlier, later):
    return earlier[0] + later[0], jnp.exp(later[0]) * earlier[1] + later[1]


def pack(part):
    heads = part[1].shape[0]
    return jnp.concatenate(
        [part[1], jnp.broadcast_to(part[0], (heads, 8, HEAD_DIM))], axis=1
    )


def masked(flag, part):
    return jax.tree.map(lambda a: jnp.where(flag, a, 0.0), part)


def arriving_state(packed):
    core = lax.axis_index("ep_2")
    row = lax.axis_index("ep_1")
    other = lax.ppermute(packed, "ep_2", [(0, 1), (1, 0)])
    is_second = core == 1
    low = jnp.where(is_second, other, packed)
    high = jnp.where(is_second, packed, other)
    half = packed.shape[0] // 2
    mine = lambda a: lax.dynamic_slice_in_dim(a, core * half, half, 0)
    chip = link(pieces(mine(low)), pieces(mine(high)))
    count = lax.axis_size("ep_1")
    sent = pack(chip)
    before = after = None
    for d in range(count - 1, 0, -1):
        came = pieces(lax.ppermute(sent, "ep_1", [(i, (i + d) % count) for i in range(count)]))
        early = masked(row >= d, came)
        late = masked(row < d, came)
        before = early if before is None else link(before, early)
        after = late if after is None else link(after, late)
    plane = pack(link(link(before, chip), after))
    planes = None
    count = lax.axis_size("ep_0")
    for d in range(count - 1, 0, -1):
        came = pieces(lax.ppermute(plane, "ep_0", [(i, i + d) for i in range(count - d)]))
        planes = came if planes is None else link(planes, came)
    state = link(planes, before)[1]
    swapped = lax.ppermute(state, "ep_2", [(0, 1), (1, 0)])
    entering = jnp.concatenate(
        [jnp.where(is_second, swapped, state), jnp.where(is_second, state, swapped)], axis=0
    )
    first_core = pieces(low)
    return jnp.where(is_second, jnp.exp(first_core[0]) * entering + first_core[1], entering)


def hidden_kernel(rows_ref, go_ref, uo_ref, gr_ref, ur_ref, out_ref, gate, up):
    step = pl.program_id(0)

    @pl.when(step == 0)
    def _():
        gate[...] = jnp.zeros_like(gate)
        up[...] = jnp.zeros_like(up)

    rows = rows_ref[...]
    n = go_ref.shape[1]
    gate[:, :n] += mm(rows, go_ref[...])
    gate[:, n:] += mm(rows, gr_ref[...])
    up[:, :n] += mm(rows, uo_ref[...])
    up[:, n:] += mm(rows, ur_ref[...])

    @pl.when(step == pl.num_programs(0) - 1)
    def _():
        gated = jnp.minimum(gate[...], CLAMP_LIMIT)
        opened = jnp.clip(up[...], -CLAMP_LIMIT, CLAMP_LIMIT)
        out_ref[...] = (
            (opened + 1.0) * gated * jax.nn.sigmoid(SWISH_SLOPE * gated)
        ).astype(BF16)


def hidden_units(rows, go, uo, gr, ur):
    count, width = rows.shape
    n = go.shape[1]
    kb = 1024
    weight = pl.BlockSpec((kb, n), lambda i: (i, 0))
    return pl.pallas_call(
        hidden_kernel,
        grid=(width // kb,),
        in_specs=[pl.BlockSpec((count, kb), lambda i: (0, i)), weight, weight, weight, weight],
        out_specs=pl.BlockSpec((count, 2 * n), lambda i: (0, 0)),
        out_shape=jax.ShapeDtypeStruct((count, 2 * n), BF16),
        scratch_shapes=[pltpu.VMEM((count, 2 * n), F32)] * 2,
        compiler_params=params(),
        name="hidden",
    )(rows, go, uo, gr, ur)


def down_kernel(ho_ref, hp_ref, down_ref, out_ref):
    r = pl.program_id(0)
    n = down_ref.shape[0] // 4
    unit = lambda s: down_ref[pl.ds(pl.multiple_of(s * n, n), n), :]
    near = r + 1 - 2 * (r % 2)
    total = mm(ho_ref[0, :, :n], unit(r)) + mm(ho_ref[0, :, n:], unit(3 - r))
    total += mm(hp_ref[0, :, :n], unit(near)) + mm(hp_ref[0, :, n:], unit(3 - near))
    out_ref[...] = total.astype(BF16).reshape(out_ref.shape)


def down_rows(ho, hp, down):
    sources, rows, both = ho.shape
    cols = down.shape[1]
    near = lambda r: (r + 1 - 2 * (r % 2), 0, 0)
    return pl.pallas_call(
        down_kernel,
        grid=(sources,),
        in_specs=[
            pl.BlockSpec((1, rows, both), lambda r: (r, 0, 0)),
            pl.BlockSpec((1, rows, both), near),
            pl.BlockSpec(down.shape, lambda r: (0, 0)),
        ],
        out_specs=pl.BlockSpec((rows // CAP, 1, CAP, cols), lambda r: (0, r, 0, 0)),
        out_shape=jax.ShapeDtypeStruct((rows // CAP, sources, CAP, cols), BF16),
        compiler_params=params(),
        name="down",
    )(ho, hp, down)


def combine_kernel(res_ref, routes_ref, logits_ref, out_ref):
    experts = res_ref.shape[0]
    first, second, count, before = chosen(routes_ref[0], experts)
    logits = logits_ref[0].astype(F32)
    l0 = jnp.sum(jnp.where(first, logits, 0.0), axis=0, keepdims=True)
    l1 = jnp.sum(jnp.where(second, logits, 0.0), axis=0, keepdims=True)
    w0 = 1.0 / (1.0 + jnp.exp(l1 - l0))
    w1 = 1.0 / (1.0 + jnp.exp(l0 - l1))
    weight = jnp.where(first, w0, 0.0) + jnp.where(second, w1, 0.0)
    place = slot_matrix(weight, before, count)
    coarse = place.astype(BF16)
    fine = (place - coarse.astype(F32)).astype(BF16)
    res = res_ref[...].reshape(experts * CAP, res_ref.shape[3])
    total = mm(coarse, res, ((0,), (0,))) + mm(fine, res, ((0,), (0,)))
    out_ref[...] = total.astype(BF16)


def combined(res, routes, logits):
    experts, blocks, _, cols = res.shape
    toks = routes.shape[2]
    return pl.pallas_call(
        combine_kernel,
        grid=(blocks,),
        in_specs=[
            pl.BlockSpec((experts, 1, CAP, cols), lambda r: (0, r, 0, 0)),
            pl.BlockSpec((1, 2, toks), lambda r: (r, 0, 0)),
            pl.BlockSpec((1, experts, toks), lambda r: (r, 0, 0)),
        ],
        out_specs=pl.BlockSpec((toks, cols), lambda r: (r, 0)),
        out_shape=jax.ShapeDtypeStruct((blocks * toks, cols), BF16),
        compiler_params=params(),
        name="combine",
    )(res, routes, logits)


def per_device(
    mix_input,
    moe_input,
    norm_mix,
    query_weight,
    forget_weight,
    value_weight,
    forget_gap,
    norm_out,
    norm_moe,
    router_weight,
    expert_gate,
    expert_up,
    expert_down,
    routes,
):
    toks, width = moe_input.shape
    experts = router_weight.shape[1]
    x = lax.axis_index("tp").astype(jnp.int32).reshape(1)
    near = [(i, i ^ 1) for i in range(4)]
    far = [(i, 3 - i) for i in range(4)]
    by_block = routes.reshape(4, toks, 2).transpose(0, 2, 1)

    rows_b, logits, own = front(
        x, moe_input, norm_moe.reshape(1, -1), router_weight, by_block, experts
    )
    rows_near = lax.ppermute(rows_b, "tp", near)
    gate_far = lax.ppermute(expert_gate[0], "tp", far)
    up_far = lax.ppermute(expert_up[0], "tp", far)
    swap = lambda a: lax.all_to_all(a, EP, split_axis=0, concat_axis=0, tiled=True)
    own_rows = swap(own).reshape(experts * CAP, width)
    other = refill(x ^ 1, rows_near, by_block, experts)
    near_rows = swap(other).reshape(experts * CAP, width)

    rows_a = normed(mix_input, norm_mix).astype(BF16)
    group_a = lax.all_gather(rows_a, "tp", axis=0, tiled=True)
    group_logits = lax.all_gather(logits, "tp", axis=0).transpose(0, 2, 1)
    inside, query, packed = mixer(
        group_a, query_weight, forget_weight, value_weight, forget_gap.reshape(1, -1)
    )
    state = arriving_state(packed)
    mixer_out = readout(inside, query, state, norm_out.reshape(1, -1))

    weights = (expert_gate[0], expert_up[0], gate_far, up_far)
    h_own = lax.all_gather(hidden_units(own_rows, *weights), "tp", axis=0)
    h_near = lax.all_gather(hidden_units(near_rows, *weights), "tp", axis=0)
    summed = down_rows(h_own, h_near, expert_down[0])
    returned = swap(summed)
    expert_out = combined(returned, by_block, group_logits)
    return (mixer_out, expert_out)


def solution(mesh):
    finer = Mesh(mesh.devices.reshape(4, 4, 2, mesh.shape["tp"]), ("ep_0", "ep_1", "ep_2", "tp"))
    placed = (
        P(EP_TP, None),
        P(EP_TP, None),
        P(),
        P(None, "tp"),
        P(None, "tp"),
        P(None, "tp"),
        P("tp"),
        P("tp"),
        P(),
        P(),
        P(EP, None, "tp"),
        P(EP, None, "tp"),
        P(EP, None, "tp"),
        P(EP, None),
    )
    return jax.shard_map(
        per_device,
        mesh=finer,
        in_specs=placed,
        out_specs=(P(EP, "tp"), P(EP, "tp")),
        check_vma=False,
    )
```

```python
import functools

import jax
import jax.numpy as jnp
from jax import lax
from jax.experimental import pallas as pl
from jax.experimental.pallas import tpu as pltpu
from jax.sharding import Mesh
from jax.sharding import PartitionSpec as P

HEAD_DIM = 128
HALF = 8
EP = ("ep_0", "ep_1", "ep_2")
EP_TP = ("ep_0", "ep_1", "ep_2", "tp")

EPSILON = 1e-06
CLAMP_LIMIT = 7.0
SWISH_SLOPE = 1.702
EXACT = lax.Precision.HIGHEST
F32 = jnp.float32
BF16 = jnp.bfloat16


def mm(a, b, contract=((1,), (0,)), precision=None):
    return lax.dot_general(
        a, b, (contract, ((), ())), precision=precision, preferred_element_type=F32
    )


def params(mib=56, axes=("arbitrary",)):
    return pltpu.CompilerParams(vmem_limit_bytes=mib << 20, dimension_semantics=axes)


def normed(row_data, gain_vec):
    as_float = row_data.astype(F32)
    scale = lax.rsqrt(jnp.mean(as_float * as_float, axis=-1, keepdims=True) + EPSILON)
    return as_float * scale * gain_vec


def chosen(routes, experts):
    toks = routes.shape[1]
    ids = lax.broadcasted_iota(jnp.int32, (experts, toks), 0)
    first = routes[0:1, :] == ids
    second = routes[1:2, :] == ids
    count = jnp.where(first | second, 1.0, 0.0)
    earlier = (
        lax.broadcasted_iota(jnp.int32, (toks, toks), 0)
        < lax.broadcasted_iota(jnp.int32, (toks, toks), 1)
    )
    before = mm(count.astype(BF16), jnp.where(earlier, 1.0, 0.0).astype(BF16))
    return first, second, count, before


def slot_matrix(weight, before, count, half):
    experts, toks = weight.shape
    place = lax.broadcasted_iota(jnp.int32, (experts, HALF, toks), 1) + half * HALF
    here = (before[:, None, :] == place.astype(F32)) & (count[:, None, :] > 0.5)
    return jnp.where(here, weight[:, None, :], 0.0).reshape(experts * HALF, toks)


def fill(routes, rows, experts):
    _, _, count, before = chosen(routes, experts)
    pick = lambda half: slot_matrix(count, before, count, half).astype(BF16)
    return [mm(pick(half), rows).astype(BF16) for half in range(2)]


def front_kernel(src, x_ref, gain_ref, router_ref, routes_ref, rows_ref, logits_ref, buf_ref, *, group):
    step = pl.program_id(0)
    width = x_ref.shape[1]

    @pl.when(step == 0)
    def _():
        rows_ref[...] = normed(x_ref[...], gain_ref[...]).astype(BF16)
        logits_ref[...] = mm(router_ref[...], rows_ref[...], ((1,), (1,))).astype(BF16)

    low, high = fill(routes_ref[0] - step * group, rows_ref[...], group)
    buf_ref[:, :width] = low
    buf_ref[:, width:] = high


def refill_kernel(src, rows_ref, router_ref, routes_ref, logits_ref, low_ref, high_ref, *, group):
    step = pl.program_id(0)

    @pl.when(step == 0)
    def _():
        logits_ref[...] = mm(router_ref[...], rows_ref[...], ((1,), (1,))).astype(BF16)

    low_ref[...], high_ref[...] = fill(routes_ref[0] - step * group, rows_ref[...], group)


def front(src, x, gain, router, routes):
    toks, width = x.shape
    experts = router.shape[0]
    group = 8
    whole = lambda i, s: (0, 0)
    return pl.pallas_call(
        functools.partial(front_kernel, group=group),
        grid_spec=pltpu.PrefetchScalarGridSpec(
            num_scalar_prefetch=1,
            grid=(experts // group,),
            in_specs=[
                pl.BlockSpec((toks, width), whole),
                pl.BlockSpec((1, width), whole),
                pl.BlockSpec(router.shape, whole),
                pl.BlockSpec((1, 2, toks), lambda i, s: (s[0], 0, 0)),
            ],
            out_specs=[
                pl.BlockSpec((toks, width), whole),
                pl.BlockSpec((experts, toks), whole),
                pl.BlockSpec((group * HALF, 2 * width), lambda i, s: (i, 0)),
            ],
        ),
        out_shape=[
            jax.ShapeDtypeStruct((toks, width), BF16),
            jax.ShapeDtypeStruct((experts, toks), BF16),
            jax.ShapeDtypeStruct((experts * HALF, 2 * width), BF16),
        ],
        compiler_params=params(),
        name="front",
    )(src, x, gain, router, routes)


def refill(src, rows, router, routes):
    toks, width = rows.shape
    experts = router.shape[0]
    group = 8
    whole = lambda i, s: (0, 0)
    return pl.pallas_call(
        functools.partial(refill_kernel, group=group),
        grid_spec=pltpu.PrefetchScalarGridSpec(
            num_scalar_prefetch=1,
            grid=(experts // group,),
            in_specs=[
                pl.BlockSpec((toks, width), whole),
                pl.BlockSpec(router.shape, whole),
                pl.BlockSpec((1, 2, toks), lambda i, s: (s[1], 0, 0)),
            ],
            out_specs=[
                pl.BlockSpec((experts, toks), whole),
                pl.BlockSpec((group * HALF, width), lambda i, s: (i, 0)),
                pl.BlockSpec((group * HALF, width), lambda i, s: (i, 0)),
            ],
        ),
        out_shape=[
            jax.ShapeDtypeStruct((experts, toks), BF16),
            jax.ShapeDtypeStruct((experts * HALF, width), BF16),
            jax.ShapeDtypeStruct((experts * HALF, width), BF16),
        ],
        compiler_params=params(),
        name="refill",
    )(src, rows, router, routes)


def mixer_kernel(
    src, a0, a1, a2, a3, q_ref, f_ref, v_ref, gap_ref, inside_ref, query_ref, packed_ref, qa, fa, va, group
):
    step = pl.program_id(0)

    @pl.when(step == 0)
    def _():
        qa[...] = jnp.zeros_like(qa)
        fa[...] = jnp.zeros_like(fa)
        va[...] = jnp.zeros_like(va)

    toks = a0.shape[0]
    for k, part in enumerate((a0, a1, a2, a3)):
        group[pl.ds(pl.multiple_of(src[k] * toks, toks), toks), :] = part[...]
    a = group[...]
    qa[...] += mm(a, q_ref[...])
    fa[...] += mm(a, f_ref[...])
    va[...] += mm(a, v_ref[...])

    @pl.when(step == pl.num_programs(0) - 1)
    def _():
        rows = a.shape[0]
        causal = (
            lax.broadcasted_iota(jnp.int32, (rows, rows), 0)
            >= lax.broadcasted_iota(jnp.int32, (rows, rows), 1)
        )
        ones = jnp.where(causal, 1.0, 0.0)
        heads = packed_ref.shape[0]
        for h in range(heads):
            at = slice(h * HEAD_DIM, (h + 1) * HEAD_DIM)
            shut = gap_ref[:, at] * jax.nn.sigmoid(-fa[:, at])
            sums = mm(ones, jnp.log1p(-shut), precision=EXACT)
            last = sums[rows - 1 :, :]
            value = va[:, at]
            query = qa[:, at] * jnp.exp(sums)
            scores = mm(query, shut * jnp.exp(-sums), ((1,), (1,)), EXACT)
            scores = jnp.where(causal, scores, 0.0)
            inside_ref[:, at] = mm(scores, value, precision=EXACT)
            query_ref[:, at] = query
            packed_ref[h, :HEAD_DIM, :] = mm(
                value, shut * jnp.exp(last - sums), ((0,), (0,)), EXACT
            )
            packed_ref[h, HEAD_DIM:, :] = jnp.broadcast_to(last, (8, HEAD_DIM))


def mixer(src, parts, wq, wf, wv, gap):
    toks, width = parts[0].shape
    rows = 4 * toks
    cols = wq.shape[1]
    heads = cols // HEAD_DIM
    kb = 512
    fixed = lambda i, s: (0, 0)
    weight = pl.BlockSpec((kb, cols), lambda i, s: (i, 0))
    return pl.pallas_call(
        mixer_kernel,
        grid_spec=pltpu.PrefetchScalarGridSpec(
            num_scalar_prefetch=1,
            grid=(width // kb,),
            in_specs=[pl.BlockSpec((toks, kb), lambda i, s: (0, i))] * 4
            + [weight, weight, weight, pl.BlockSpec((1, cols), fixed)],
            out_specs=[
                pl.BlockSpec((rows, cols), fixed),
                pl.BlockSpec((rows, cols), fixed),
                pl.BlockSpec((heads, HEAD_DIM + 8, HEAD_DIM), lambda i, s: (0, 0, 0)),
            ],
            scratch_shapes=[pltpu.VMEM((rows, cols), F32)] * 3 + [pltpu.VMEM((rows, kb), BF16)],
        ),
        out_shape=[
            jax.ShapeDtypeStruct((rows, cols), F32),
            jax.ShapeDtypeStruct((rows, cols), F32),
            jax.ShapeDtypeStruct((heads, HEAD_DIM + 8, HEAD_DIM), F32),
        ],
        compiler_params=params(),
        name="mixer",
    )(src, *parts, wq, wf, wv, gap)


def readout_kernel(inside_ref, query_ref, state_ref, gain_ref, out_ref):
    total = inside_ref[...] + mm(query_ref[...], state_ref[0], ((1,), (1,)), EXACT)
    out_ref[...] = normed(total, gain_ref[...]).astype(BF16)


def readout(inside, query, state, gain):
    rows, cols = inside.shape
    block = pl.BlockSpec((rows, HEAD_DIM), lambda h: (0, h))
    return pl.pallas_call(
        readout_kernel,
        grid=(cols // HEAD_DIM,),
        in_specs=[
            block,
            block,
            pl.BlockSpec((1, HEAD_DIM, HEAD_DIM), lambda h: (h, 0, 0)),
            pl.BlockSpec((1, HEAD_DIM), lambda h: (0, h)),
        ],
        out_specs=block,
        out_shape=jax.ShapeDtypeStruct((rows, cols), BF16),
        compiler_params=params(),
        name="readout",
    )(inside, query, state, gain)


def pieces(packed):
    return packed[:, HEAD_DIM : HEAD_DIM + 1, :], packed[:, :HEAD_DIM, :]


def link(earlier, later):
    return earlier[0] + later[0], jnp.exp(later[0]) * earlier[1] + later[1]


def pack(part):
    heads = part[1].shape[0]
    return jnp.concatenate(
        [part[1], jnp.broadcast_to(part[0], (heads, 8, HEAD_DIM))], axis=1
    )


def masked(flag, part):
    return jax.tree.map(lambda a: jnp.where(flag, a, 0.0), part)


def arriving_state(packed):
    core = lax.axis_index("ep_2")
    row = lax.axis_index("ep_1")
    other = lax.ppermute(packed, "ep_2", [(0, 1), (1, 0)])
    is_second = core == 1
    low = jnp.where(is_second, other, packed)
    high = jnp.where(is_second, packed, other)
    half = packed.shape[0] // 2
    mine = lambda a: lax.dynamic_slice_in_dim(a, core * half, half, 0)
    chip = link(pieces(mine(low)), pieces(mine(high)))
    count = lax.axis_size("ep_1")
    sent = pack(chip)
    before = after = None
    for d in range(count - 1, 0, -1):
        came = pieces(lax.ppermute(sent, "ep_1", [(i, (i + d) % count) for i in range(count)]))
        early = masked(row >= d, came)
        late = masked(row < d, came)
        before = early if before is None else link(before, early)
        after = late if after is None else link(after, late)
    plane = pack(link(link(before, chip), after))
    planes = None
    count = lax.axis_size("ep_0")
    for d in range(count - 1, 0, -1):
        came = pieces(lax.ppermute(plane, "ep_0", [(i, i + d) for i in range(count - d)]))
        planes = came if planes is None else link(planes, came)
    state = link(planes, before)[1]
    swapped = lax.ppermute(state, "ep_2", [(0, 1), (1, 0)])
    entering = jnp.concatenate(
        [jnp.where(is_second, swapped, state), jnp.where(is_second, state, swapped)], axis=0
    )
    first_core = pieces(low)
    return jnp.where(is_second, jnp.exp(first_core[0]) * entering + first_core[1], entering)


def hidden_kernel(own_ref, near_ref, go_ref, uo_ref, gf_ref, uf_ref, out_ref, gate, up):
    step = pl.program_id(0)

    @pl.when(step == 0)
    def _():
        gate[...] = jnp.zeros_like(gate)
        up[...] = jnp.zeros_like(up)

    rows = jnp.concatenate([own_ref[...], near_ref[...]], axis=0)
    n = go_ref.shape[1]
    gate[:, :n] += mm(rows, go_ref[...])
    gate[:, n:] += mm(rows, gf_ref[...])
    up[:, :n] += mm(rows, uo_ref[...])
    up[:, n:] += mm(rows, uf_ref[...])

    @pl.when(step == pl.num_programs(0) - 1)
    def _():
        gated = jnp.minimum(gate[...], CLAMP_LIMIT)
        opened = jnp.clip(up[...], -CLAMP_LIMIT, CLAMP_LIMIT)
        out_ref[...] = (
            (opened + 1.0) * gated * jax.nn.sigmoid(SWISH_SLOPE * gated)
        ).astype(BF16)


def hidden_units(own, near, half, weights):
    count = own.shape[0]
    width, n = weights[0].shape
    kb = 1024
    weight = pl.BlockSpec((kb, n), lambda i: (i, 0))
    return pl.pallas_call(
        hidden_kernel,
        grid=(width // kb,),
        in_specs=[
            pl.BlockSpec((count, kb), lambda i: (0, i + half * (width // kb))),
            pl.BlockSpec((count, kb), lambda i: (0, i)),
            weight,
            weight,
            weight,
            weight,
        ],
        out_specs=pl.BlockSpec((2 * count, 2 * n), lambda i: (0, 0)),
        out_shape=jax.ShapeDtypeStruct((2 * count, 2 * n), BF16),
        scratch_shapes=[pltpu.VMEM((2 * count, 2 * n), F32)] * 2,
        compiler_params=params(),
        name="hidden",
    )(own, near, *weights)


def down_kernel(src, h_own, h_near, h_far, h_opp, down_ref, out_ref):
    k = pl.program_id(0)
    n = down_ref.shape[0] // 4
    rows = out_ref.shape[0]
    unit = lambda s: down_ref[pl.ds(pl.multiple_of(s * n, n), n), :]
    for this, (mine, other, twin) in enumerate(
        ((h_own, h_near, 1), (h_near, h_own, 0), (h_far, h_opp, 3), (h_opp, h_far, 2))
    ):

        @pl.when(k == this)
        def _():
            s, t = src[this], src[twin]
            total = mm(mine[:rows, :n], unit(s)) + mm(mine[:rows, n:], unit(3 - s))
            total += mm(other[rows:, :n], unit(t)) + mm(other[rows:, n:], unit(3 - t))
            out_ref[...] = total.astype(BF16)


def down_rows(src, parts, down):
    both, width = parts[0].shape
    cols = down.shape[1]
    whole = lambda k, s: (0, 0)
    return pl.pallas_call(
        down_kernel,
        grid_spec=pltpu.PrefetchScalarGridSpec(
            num_scalar_prefetch=1,
            grid=(4,),
            in_specs=[pl.BlockSpec((both, width), whole)] * 4 + [pl.BlockSpec(down.shape, whole)],
            out_specs=pl.BlockSpec((both // 2, cols), lambda k, s: (0, s[k])),
        ),
        out_shape=jax.ShapeDtypeStruct((both // 2, 4 * cols), BF16),
        compiler_params=params(),
        name="down",
    )(src, *parts, down)


def combine_kernel(src, low_ref, high_ref, routes_ref, logits_ref, out_ref):
    experts = logits_ref.shape[1]
    first, second, count, before = chosen(routes_ref[0], experts)
    logits = logits_ref[0].astype(F32)
    l0 = jnp.sum(jnp.where(first, logits, 0.0), axis=0, keepdims=True)
    l1 = jnp.sum(jnp.where(second, logits, 0.0), axis=0, keepdims=True)
    w0 = 1.0 / (1.0 + jnp.exp(l1 - l0))
    w1 = 1.0 / (1.0 + jnp.exp(l0 - l1))
    weight = jnp.where(first, w0, 0.0) + jnp.where(second, w1, 0.0)
    total = None
    for half, res_ref in enumerate((low_ref, high_ref)):
        place = slot_matrix(weight, before, count, half)
        coarse = place.astype(BF16)
        fine = (place - coarse.astype(F32)).astype(BF16)
        res = res_ref[...]
        part = mm(coarse, res, ((0,), (0,))) + mm(fine, res, ((0,), (0,)))
        total = part if total is None else total + part
    out_ref[...] = total.astype(BF16)


def combined(src, low, high, routes, logits):
    slots = low.shape[0]
    cols = low.shape[1] // 4
    toks = routes.shape[2]
    res = pl.BlockSpec((slots, cols), lambda k, s: (0, s[k]))
    return pl.pallas_call(
        combine_kernel,
        grid_spec=pltpu.PrefetchScalarGridSpec(
            num_scalar_prefetch=1,
            grid=(4,),
            in_specs=[
                res,
                res,
                pl.BlockSpec((1, 2, toks), lambda k, s: (s[k], 0, 0)),
                pl.BlockSpec((1,) + logits.shape[1:], lambda k, s: (k, 0, 0)),
            ],
            out_specs=pl.BlockSpec((toks, cols), lambda k, s: (s[k], 0)),
        ),
        out_shape=jax.ShapeDtypeStruct((4 * toks, cols), BF16),
        compiler_params=params(),
        name="combine",
    )(src, low, high, routes, logits)


NEAR = [(i, i ^ 1) for i in range(4)]
FAR = [(i, 3 - i) for i in range(4)]


def to_near(a):
    return lax.ppermute(a, "tp", NEAR)


def to_far(a):
    return lax.ppermute(a, "tp", FAR)


def shared(a):
    far = to_far(a)
    near = to_near(a)
    return a, near, far, to_near(far)


def swap(a):
    experts = 32
    rows, cols = a.shape
    out = lax.all_to_all(
        a.reshape(experts, rows // experts, cols), EP, split_axis=0, concat_axis=0, tiled=True
    )
    return out.reshape(rows, cols)


def per_device(
    mix_input,
    moe_input,
    norm_mix,
    query_weight,
    forget_weight,
    value_weight,
    forget_gap,
    norm_out,
    norm_moe,
    router_weight,
    expert_gate,
    expert_up,
    expert_down,
    routes,
):
    toks = moe_input.shape[0]
    x = lax.axis_index("tp").astype(jnp.int32)
    src = jnp.stack([x, x ^ 1, 3 - x, x ^ 2])
    by_block = routes.reshape(4, toks, 2).transpose(0, 2, 1)
    router = router_weight.T

    gate_far = to_far(expert_gate[0])
    rows_b, logits, own = front(src, moe_input, norm_moe.reshape(1, -1), router, by_block)
    own_rows = swap(own)
    rows_near = to_near(rows_b)
    mix_input, _ = lax.optimization_barrier((mix_input, rows_b))
    rows_a = normed(mix_input, norm_mix).astype(BF16)
    group_a = shared(rows_a)
    up_far = to_far(expert_up[0])
    logits_near, low, high = refill(src, rows_near, router, by_block)
    low, own_rows = lax.optimization_barrier((low, own_rows))
    low_rows = swap(low)
    high, low_rows = lax.optimization_barrier((high, low_rows))
    high_rows = swap(high)
    logits = jnp.stack([logits, logits_near])
    logits = jnp.concatenate([logits, to_far(logits)])

    inside, query, packed = mixer(
        src,
        group_a,
        query_weight,
        forget_weight,
        value_weight,
        forget_gap.reshape(1, -1),
    )

    low_rows, packed = lax.optimization_barrier((low_rows, packed))
    weights = (expert_gate[0], expert_up[0], gate_far, up_far)
    h_low = shared(hidden_units(own_rows, low_rows, 0, weights))
    high_rows, far = lax.optimization_barrier((high_rows, h_low[2]))
    h_high = shared(hidden_units(own_rows, high_rows, 1, weights))
    opp, high_own = lax.optimization_barrier((h_low[3], h_high[0]))
    back_low = swap(down_rows(src, h_low[:2] + (far, opp), expert_down[0]))
    back_high = swap(down_rows(src, (high_own,) + h_high[1:], expert_down[0]))

    state = arriving_state(packed)
    mixer_out = readout(inside, query, state, norm_out.reshape(1, -1))
    expert_out = combined(src, back_low, back_high, by_block, logits)
    return (mixer_out, expert_out)


def solution(mesh):
    finer = Mesh(mesh.devices.reshape(4, 4, 2, mesh.shape["tp"]), ("ep_0", "ep_1", "ep_2", "tp"))
    placed = (
        P(EP_TP, None),
        P(EP_TP, None),
        P(),
        P(None, "tp"),
        P(None, "tp"),
        P(None, "tp"),
        P("tp"),
        P("tp"),
        P(),
        P(),
        P(EP, None, "tp"),
        P(EP, None, "tp"),
        P(EP, None, "tp"),
        P(EP, None),
    )

    return jax.shard_map(
        per_device,
        mesh=finer,
        in_specs=placed,
        out_specs=(P(EP, "tp"), P(EP, "tp")),
        check_vma=False,
    )
```

```python
import functools

import jax
import jax.numpy as jnp
from jax import lax
from jax.experimental import pallas as pl
from jax.experimental.pallas import tpu as pltpu
from jax.sharding import Mesh
from jax.sharding import PartitionSpec as P

HEAD_DIM = 128

CAP = 16
HALF = 8
EP = ("ep_0", "ep_1", "ep_2")
EP_TP = ("ep_0", "ep_1", "ep_2", "tp")

EPSILON = 1e-06
CLAMP_LIMIT = 7.0
SWISH_SLOPE = 1.702
F32 = jnp.float32
BF16 = jnp.bfloat16


def mm(a, b, contract=((1,), (0,))):
    return lax.dot_general(a, b, (contract, ((), ())), preferred_element_type=F32)


def halves(a):
    high = a.astype(BF16)
    return high, (a - high.astype(F32)).astype(BF16)


def params(mib=56, axes=("arbitrary",)):
    return pltpu.CompilerParams(vmem_limit_bytes=mib << 20, dimension_semantics=axes)


def normed(row_data, gain_vec):
    as_float = row_data.astype(F32)
    scale = lax.rsqrt(jnp.mean(as_float * as_float, axis=-1, keepdims=True) + EPSILON)
    return as_float * scale * gain_vec


def chosen(routes, experts):
    toks = routes.shape[1]
    ids = lax.broadcasted_iota(jnp.int32, (experts, toks), 0)
    first = routes[0:1, :] == ids
    second = routes[1:2, :] == ids
    count = jnp.where(first | second, 1.0, 0.0)
    earlier = (
        lax.broadcasted_iota(jnp.int32, (toks, toks), 0)
        < lax.broadcasted_iota(jnp.int32, (toks, toks), 1)
    )
    before = mm(count.astype(BF16), jnp.where(earlier, 1.0, 0.0).astype(BF16))
    return first, second, count, before


def slot_matrix(weight, before, count, half):
    experts, toks = weight.shape
    place = lax.broadcasted_iota(jnp.int32, (experts, HALF, toks), 1) + half * HALF
    here = (before[:, None, :] == place.astype(F32)) & (count[:, None, :] > 0.5)
    return jnp.where(here, weight[:, None, :], 0.0).reshape(experts * HALF, toks)


def fill(routes, rows, experts):
    _, _, count, before = chosen(routes, experts)
    pick = [slot_matrix(count, before, count, half) for half in range(2)]
    both = mm(jnp.concatenate(pick, axis=0).astype(BF16), rows).astype(BF16)
    return both[: experts * HALF], both[experts * HALF :]


def front_kernel(src, x_ref, gain_ref, routes_ref, rows_ref, buf_ref, *, group):
    step = pl.program_id(0)
    width = x_ref.shape[1]

    @pl.when(step == 0)
    def _():
        rows_ref[...] = normed(x_ref[...], gain_ref[...]).astype(BF16)

    low, high = fill(routes_ref[0] - step * group, rows_ref[...], group)
    buf_ref[:, :width] = low
    buf_ref[:, width:] = high


def refill_kernel(src, own_ref, rows_ref, router_ref, routes_ref, logits_ref, low_ref, high_ref, *, group):
    step = pl.program_id(0)

    @pl.when(step == 0)
    def _():
        for k, ref in enumerate((own_ref, rows_ref)):
            logits_ref[k] = mm(router_ref[...], ref[...], ((1,), (1,))).astype(BF16)

    low_ref[...], high_ref[...] = fill(routes_ref[0] - step * group, rows_ref[...], group)


def front(src, x, gain, routes, experts):
    toks, width = x.shape
    group = 16
    whole = lambda i, s: (0, 0)
    return pl.pallas_call(
        functools.partial(front_kernel, group=group),
        grid_spec=pltpu.PrefetchScalarGridSpec(
            num_scalar_prefetch=1,
            grid=(experts // group,),
            in_specs=[
                pl.BlockSpec((toks, width), whole),
                pl.BlockSpec((1, width), whole),
                pl.BlockSpec((1, 2, toks), lambda i, s: (s[0], 0, 0)),
            ],
            out_specs=[
                pl.BlockSpec((toks, width), whole),
                pl.BlockSpec((group * HALF, 2 * width), lambda i, s: (i, 0)),
            ],
        ),
        out_shape=[
            jax.ShapeDtypeStruct((toks, width), BF16),
            jax.ShapeDtypeStruct((experts * HALF, 2 * width), BF16),
        ],
        compiler_params=params(),
        name="front",
    )(src, x, gain, routes)


def refill(src, own, rows, router, routes):
    toks, width = rows.shape
    experts = router.shape[0]
    group = 16
    whole = lambda i, s: (0, 0)
    return pl.pallas_call(
        functools.partial(refill_kernel, group=group),
        grid_spec=pltpu.PrefetchScalarGridSpec(
            num_scalar_prefetch=1,
            grid=(experts // group,),
            in_specs=[
                pl.BlockSpec((toks, width), whole),
                pl.BlockSpec((toks, width), whole),
                pl.BlockSpec(router.shape, whole),
                pl.BlockSpec((1, 2, toks), lambda i, s: (s[1], 0, 0)),
            ],
            out_specs=[
                pl.BlockSpec((2, experts, toks), lambda i, s: (0, 0, 0)),
                pl.BlockSpec((group * HALF, width), lambda i, s: (i, 0)),
                pl.BlockSpec((group * HALF, width), lambda i, s: (i, 0)),
            ],
        ),
        out_shape=[
            jax.ShapeDtypeStruct((2, experts, toks), BF16),
            jax.ShapeDtypeStruct((experts * HALF, width), BF16),
            jax.ShapeDtypeStruct((experts * HALF, width), BF16),
        ],
        compiler_params=params(),
        name="refill",
    )(src, own, rows, router, routes)


def mixer_kernel(
    src, a0, a1, a2, a3, q_ref, f_ref, v_ref, gap_ref, inside_ref, query_ref, packed_ref, qa, fa, va, group
):
    step = pl.program_id(0)

    @pl.when(step == 0)
    def _():
        qa[...] = jnp.zeros_like(qa)
        fa[...] = jnp.zeros_like(fa)
        va[...] = jnp.zeros_like(va)

    toks = a0.shape[0]
    for k, part in enumerate((a0, a1, a2, a3)):
        group[pl.ds(pl.multiple_of(src[k] * toks, toks), toks), :] = part[...]
    a = group[...]
    qa[...] += mm(a, q_ref[...])
    fa[...] += mm(a, f_ref[...])
    va[...] += mm(a, v_ref[...])

    @pl.when(step == pl.num_programs(0) - 1)
    def _():
        rows = a.shape[0]
        causal = (
            lax.broadcasted_iota(jnp.int32, (rows, rows), 0)
            >= lax.broadcasted_iota(jnp.int32, (rows, rows), 1)
        )
        ones = jnp.where(causal[:toks, :toks], 1.0, 0.0).astype(BF16)
        shut = gap_ref[...] * jax.nn.sigmoid(-fa[...])
        fa[...] = jnp.log1p(-shut)
        cols = shut.shape[1]
        base = None
        for k in range(rows // toks):
            part = fa[k * toks : (k + 1) * toks, :]
            high = part.astype(BF16)
            rest = part - high.astype(F32)
            mid = rest.astype(BF16)
            low = (rest - mid.astype(F32)).astype(BF16)
            sums = mm(ones, jnp.concatenate([high, mid, low], axis=1))
            sums = sums[:, :cols] + sums[:, cols : 2 * cols] + sums[:, 2 * cols :]
            sums = sums if base is None else sums + base
            base = sums[toks - 1 :, :]
            fa[k * toks : (k + 1) * toks, :] = sums
        sums = fa[...]
        last = sums[rows - 1 :, :]
        query_ref[...] = qa[...] * jnp.exp(sums)
        keys = shut * jnp.exp(-sums)
        late = shut * jnp.exp(last - sums)
        half = rows // 2
        for h in range(packed_ref.shape[0]):
            at = slice(h * HEAD_DIM, (h + 1) * HEAD_DIM)
            q_high, q_low = halves(query_ref[:, at])
            k_high, k_low = halves(keys[:, at])
            v_high, v_low = halves(va[:, at])
            l_high, l_low = halves(late[:, at])
            left = jnp.concatenate([q_high, q_low, q_high], axis=1)
            right = jnp.concatenate([k_high, k_high, k_low], axis=1)
            values = jnp.concatenate([v_high, v_low], axis=1)
            for k in range(2):
                end = (k + 1) * half
                scores = mm(left[end - half : end], right[:end], ((1,), (1,)))
                s_high, s_low = halves(jnp.where(causal[end - half : end, :end], scores, 0.0))
                part = mm(s_high, values[:end])
                part = part[:, :HEAD_DIM] + part[:, HEAD_DIM:] + mm(s_low, v_high[:end])
                inside_ref[end - half : end, at] = part
            outer = mm(values, jnp.concatenate([l_high, l_low], axis=1), ((0,), (0,)))
            packed_ref[h, :HEAD_DIM, :] = (
                outer[:HEAD_DIM, :HEAD_DIM]
                + outer[:HEAD_DIM, HEAD_DIM:]
                + outer[HEAD_DIM:, :HEAD_DIM]
            )
            packed_ref[h, HEAD_DIM:, :] = jnp.broadcast_to(last[:, at], (8, HEAD_DIM))


def mixer(src, parts, wq, wf, wv, gap):
    toks, width = parts[0].shape
    rows = 4 * toks
    cols = wq.shape[1]
    heads = cols // HEAD_DIM
    kb = 512
    fixed = lambda i, s: (0, 0)
    weight = pl.BlockSpec((kb, cols), lambda i, s: (i, 0))
    return pl.pallas_call(
        mixer_kernel,
        grid_spec=pltpu.PrefetchScalarGridSpec(
            num_scalar_prefetch=1,
            grid=(width // kb,),
            in_specs=[pl.BlockSpec((toks, kb), lambda i, s: (0, i))] * 4
            + [weight, weight, weight, pl.BlockSpec((1, cols), fixed)],
            out_specs=[
                pl.BlockSpec((rows, cols), fixed),
                pl.BlockSpec((rows, cols), fixed),
                pl.BlockSpec((heads, HEAD_DIM + 8, HEAD_DIM), lambda i, s: (0, 0, 0)),
            ],
            scratch_shapes=[pltpu.VMEM((rows, cols), F32)] * 3 + [pltpu.VMEM((rows, kb), BF16)],
        ),
        out_shape=[
            jax.ShapeDtypeStruct((rows, cols), F32),
            jax.ShapeDtypeStruct((rows, cols), F32),
            jax.ShapeDtypeStruct((heads, HEAD_DIM + 8, HEAD_DIM), F32),
        ],
        compiler_params=params(),
        name="mixer",
    )(src, *parts, wq, wf, wv, gap)


def readout_kernel(inside_ref, query_ref, state_ref, gain_ref, out_ref):
    q_high, q_low = halves(query_ref[...])
    s_high, s_low = halves(state_ref[0])
    total = inside_ref[...] + mm(
        jnp.concatenate([q_high, q_low, q_high], axis=1),
        jnp.concatenate([s_high, s_high, s_low], axis=1),
        ((1,), (1,)),
    )
    out_ref[...] = normed(total, gain_ref[...]).astype(BF16)


def readout(inside, query, state, gain):
    rows, cols = inside.shape
    block = pl.BlockSpec((rows, HEAD_DIM), lambda h: (0, h))
    return pl.pallas_call(
        readout_kernel,
        grid=(cols // HEAD_DIM,),
        in_specs=[
            block,
            block,
            pl.BlockSpec((1, HEAD_DIM, HEAD_DIM), lambda h: (h, 0, 0)),
            pl.BlockSpec((1, HEAD_DIM), lambda h: (0, h)),
        ],
        out_specs=block,
        out_shape=jax.ShapeDtypeStruct((rows, cols), BF16),
        compiler_params=params(),
        name="readout",
    )(inside, query, state, gain)


def pieces(packed):
    return packed[:, HEAD_DIM : HEAD_DIM + 1, :], packed[:, :HEAD_DIM, :]


def link(earlier, later):
    return earlier[0] + later[0], jnp.exp(later[0]) * earlier[1] + later[1]


def pack(part):
    heads = part[1].shape[0]
    return jnp.concatenate(
        [part[1], jnp.broadcast_to(part[0], (heads, 8, HEAD_DIM))], axis=1
    )


def masked(flag, part):
    return jax.tree.map(lambda a: jnp.where(flag, a, 0.0), part)


def both_cores(a):
    return lax.ppermute(a, "ep_2", [(0, 1), (1, 0)])


def along_rows(packed):
    core = lax.axis_index("ep_2")
    other = both_cores(packed)
    is_second = core == 1
    low = jnp.where(is_second, other, packed)
    high = jnp.where(is_second, packed, other)
    half = packed.shape[0] // 2
    mine = lambda a: lax.dynamic_slice_in_dim(a, core * half, half, 0)
    chip = link(pieces(mine(low)), pieces(mine(high)))
    count = lax.axis_size("ep_1")
    sent = pack(chip)
    came = [
        lax.ppermute(sent, "ep_1", [(i, (i + d) % count) for i in range(count)])
        for d in range(count - 1, 0, -1)
    ]
    return low, chip, came


def along_planes(chip, came):
    row = lax.axis_index("ep_1")
    before = after = None
    for k, part in enumerate(came):
        d = len(came) - k
        early = masked(row >= d, pieces(part))
        late = masked(row < d, pieces(part))
        before = early if before is None else link(before, early)
        after = late if after is None else link(after, late)
    plane = pack(link(link(before, chip), after))
    count = lax.axis_size("ep_0")
    planes = [
        lax.ppermute(plane, "ep_0", [(i, i + d) for i in range(count - d)])
        for d in range(count - 1, 0, -1)
    ]
    return before, planes


def arriving_state(low, before, planes):
    is_second = lax.axis_index("ep_2") == 1
    total = None
    for part in planes:
        total = pieces(part) if total is None else link(total, pieces(part))
    state = link(total, before)[1]
    swapped = both_cores(state)
    entering = jnp.concatenate(
        [jnp.where(is_second, swapped, state), jnp.where(is_second, state, swapped)], axis=0
    )
    first_core = pieces(low)
    return jnp.where(is_second, jnp.exp(first_core[0]) * entering + first_core[1], entering)


def hidden_kernel(own_ref, near_ref, go_ref, uo_ref, gf_ref, uf_ref, out_ref, gate, up):
    step = pl.program_id(0)

    @pl.when(step == 0)
    def _():
        gate[...] = jnp.zeros_like(gate)
        up[...] = jnp.zeros_like(up)

    rows = jnp.concatenate([own_ref[...], near_ref[...]], axis=0)
    n = go_ref.shape[1]
    gate[:, :n] += mm(rows, go_ref[...])
    gate[:, n:] += mm(rows, gf_ref[...])
    up[:, :n] += mm(rows, uo_ref[...])
    up[:, n:] += mm(rows, uf_ref[...])

    @pl.when(step == pl.num_programs(0) - 1)
    def _():
        gated = jnp.minimum(gate[...], CLAMP_LIMIT)
        opened = jnp.clip(up[...], -CLAMP_LIMIT, CLAMP_LIMIT)
        out_ref[...] = (
            (opened + 1.0) * gated * jax.nn.sigmoid(SWISH_SLOPE * gated)
        ).astype(BF16)


def hidden_units(own, near, half, weights):
    count = own.shape[0]
    width, n = weights[0].shape
    kb = 1024
    weight = pl.BlockSpec((kb, n), lambda i: (i, 0))
    return pl.pallas_call(
        hidden_kernel,
        grid=(width // kb,),
        in_specs=[
            pl.BlockSpec((count, kb), lambda i: (0, i + half * (width // kb))),
            pl.BlockSpec((count, kb), lambda i: (0, i)),
            weight,
            weight,
            weight,
            weight,
        ],
        out_specs=pl.BlockSpec((2 * count, 2 * n), lambda i: (0, 0)),
        out_shape=jax.ShapeDtypeStruct((2 * count, 2 * n), BF16),
        scratch_shapes=[pltpu.VMEM((2 * count, 2 * n), F32)] * 2,
        compiler_params=params(),
        name="hidden",
    )(own, near, *weights)


def down_kernel(src, h_own, h_near, h_far, h_opp, down_ref, out_ref):
    k = pl.program_id(0)
    n = down_ref.shape[0] // 4
    rows = out_ref.shape[0]
    unit = lambda s: down_ref[pl.ds(pl.multiple_of(s * n, n), n), :]
    for this, (mine, other, twin) in enumerate(
        ((h_own, h_near, 1), (h_near, h_own, 0), (h_far, h_opp, 3), (h_opp, h_far, 2))
    ):

        @pl.when(k == this)
        def _():
            s, t = src[this], src[twin]
            total = mm(mine[:rows, :n], unit(s)) + mm(mine[:rows, n:], unit(3 - s))
            total += mm(other[rows:, :n], unit(t)) + mm(other[rows:, n:], unit(3 - t))
            out_ref[...] = total.astype(BF16)


def down_rows(src, parts, down):
    both, width = parts[0].shape
    cols = down.shape[1]
    whole = lambda k, s: (0, 0)
    return pl.pallas_call(
        down_kernel,
        grid_spec=pltpu.PrefetchScalarGridSpec(
            num_scalar_prefetch=1,
            grid=(4,),
            in_specs=[pl.BlockSpec((both, width), whole)] * 4 + [pl.BlockSpec(down.shape, whole)],
            out_specs=pl.BlockSpec((both // 2, cols), lambda k, s: (0, s[k])),
        ),
        out_shape=jax.ShapeDtypeStruct((both // 2, 4 * cols), BF16),
        compiler_params=params(),
        name="down",
    )(src, *parts, down)


def places_kernel(src, routes_ref, logits_ref, out_ref):
    experts = logits_ref.shape[1]
    first, second, count, before = chosen(routes_ref[0], experts)
    logits = logits_ref[0].astype(F32)
    l0 = jnp.sum(jnp.where(first, logits, 0.0), axis=0, keepdims=True)
    l1 = jnp.sum(jnp.where(second, logits, 0.0), axis=0, keepdims=True)
    w0 = 1.0 / (1.0 + jnp.exp(l1 - l0))
    w1 = 1.0 / (1.0 + jnp.exp(l0 - l1))
    weight = jnp.where(first, w0, 0.0) + jnp.where(second, w1, 0.0)
    both = [slot_matrix(weight, before, count, half) for half in range(2)]
    place = jnp.concatenate(both, axis=0).T
    out_ref[0] = jnp.concatenate(halves(place), axis=0)


def places(src, routes, logits):
    experts, toks = logits.shape[1:]
    return pl.pallas_call(
        places_kernel,
        grid_spec=pltpu.PrefetchScalarGridSpec(
            num_scalar_prefetch=1,
            grid=(4,),
            in_specs=[
                pl.BlockSpec((1, 2, toks), lambda k, s: (s[k], 0, 0)),
                pl.BlockSpec((1, experts, toks), lambda k, s: (k, 0, 0)),
            ],
            out_specs=pl.BlockSpec((1, 2 * toks, experts * CAP), lambda k, s: (k, 0, 0)),
        ),
        out_shape=jax.ShapeDtypeStruct((4, 2 * toks, experts * CAP), BF16),
        compiler_params=params(),
        name="places",
    )(src, routes, logits)


def combine_kernel(src, low_ref, high_ref, place_ref, out_ref):
    slots = low_ref.shape[0]
    total = mm(place_ref[0, :, :slots], low_ref[...]) + mm(place_ref[0, :, slots:], high_ref[...])
    toks = out_ref.shape[0]
    out_ref[...] = (total[:toks] + total[toks:]).astype(BF16)


def combined(src, low, high, place):
    slots = low.shape[0]
    cols = low.shape[1] // 4
    toks = place.shape[1] // 2
    res = pl.BlockSpec((slots, cols), lambda k, s: (0, s[k]))
    return pl.pallas_call(
        combine_kernel,
        grid_spec=pltpu.PrefetchScalarGridSpec(
            num_scalar_prefetch=1,
            grid=(4,),
            in_specs=[
                res,
                res,
                pl.BlockSpec((1,) + place.shape[1:], lambda k, s: (k, 0, 0)),
            ],
            out_specs=pl.BlockSpec((toks, cols), lambda k, s: (s[k], 0)),
        ),
        out_shape=jax.ShapeDtypeStruct((4 * toks, cols), BF16),
        compiler_params=params(),
        name="combine",
    )(src, low, high, place)


NEAR = [(i, i ^ 1) for i in range(4)]
FAR = [(i, 3 - i) for i in range(4)]


def to_near(a):
    return lax.ppermute(a, "tp", NEAR)


def to_far(a):
    return lax.ppermute(a, "tp", FAR)


def shared(a):
    far = to_far(a)
    near = to_near(a)
    return a, near, far, to_near(far)


def swap(a):
    experts = 32
    rows, cols = a.shape
    out = lax.all_to_all(
        a.reshape(experts, rows // experts, cols), EP, split_axis=0, concat_axis=0, tiled=True
    )
    return out.reshape(rows, cols)


def per_device(
    mix_input,
    moe_input,
    norm_mix,
    query_weight,
    forget_weight,
    value_weight,
    forget_gap,
    norm_out,
    norm_moe,
    router_weight,
    expert_gate,
    expert_up,
    expert_down,
    routes,
):
    toks = moe_input.shape[0]
    x = lax.axis_index("tp").astype(jnp.int32)
    src = jnp.stack([x, x ^ 1, 3 - x, x ^ 2])
    by_block = routes.reshape(4, toks, 2).transpose(0, 2, 1)
    router = router_weight.T

    rows_a = normed(mix_input, norm_mix).astype(BF16)
    group_a = shared(rows_a)
    rows_b, own = front(src, moe_input, norm_moe.reshape(1, -1), by_block, router_weight.shape[1])
    own_rows = swap(own)
    rows_near = to_near(rows_b)
    gate_far = to_far(expert_gate[0])
    up_far = to_far(expert_up[0])
    logits, low, high = refill(src, rows_b, rows_near, router, by_block)
    low, own_rows = lax.optimization_barrier((low, own_rows))
    low_rows = swap(low)
    high, low_rows = lax.optimization_barrier((high, low_rows))
    high_rows = swap(high)
    logits = jnp.concatenate([logits, to_far(logits)])
    place = places(src, by_block, logits)

    inside, query, packed = mixer(
        src, group_a, query_weight, forget_weight, value_weight, forget_gap.reshape(1, -1)
    )
    first_core, chip, came = along_rows(packed)

    low_rows, packed = lax.optimization_barrier((low_rows, packed))
    weights = (expert_gate[0], expert_up[0], gate_far, up_far)
    h_low = hidden_units(own_rows, low_rows, 0, weights)
    h_low = shared(h_low)
    high_rows, far = lax.optimization_barrier((high_rows, h_low[2]))
    h_high = hidden_units(own_rows, high_rows, 1, weights)
    h_high = shared(h_high)
    opp, high_own = lax.optimization_barrier((h_low[3], h_high[0]))
    down_low = down_rows(src, h_low[:2] + (far, opp), expert_down[0])
    back_low = swap(down_low)
    came, _ = lax.optimization_barrier((came, down_low))
    before, planes = along_planes(chip, came)
    down_high = down_rows(src, (high_own,) + h_high[1:], expert_down[0])
    back_high = swap(down_high)
    planes, _ = lax.optimization_barrier((planes, down_high))

    state = arriving_state(first_core, before, planes)
    mixer_out = readout(inside, query, state, norm_out.reshape(1, -1))
    expert_out = combined(src, back_low, back_high, place)
    return (mixer_out, expert_out)


def solution(mesh):
    finer = Mesh(mesh.devices.reshape(4, 4, 2, mesh.shape["tp"]), ("ep_0", "ep_1", "ep_2", "tp"))
    placed = (
        P(EP_TP, None),
        P(EP_TP, None),
        P(),
        P(None, "tp"),
        P(None, "tp"),
        P(None, "tp"),
        P("tp"),
        P("tp"),
        P(),
        P(),
        P(EP, None, "tp"),
        P(EP, None, "tp"),
        P(EP, None, "tp"),
        P(EP, None),
    )

    return jax.shard_map(
        per_device,
        mesh=finer,
        in_specs=placed,
        out_specs=(P(EP, "tp"), P(EP, "tp")),
        check_vma=False,
    )
```

```python
import functools

import jax
import jax.numpy as jnp
from jax import lax
from jax.experimental import pallas as pl
from jax.experimental.pallas import tpu as pltpu
from jax.sharding import Mesh
from jax.sharding import PartitionSpec as P

HEAD_DIM = 128

CAP = 16
HALF = 8
EP = ("ep_0", "ep_1", "ep_2")
EP_TP = ("ep_0", "ep_1", "ep_2", "tp")

EPSILON = 1e-06
CLAMP_LIMIT = 7.0
SWISH_SLOPE = 1.702
F32 = jnp.float32
BF16 = jnp.bfloat16


def mm(a, b, contract=((1,), (0,))):
    return lax.dot_general(a, b, (contract, ((), ())), preferred_element_type=F32)


def halves(a):
    high = a.astype(BF16)
    return high, (a - high.astype(F32)).astype(BF16)


def params(mib=56, axes=("arbitrary",)):
    return pltpu.CompilerParams(vmem_limit_bytes=mib << 20, dimension_semantics=axes)


def normed(row_data, gain_vec):
    as_float = row_data.astype(F32)
    scale = lax.rsqrt(jnp.mean(as_float * as_float, axis=-1, keepdims=True) + EPSILON)
    return as_float * scale * gain_vec


def chosen(routes, experts):
    toks = routes.shape[1]
    ids = lax.broadcasted_iota(jnp.int32, (experts, toks), 0)
    first = routes[0:1, :] == ids
    second = routes[1:2, :] == ids
    count = jnp.where(first | second, 1.0, 0.0)
    earlier = (
        lax.broadcasted_iota(jnp.int32, (toks, toks), 0)
        < lax.broadcasted_iota(jnp.int32, (toks, toks), 1)
    )
    before = mm(count.astype(BF16), jnp.where(earlier, 1.0, 0.0).astype(BF16))
    return first, second, count, before


def slot_matrix(weight, before, count, half):
    experts, toks = weight.shape
    place = lax.broadcasted_iota(jnp.int32, (experts, HALF, toks), 1) + half * HALF
    here = (before[:, None, :] == place.astype(F32)) & (count[:, None, :] > 0.5)
    return jnp.where(here, weight[:, None, :], 0.0).reshape(experts * HALF, toks)


def fill(routes, rows, experts):
    _, _, count, before = chosen(routes, experts)
    pick = [slot_matrix(count, before, count, half) for half in range(2)]
    both = mm(jnp.concatenate(pick, axis=0).astype(BF16), rows).astype(BF16)
    return both[: experts * HALF], both[experts * HALF :]


def front_kernel(src, x_ref, gain_ref, routes_ref, rows_ref, buf_ref, *, group):
    step = pl.program_id(0)
    width = x_ref.shape[1]

    @pl.when(step == 0)
    def _():
        rows_ref[...] = normed(x_ref[...], gain_ref[...]).astype(BF16)

    low, high = fill(routes_ref[0] - step * group, rows_ref[...], group)
    buf_ref[:, :width] = low
    buf_ref[:, width:] = high


def refill_kernel(src, own_ref, rows_ref, router_ref, routes_ref, logits_ref, low_ref, high_ref, *, group):
    step = pl.program_id(0)

    @pl.when(step == 0)
    def _():
        for k, ref in enumerate((own_ref, rows_ref)):
            logits_ref[k] = mm(router_ref[...], ref[...], ((1,), (1,))).astype(BF16)

    low_ref[...], high_ref[...] = fill(routes_ref[0] - step * group, rows_ref[...], group)


def front(src, x, gain, routes, experts):
    toks, width = x.shape
    group = 16
    whole = lambda i, s: (0, 0)
    return pl.pallas_call(
        functools.partial(front_kernel, group=group),
        grid_spec=pltpu.PrefetchScalarGridSpec(
            num_scalar_prefetch=1,
            grid=(experts // group,),
            in_specs=[
                pl.BlockSpec((toks, width), whole),
                pl.BlockSpec((1, width), whole),
                pl.BlockSpec((1, 2, toks), lambda i, s: (s[0], 0, 0)),
            ],
            out_specs=[
                pl.BlockSpec((toks, width), whole),
                pl.BlockSpec((group * HALF, 2 * width), lambda i, s: (i, 0)),
            ],
        ),
        out_shape=[
            jax.ShapeDtypeStruct((toks, width), BF16),
            jax.ShapeDtypeStruct((experts * HALF, 2 * width), BF16),
        ],
        compiler_params=params(),
        name="front",
    )(src, x, gain, routes)


def refill(src, own, rows, router, routes):
    toks, width = rows.shape
    experts = router.shape[0]
    group = 16
    whole = lambda i, s: (0, 0)
    return pl.pallas_call(
        functools.partial(refill_kernel, group=group),
        grid_spec=pltpu.PrefetchScalarGridSpec(
            num_scalar_prefetch=1,
            grid=(experts // group,),
            in_specs=[
                pl.BlockSpec((toks, width), whole),
                pl.BlockSpec((toks, width), whole),
                pl.BlockSpec(router.shape, whole),
                pl.BlockSpec((1, 2, toks), lambda i, s: (s[1], 0, 0)),
            ],
            out_specs=[
                pl.BlockSpec((2, experts, toks), lambda i, s: (0, 0, 0)),
                pl.BlockSpec((group * HALF, width), lambda i, s: (i, 0)),
                pl.BlockSpec((group * HALF, width), lambda i, s: (i, 0)),
            ],
        ),
        out_shape=[
            jax.ShapeDtypeStruct((2, experts, toks), BF16),
            jax.ShapeDtypeStruct((experts * HALF, width), BF16),
            jax.ShapeDtypeStruct((experts * HALF, width), BF16),
        ],
        compiler_params=params(),
        name="refill",
    )(src, own, rows, router, routes)


def mixer_kernel(
    src, a0, a1, a2, a3, q_ref, f_ref, v_ref, gap_ref, inside_ref, query_ref, packed_ref, qa, fa, va, group
):
    step = pl.program_id(0)

    @pl.when(step == 0)
    def _():
        qa[...] = jnp.zeros_like(qa)
        fa[...] = jnp.zeros_like(fa)
        va[...] = jnp.zeros_like(va)

    toks = a0.shape[0]
    for k, part in enumerate((a0, a1, a2, a3)):
        group[pl.ds(pl.multiple_of(src[k] * toks, toks), toks), :] = part[...]
    a = group[...]
    qa[...] += mm(a, q_ref[...])
    fa[...] += mm(a, f_ref[...])
    va[...] += mm(a, v_ref[...])

    @pl.when(step == pl.num_programs(0) - 1)
    def _():
        rows = a.shape[0]
        causal = (
            lax.broadcasted_iota(jnp.int32, (rows, rows), 0)
            >= lax.broadcasted_iota(jnp.int32, (rows, rows), 1)
        )
        ones = jnp.where(causal[:toks, :toks], 1.0, 0.0).astype(BF16)
        shut = gap_ref[...] * jax.nn.sigmoid(-fa[...])
        fa[...] = jnp.log1p(-shut)
        cols = shut.shape[1]
        base = None
        for k in range(rows // toks):
            part = fa[k * toks : (k + 1) * toks, :]
            high = part.astype(BF16)
            rest = part - high.astype(F32)
            mid = rest.astype(BF16)
            low = (rest - mid.astype(F32)).astype(BF16)
            sums = mm(ones, jnp.concatenate([high, mid, low], axis=1))
            sums = sums[:, :cols] + sums[:, cols : 2 * cols] + sums[:, 2 * cols :]
            sums = sums if base is None else sums + base
            base = sums[toks - 1 :, :]
            fa[k * toks : (k + 1) * toks, :] = sums
        sums = fa[...]
        last = sums[rows - 1 :, :]
        query_ref[...] = qa[...] * jnp.exp(sums)
        keys = shut * jnp.exp(-sums)
        late = shut * jnp.exp(last - sums)
        half = rows // 2
        for h in range(packed_ref.shape[0]):
            at = slice(h * HEAD_DIM, (h + 1) * HEAD_DIM)
            q_high, q_low = halves(query_ref[:, at])
            k_high, k_low = halves(keys[:, at])
            v_high, v_low = halves(va[:, at])
            l_high, l_low = halves(late[:, at])
            left = jnp.concatenate([q_high, q_low, q_high], axis=1)
            right = jnp.concatenate([k_high, k_high, k_low], axis=1)
            values = jnp.concatenate([v_high, v_low], axis=1)
            for k in range(2):
                end = (k + 1) * half
                scores = mm(left[end - half : end], right[:end], ((1,), (1,)))
                s_high, s_low = halves(jnp.where(causal[end - half : end, :end], scores, 0.0))
                part = mm(s_high, values[:end])
                part = part[:, :HEAD_DIM] + part[:, HEAD_DIM:] + mm(s_low, v_high[:end])
                inside_ref[end - half : end, at] = part
            outer = mm(values, jnp.concatenate([l_high, l_low], axis=1), ((0,), (0,)))
            packed_ref[h, :HEAD_DIM, :] = (
                outer[:HEAD_DIM, :HEAD_DIM]
                + outer[:HEAD_DIM, HEAD_DIM:]
                + outer[HEAD_DIM:, :HEAD_DIM]
            )
            packed_ref[h, HEAD_DIM:, :] = jnp.broadcast_to(last[:, at], (8, HEAD_DIM))


def mixer(src, parts, wq, wf, wv, gap):
    toks, width = parts[0].shape
    rows = 4 * toks
    cols = wq.shape[1]
    heads = cols // HEAD_DIM
    kb = 512
    fixed = lambda i, s: (0, 0)
    weight = pl.BlockSpec((kb, cols), lambda i, s: (i, 0))
    return pl.pallas_call(
        mixer_kernel,
        grid_spec=pltpu.PrefetchScalarGridSpec(
            num_scalar_prefetch=1,
            grid=(width // kb,),
            in_specs=[pl.BlockSpec((toks, kb), lambda i, s: (0, i))] * 4
            + [weight, weight, weight, pl.BlockSpec((1, cols), fixed)],
            out_specs=[
                pl.BlockSpec((rows, cols), fixed),
                pl.BlockSpec((rows, cols), fixed),
                pl.BlockSpec((heads, HEAD_DIM + 8, HEAD_DIM), lambda i, s: (0, 0, 0)),
            ],
            scratch_shapes=[pltpu.VMEM((rows, cols), F32)] * 3 + [pltpu.VMEM((rows, kb), BF16)],
        ),
        out_shape=[
            jax.ShapeDtypeStruct((rows, cols), F32),
            jax.ShapeDtypeStruct((rows, cols), F32),
            jax.ShapeDtypeStruct((heads, HEAD_DIM + 8, HEAD_DIM), F32),
        ],
        compiler_params=params(),
        name="mixer",
    )(src, *parts, wq, wf, wv, gap)


def readout_kernel(inside_ref, query_ref, state_ref, gain_ref, out_ref):
    q_high, q_low = halves(query_ref[...])
    s_high, s_low = halves(state_ref[0])
    total = inside_ref[...] + mm(
        jnp.concatenate([q_high, q_low, q_high], axis=1),
        jnp.concatenate([s_high, s_high, s_low], axis=1),
        ((1,), (1,)),
    )
    out_ref[...] = normed(total, gain_ref[...]).astype(BF16)


def readout(inside, query, state, gain):
    rows, cols = inside.shape
    block = pl.BlockSpec((rows, HEAD_DIM), lambda h: (0, h))
    return pl.pallas_call(
        readout_kernel,
        grid=(cols // HEAD_DIM,),
        in_specs=[
            block,
            block,
            pl.BlockSpec((1, HEAD_DIM, HEAD_DIM), lambda h: (h, 0, 0)),
            pl.BlockSpec((1, HEAD_DIM), lambda h: (0, h)),
        ],
        out_specs=block,
        out_shape=jax.ShapeDtypeStruct((rows, cols), BF16),
        compiler_params=params(),
        name="readout",
    )(inside, query, state, gain)


def pieces(packed):
    return packed[:, HEAD_DIM : HEAD_DIM + 1, :], packed[:, :HEAD_DIM, :]


def link(earlier, later):
    return earlier[0] + later[0], jnp.exp(later[0]) * earlier[1] + later[1]


def pack(part):
    heads = part[1].shape[0]
    return jnp.concatenate(
        [part[1], jnp.broadcast_to(part[0], (heads, 8, HEAD_DIM))], axis=1
    )


def masked(flag, part):
    return jax.tree.map(lambda a: jnp.where(flag, a, 0.0), part)


def both_cores(a):
    return lax.ppermute(a, "ep_2", [(0, 1), (1, 0)])


def along_rows(packed):
    core = lax.axis_index("ep_2")
    other = both_cores(packed)
    is_second = core == 1
    low = jnp.where(is_second, other, packed)
    high = jnp.where(is_second, packed, other)
    half = packed.shape[0] // 2
    mine = lambda a: lax.dynamic_slice_in_dim(a, core * half, half, 0)
    chip = link(pieces(mine(low)), pieces(mine(high)))
    count = lax.axis_size("ep_1")
    sent = pack(chip)
    came = [
        lax.ppermute(sent, "ep_1", [(i, (i + d) % count) for i in range(count)])
        for d in range(count - 1, 0, -1)
    ]
    return low, chip, came


def along_planes(chip, came):
    row = lax.axis_index("ep_1")
    before = after = None
    for k, part in enumerate(came):
        d = len(came) - k
        early = masked(row >= d, pieces(part))
        late = masked(row < d, pieces(part))
        before = early if before is None else link(before, early)
        after = late if after is None else link(after, late)
    plane = pack(link(link(before, chip), after))
    count = lax.axis_size("ep_0")
    planes = [
        lax.ppermute(plane, "ep_0", [(i, i + d) for i in range(count - d)])
        for d in range(count - 1, 0, -1)
    ]
    return before, planes


def arriving_state(low, before, planes):
    is_second = lax.axis_index("ep_2") == 1
    total = None
    for part in planes:
        total = pieces(part) if total is None else link(total, pieces(part))
    state = link(total, before)[1]
    swapped = both_cores(state)
    entering = jnp.concatenate(
        [jnp.where(is_second, swapped, state), jnp.where(is_second, state, swapped)], axis=0
    )
    first_core = pieces(low)
    return jnp.where(is_second, jnp.exp(first_core[0]) * entering + first_core[1], entering)


def hidden_kernel(own_ref, near_ref, go_ref, uo_ref, gf_ref, uf_ref, out_ref, gate, up):
    step = pl.program_id(0)

    @pl.when(step == 0)
    def _():
        gate[...] = jnp.zeros_like(gate)
        up[...] = jnp.zeros_like(up)

    rows = jnp.concatenate([own_ref[...], near_ref[...]], axis=0)
    n = go_ref.shape[1]
    gate[:, :n] += mm(rows, go_ref[...])
    gate[:, n:] += mm(rows, gf_ref[...])
    up[:, :n] += mm(rows, uo_ref[...])
    up[:, n:] += mm(rows, uf_ref[...])

    @pl.when(step == pl.num_programs(0) - 1)
    def _():
        gated = jnp.minimum(gate[...], CLAMP_LIMIT)
        opened = jnp.clip(up[...], -CLAMP_LIMIT, CLAMP_LIMIT)
        out_ref[...] = (
            (opened + 1.0) * gated * jax.nn.sigmoid(SWISH_SLOPE * gated)
        ).astype(BF16)


def hidden_units(own, near, half, weights):
    count = own.shape[0]
    width, n = weights[0].shape
    kb = 1024
    weight = pl.BlockSpec((kb, n), lambda i: (i, 0))
    return pl.pallas_call(
        hidden_kernel,
        grid=(width // kb,),
        in_specs=[
            pl.BlockSpec((count, kb), lambda i: (0, i + half * (width // kb))),
            pl.BlockSpec((count, kb), lambda i: (0, i)),
            weight,
            weight,
            weight,
            weight,
        ],
        out_specs=pl.BlockSpec((2 * count, 2 * n), lambda i: (0, 0)),
        out_shape=jax.ShapeDtypeStruct((2 * count, 2 * n), BF16),
        scratch_shapes=[pltpu.VMEM((2 * count, 2 * n), F32)] * 2,
        compiler_params=params(),
        name="hidden",
    )(own, near, *weights)


def down_kernel(src, this, twin, down_ref, out_ref, *, first):
    k = pl.program_id(0)
    n = down_ref.shape[0] // 4
    rows = out_ref.shape[0]
    unit = lambda s: down_ref[pl.ds(pl.multiple_of(s * n, n), n), :]
    for step, (mine, other) in enumerate(((this, twin), (twin, this))):

        @pl.when(k == step)
        def _():
            s, t = src[first + step], src[first + 1 - step]
            total = mm(mine[:rows, :n], unit(s)) + mm(mine[:rows, n:], unit(3 - s))
            total += mm(other[rows:, :n], unit(t)) + mm(other[rows:, n:], unit(3 - t))
            out_ref[...] = total.astype(BF16)


def down_rows(src, this, twin, first, down):
    both, width = this.shape
    cols = down.shape[1]
    whole = lambda k, s: (0, 0)
    return pl.pallas_call(
        functools.partial(down_kernel, first=first),
        grid_spec=pltpu.PrefetchScalarGridSpec(
            num_scalar_prefetch=1,
            grid=(2,),
            in_specs=[pl.BlockSpec((both, width), whole)] * 2 + [pl.BlockSpec(down.shape, whole)],
            out_specs=pl.BlockSpec((both // 2, cols), lambda k, s: (0, k)),
        ),
        out_shape=jax.ShapeDtypeStruct((both // 2, 2 * cols), BF16),
        compiler_params=params(),
        name="down",
    )(src, this, twin, down)


def down4_kernel(src, h_own, h_near, h_far, h_opp, down_ref, out_ref):
    k = pl.program_id(0)
    n = down_ref.shape[0] // 4
    rows = out_ref.shape[0]
    unit = lambda s: down_ref[pl.ds(pl.multiple_of(s * n, n), n), :]
    for this, (mine, other, twin) in enumerate(
        ((h_own, h_near, 1), (h_near, h_own, 0), (h_far, h_opp, 3), (h_opp, h_far, 2))
    ):

        @pl.when(k == this)
        def _():
            s, t = src[this], src[twin]
            total = mm(mine[:rows, :n], unit(s)) + mm(mine[:rows, n:], unit(3 - s))
            total += mm(other[rows:, :n], unit(t)) + mm(other[rows:, n:], unit(3 - t))
            out_ref[...] = total.astype(BF16)


def down_rows4(src, parts, down):
    both, width = parts[0].shape
    cols = down.shape[1]
    whole = lambda k, s: (0, 0)
    return pl.pallas_call(
        down4_kernel,
        grid_spec=pltpu.PrefetchScalarGridSpec(
            num_scalar_prefetch=1,
            grid=(4,),
            in_specs=[pl.BlockSpec((both, width), whole)] * 4 + [pl.BlockSpec(down.shape, whole)],
            out_specs=pl.BlockSpec((both // 2, cols), lambda k, s: (0, k)),
        ),
        out_shape=jax.ShapeDtypeStruct((both // 2, 4 * cols), BF16),
        compiler_params=params(),
        name="down4",
    )(src, *parts, down)


def places_kernel(src, routes_ref, logits_ref, out_ref):
    experts = logits_ref.shape[1]
    first, second, count, before = chosen(routes_ref[0], experts)
    logits = logits_ref[0].astype(F32)
    l0 = jnp.sum(jnp.where(first, logits, 0.0), axis=0, keepdims=True)
    l1 = jnp.sum(jnp.where(second, logits, 0.0), axis=0, keepdims=True)
    w0 = 1.0 / (1.0 + jnp.exp(l1 - l0))
    w1 = 1.0 / (1.0 + jnp.exp(l0 - l1))
    weight = jnp.where(first, w0, 0.0) + jnp.where(second, w1, 0.0)
    both = [slot_matrix(weight, before, count, half) for half in range(2)]
    place = jnp.concatenate(both, axis=0).T
    out_ref[0] = jnp.concatenate(halves(place), axis=0)


def places(src, routes, logits):
    experts, toks = logits.shape[1:]
    return pl.pallas_call(
        places_kernel,
        grid_spec=pltpu.PrefetchScalarGridSpec(
            num_scalar_prefetch=1,
            grid=(4,),
            in_specs=[
                pl.BlockSpec((1, 2, toks), lambda k, s: (s[k], 0, 0)),
                pl.BlockSpec((1, experts, toks), lambda k, s: (k, 0, 0)),
            ],
            out_specs=pl.BlockSpec((1, 2 * toks, experts * CAP), lambda k, s: (k, 0, 0)),
        ),
        out_shape=jax.ShapeDtypeStruct((4, 2 * toks, experts * CAP), BF16),
        compiler_params=params(),
        name="places",
    )(src, routes, logits)


def combine_kernel(src, first_ref, second_ref, high_ref, place_ref, out_ref):
    k = pl.program_id(0)
    slots = high_ref.shape[0]
    toks = out_ref.shape[0]
    for pair, low_ref in enumerate((first_ref, second_ref)):

        @pl.when(k // 2 == pair)
        def _():
            total = mm(place_ref[0, :, :slots], low_ref[...])
            total += mm(place_ref[0, :, slots:], high_ref[...])
            out_ref[...] = (total[:toks] + total[toks:]).astype(BF16)


def combined(src, first, second, high, place):
    slots = high.shape[0]
    cols = high.shape[1] // 4
    toks = place.shape[1] // 2
    return pl.pallas_call(
        combine_kernel,
        grid_spec=pltpu.PrefetchScalarGridSpec(
            num_scalar_prefetch=1,
            grid=(4,),
            in_specs=[
                pl.BlockSpec((slots, cols), lambda k, s: (0, jnp.minimum(k, 1))),
                pl.BlockSpec((slots, cols), lambda k, s: (0, jnp.maximum(k - 2, 0))),
                pl.BlockSpec((slots, cols), lambda k, s: (0, k)),
                pl.BlockSpec((1,) + place.shape[1:], lambda k, s: (k, 0, 0)),
            ],
            out_specs=pl.BlockSpec((toks, cols), lambda k, s: (s[k], 0)),
        ),
        out_shape=jax.ShapeDtypeStruct((4 * toks, cols), BF16),
        compiler_params=params(),
        name="combine",
    )(src, first, second, high, place)


NEAR = [(i, i ^ 1) for i in range(4)]
FAR = [(i, 3 - i) for i in range(4)]


def to_near(a):
    return lax.ppermute(a, "tp", NEAR)


def to_far(a):
    return lax.ppermute(a, "tp", FAR)


def shared(a):
    far = to_far(a)
    near = to_near(a)
    return a, near, far, to_near(far)


def swap(a):
    experts = 32
    rows, cols = a.shape
    out = lax.all_to_all(
        a.reshape(experts, rows // experts, cols), EP, split_axis=0, concat_axis=0, tiled=True
    )
    return out.reshape(rows, cols)


def per_device(
    mix_input,
    moe_input,
    norm_mix,
    query_weight,
    forget_weight,
    value_weight,
    forget_gap,
    norm_out,
    norm_moe,
    router_weight,
    expert_gate,
    expert_up,
    expert_down,
    routes,
):
    toks = moe_input.shape[0]
    x = lax.axis_index("tp").astype(jnp.int32)
    src = jnp.stack([x, x ^ 1, 3 - x, x ^ 2])
    by_block = routes.reshape(4, toks, 2).transpose(0, 2, 1)
    router = router_weight.T

    rows_a = normed(mix_input, norm_mix).astype(BF16)
    group_a = shared(rows_a)
    rows_b, own = front(src, moe_input, norm_moe.reshape(1, -1), by_block, router_weight.shape[1])
    own_rows = swap(own)
    rows_near = to_near(rows_b)
    gate_far = to_far(expert_gate[0])
    up_far = to_far(expert_up[0])
    logits, low, high = refill(src, rows_b, rows_near, router, by_block)
    low, own_rows = lax.optimization_barrier((low, own_rows))
    low_rows = swap(low)
    high, low_rows = lax.optimization_barrier((high, low_rows))
    high_rows = swap(high)
    logits = jnp.concatenate([logits, to_far(logits)])
    place = places(src, by_block, logits)

    inside, query, packed = mixer(
        src, group_a, query_weight, forget_weight, value_weight, forget_gap.reshape(1, -1)
    )
    first_core, chip, came = along_rows(packed)

    low_rows, packed = lax.optimization_barrier((low_rows, packed))
    weights = (expert_gate[0], expert_up[0], gate_far, up_far)
    h_low = hidden_units(own_rows, low_rows, 0, weights)
    h_low = shared(h_low)
    came, _ = lax.optimization_barrier((came, h_low[0]))
    before, planes = along_planes(chip, came)
    down_first = down_rows(src, h_low[0], h_low[1], 0, expert_down[0])
    back_first = swap(down_first)
    high_rows, far = lax.optimization_barrier((high_rows, h_low[2]))
    h_high = hidden_units(own_rows, high_rows, 1, weights)
    h_high = shared(h_high)
    down_second = down_rows(src, far, h_low[3], 2, expert_down[0])
    down_second, back_first = lax.optimization_barrier((down_second, back_first))
    back_second = swap(down_second)
    down_high = down_rows4(src, h_high, expert_down[0])
    down_high, back_second = lax.optimization_barrier((down_high, back_second))
    back_high = swap(down_high)
    planes, _ = lax.optimization_barrier((planes, down_high))

    state = arriving_state(first_core, before, planes)
    mixer_out = readout(inside, query, state, norm_out.reshape(1, -1))
    expert_out = combined(src, back_first, back_second, back_high, place)
    return (mixer_out, expert_out)


def solution(mesh):
    finer = Mesh(mesh.devices.reshape(4, 4, 2, mesh.shape["tp"]), ("ep_0", "ep_1", "ep_2", "tp"))
    placed = (
        P(EP_TP, None),
        P(EP_TP, None),
        P(),
        P(None, "tp"),
        P(None, "tp"),
        P(None, "tp"),
        P("tp"),
        P("tp"),
        P(),
        P(),
        P(EP, None, "tp"),
        P(EP, None, "tp"),
        P(EP, None, "tp"),
        P(EP, None),
    )

    return jax.shard_map(
        per_device,
        mesh=finer,
        in_specs=placed,
        out_specs=(P(EP, "tp"), P(EP, "tp")),
        check_vma=False,
    )
```

```python
import functools

import jax
import jax.numpy as jnp
from jax import lax
from jax.experimental import pallas as pl
from jax.experimental.pallas import tpu as pltpu
from jax.sharding import Mesh
from jax.sharding import PartitionSpec as P

HEAD_DIM = 128

CAP = 16
HALF = 8
EP = ("ep_0", "ep_1", "ep_2")
EP_TP = ("ep_0", "ep_1", "ep_2", "tp")

EPSILON = 1e-06
CLAMP_LIMIT = 7.0
SWISH_SLOPE = 1.702
F32 = jnp.float32
BF16 = jnp.bfloat16


def mm(a, b, contract=((1,), (0,))):
    return lax.dot_general(a, b, (contract, ((), ())), preferred_element_type=F32)


def halves(a):
    high = a.astype(BF16)
    return high, (a - high.astype(F32)).astype(BF16)


def params(mib=56, axes=("arbitrary",)):
    return pltpu.CompilerParams(vmem_limit_bytes=mib << 20, dimension_semantics=axes)


def normed(row_data, gain_vec):
    as_float = row_data.astype(F32)
    scale = lax.rsqrt(jnp.mean(as_float * as_float, axis=-1, keepdims=True) + EPSILON)
    return as_float * scale * gain_vec


def chosen(routes, experts):
    toks = routes.shape[1]
    ids = lax.broadcasted_iota(jnp.int32, (experts, toks), 0)
    first = routes[0:1, :] == ids
    second = routes[1:2, :] == ids
    count = jnp.where(first | second, 1.0, 0.0)
    earlier = (
        lax.broadcasted_iota(jnp.int32, (toks, toks), 0)
        < lax.broadcasted_iota(jnp.int32, (toks, toks), 1)
    )
    before = mm(count.astype(BF16), jnp.where(earlier, 1.0, 0.0).astype(BF16))
    return first, second, count, before


def slot_matrix(weight, before, count, half):
    experts, toks = weight.shape
    place = lax.broadcasted_iota(jnp.int32, (experts, HALF, toks), 1) + half * HALF
    here = (before[:, None, :] == place.astype(F32)) & (count[:, None, :] > 0.5)
    return jnp.where(here, weight[:, None, :], 0.0).reshape(experts * HALF, toks)


def fill(routes, rows, experts):
    _, _, count, before = chosen(routes, experts)
    pick = [slot_matrix(count, before, count, half) for half in range(2)]
    both = mm(jnp.concatenate(pick, axis=0).astype(BF16), rows).astype(BF16)
    return both[: experts * HALF], both[experts * HALF :]


def front_kernel(src, x_ref, gain_ref, routes_ref, rows_ref, buf_ref, *, group):
    step = pl.program_id(0)
    width = x_ref.shape[1]

    @pl.when(step == 0)
    def _():
        rows_ref[...] = normed(x_ref[...], gain_ref[...]).astype(BF16)

    low, high = fill(routes_ref[0] - step * group, rows_ref[...], group)
    buf_ref[:, :width] = low
    buf_ref[:, width:] = high


def refill_kernel(src, own_ref, rows_ref, router_ref, routes_ref, logits_ref, low_ref, high_ref, *, group):
    step = pl.program_id(0)

    @pl.when(step == 0)
    def _():
        for k, ref in enumerate((own_ref, rows_ref)):
            logits_ref[k] = mm(router_ref[...], ref[...], ((1,), (1,))).astype(BF16)

    low_ref[...], high_ref[...] = fill(routes_ref[0] - step * group, rows_ref[...], group)


def front(src, x, gain, routes, experts):
    toks, width = x.shape
    group = 16
    whole = lambda i, s: (0, 0)
    return pl.pallas_call(
        functools.partial(front_kernel, group=group),
        grid_spec=pltpu.PrefetchScalarGridSpec(
            num_scalar_prefetch=1,
            grid=(experts // group,),
            in_specs=[
                pl.BlockSpec((toks, width), whole),
                pl.BlockSpec((1, width), whole),
                pl.BlockSpec((1, 2, toks), lambda i, s: (s[0], 0, 0)),
            ],
            out_specs=[
                pl.BlockSpec((toks, width), whole),
                pl.BlockSpec((group * HALF, 2 * width), lambda i, s: (i, 0)),
            ],
        ),
        out_shape=[
            jax.ShapeDtypeStruct((toks, width), BF16),
            jax.ShapeDtypeStruct((experts * HALF, 2 * width), BF16),
        ],
        compiler_params=params(),
        name="front",
    )(src, x, gain, routes)


def refill(src, own, rows, router, routes):
    toks, width = rows.shape
    experts = router.shape[0]
    group = 16
    whole = lambda i, s: (0, 0)
    return pl.pallas_call(
        functools.partial(refill_kernel, group=group),
        grid_spec=pltpu.PrefetchScalarGridSpec(
            num_scalar_prefetch=1,
            grid=(experts // group,),
            in_specs=[
                pl.BlockSpec((toks, width), whole),
                pl.BlockSpec((toks, width), whole),
                pl.BlockSpec(router.shape, whole),
                pl.BlockSpec((1, 2, toks), lambda i, s: (s[1], 0, 0)),
            ],
            out_specs=[
                pl.BlockSpec((2, experts, toks), lambda i, s: (0, 0, 0)),
                pl.BlockSpec((group * HALF, width), lambda i, s: (i, 0)),
                pl.BlockSpec((group * HALF, width), lambda i, s: (i, 0)),
            ],
        ),
        out_shape=[
            jax.ShapeDtypeStruct((2, experts, toks), BF16),
            jax.ShapeDtypeStruct((experts * HALF, width), BF16),
            jax.ShapeDtypeStruct((experts * HALF, width), BF16),
        ],
        compiler_params=params(),
        name="refill",
    )(src, own, rows, router, routes)


def mixer_kernel(
    src, a0, a1, a2, a3, q_ref, f_ref, v_ref, gap_ref, inside_ref, query_ref, packed_ref, qa, fa, va, group
):
    step = pl.program_id(0)

    @pl.when(step == 0)
    def _():
        qa[...] = jnp.zeros_like(qa)
        fa[...] = jnp.zeros_like(fa)
        va[...] = jnp.zeros_like(va)

    toks = a0.shape[0]
    for k, part in enumerate((a0, a1, a2, a3)):
        group[pl.ds(pl.multiple_of(src[k] * toks, toks), toks), :] = part[...]
    a = group[...]
    qa[...] += mm(a, q_ref[...])
    fa[...] += mm(a, f_ref[...])
    va[...] += mm(a, v_ref[...])

    @pl.when(step == pl.num_programs(0) - 1)
    def _():
        rows = a.shape[0]
        causal = (
            lax.broadcasted_iota(jnp.int32, (rows, rows), 0)
            >= lax.broadcasted_iota(jnp.int32, (rows, rows), 1)
        )
        ones = jnp.where(causal[:toks, :toks], 1.0, 0.0).astype(BF16)
        shut = gap_ref[...] * jax.nn.sigmoid(-fa[...])
        fa[...] = jnp.log1p(-shut)
        cols = shut.shape[1]
        base = None
        for k in range(rows // toks):
            part = fa[k * toks : (k + 1) * toks, :]
            high = part.astype(BF16)
            rest = part - high.astype(F32)
            mid = rest.astype(BF16)
            low = (rest - mid.astype(F32)).astype(BF16)
            sums = mm(ones, jnp.concatenate([high, mid, low], axis=1))
            sums = sums[:, :cols] + sums[:, cols : 2 * cols] + sums[:, 2 * cols :]
            sums = sums if base is None else sums + base
            base = sums[toks - 1 :, :]
            fa[k * toks : (k + 1) * toks, :] = sums
        sums = fa[...]
        last = sums[rows - 1 :, :]
        query_ref[...] = qa[...] * jnp.exp(sums)
        keys = shut * jnp.exp(-sums)
        late = shut * jnp.exp(last - sums)
        half = rows // 2
        for h in range(packed_ref.shape[0]):
            at = slice(h * HEAD_DIM, (h + 1) * HEAD_DIM)
            q_high, q_low = halves(query_ref[:, at])
            k_high, k_low = halves(keys[:, at])
            v_high, v_low = halves(va[:, at])
            l_high, l_low = halves(late[:, at])
            left = jnp.concatenate([q_high, q_low, q_high], axis=1)
            right = jnp.concatenate([k_high, k_high, k_low], axis=1)
            values = jnp.concatenate([v_high, v_low], axis=1)
            for k in range(2):
                end = (k + 1) * half
                scores = mm(left[end - half : end], right[:end], ((1,), (1,)))
                s_high, s_low = halves(jnp.where(causal[end - half : end, :end], scores, 0.0))
                part = mm(s_high, values[:end])
                part = part[:, :HEAD_DIM] + part[:, HEAD_DIM:] + mm(s_low, v_high[:end])
                inside_ref[end - half : end, at] = part
            outer = mm(values, jnp.concatenate([l_high, l_low], axis=1), ((0,), (0,)))
            packed_ref[h, :HEAD_DIM, :] = (
                outer[:HEAD_DIM, :HEAD_DIM]
                + outer[:HEAD_DIM, HEAD_DIM:]
                + outer[HEAD_DIM:, :HEAD_DIM]
            )
            packed_ref[h, HEAD_DIM:, :] = jnp.broadcast_to(last[:, at], (8, HEAD_DIM))


def mixer(src, parts, wq, wf, wv, gap):
    toks, width = parts[0].shape
    rows = 4 * toks
    cols = wq.shape[1]
    heads = cols // HEAD_DIM
    kb = 512
    fixed = lambda i, s: (0, 0)
    weight = pl.BlockSpec((kb, cols), lambda i, s: (i, 0))
    return pl.pallas_call(
        mixer_kernel,
        grid_spec=pltpu.PrefetchScalarGridSpec(
            num_scalar_prefetch=1,
            grid=(width // kb,),
            in_specs=[pl.BlockSpec((toks, kb), lambda i, s: (0, i))] * 4
            + [weight, weight, weight, pl.BlockSpec((1, cols), fixed)],
            out_specs=[
                pl.BlockSpec((rows, cols), fixed),
                pl.BlockSpec((rows, cols), fixed),
                pl.BlockSpec((heads, HEAD_DIM + 8, HEAD_DIM), lambda i, s: (0, 0, 0)),
            ],
            scratch_shapes=[pltpu.VMEM((rows, cols), F32)] * 3 + [pltpu.VMEM((rows, kb), BF16)],
        ),
        out_shape=[
            jax.ShapeDtypeStruct((rows, cols), F32),
            jax.ShapeDtypeStruct((rows, cols), F32),
            jax.ShapeDtypeStruct((heads, HEAD_DIM + 8, HEAD_DIM), F32),
        ],
        compiler_params=params(),
        name="mixer",
    )(src, *parts, wq, wf, wv, gap)


def readout_kernel(inside_ref, query_ref, state_ref, gain_ref, out_ref):
    q_high, q_low = halves(query_ref[...])
    s_high, s_low = halves(state_ref[0])
    total = inside_ref[...] + mm(
        jnp.concatenate([q_high, q_low, q_high], axis=1),
        jnp.concatenate([s_high, s_high, s_low], axis=1),
        ((1,), (1,)),
    )
    out_ref[...] = normed(total, gain_ref[...]).astype(BF16)


def readout(inside, query, state, gain):
    rows, cols = inside.shape
    block = pl.BlockSpec((rows, HEAD_DIM), lambda h: (0, h))
    return pl.pallas_call(
        readout_kernel,
        grid=(cols // HEAD_DIM,),
        in_specs=[
            block,
            block,
            pl.BlockSpec((1, HEAD_DIM, HEAD_DIM), lambda h: (h, 0, 0)),
            pl.BlockSpec((1, HEAD_DIM), lambda h: (0, h)),
        ],
        out_specs=block,
        out_shape=jax.ShapeDtypeStruct((rows, cols), BF16),
        compiler_params=params(),
        name="readout",
    )(inside, query, state, gain)


def pieces(packed):
    return packed[:, HEAD_DIM : HEAD_DIM + 1, :], packed[:, :HEAD_DIM, :]


def link(earlier, later):
    return earlier[0] + later[0], jnp.exp(later[0]) * earlier[1] + later[1]


def pack(part):
    heads = part[1].shape[0]
    return jnp.concatenate(
        [part[1], jnp.broadcast_to(part[0], (heads, 8, HEAD_DIM))], axis=1
    )


def masked(flag, part):
    return jax.tree.map(lambda a: jnp.where(flag, a, 0.0), part)


def both_cores(a):
    return lax.ppermute(a, "ep_2", [(0, 1), (1, 0)])


def along_rows(packed):
    core = lax.axis_index("ep_2")
    other = both_cores(packed)
    is_second = core == 1
    low = jnp.where(is_second, other, packed)
    high = jnp.where(is_second, packed, other)
    half = packed.shape[0] // 2
    mine = lambda a: lax.dynamic_slice_in_dim(a, core * half, half, 0)
    chip = link(pieces(mine(low)), pieces(mine(high)))
    count = lax.axis_size("ep_1")
    sent = pack(chip)
    came = [
        lax.ppermute(sent, "ep_1", [(i, (i + d) % count) for i in range(count)])
        for d in range(count - 1, 0, -1)
    ]
    return low, chip, came


def along_planes(chip, came):
    row = lax.axis_index("ep_1")
    before = after = None
    for k, part in enumerate(came):
        d = len(came) - k
        early = masked(row >= d, pieces(part))
        late = masked(row < d, pieces(part))
        before = early if before is None else link(before, early)
        after = late if after is None else link(after, late)
    plane = pack(link(link(before, chip), after))
    count = lax.axis_size("ep_0")
    planes = [
        lax.ppermute(plane, "ep_0", [(i, (i + d) % count) for i in range(count)])
        for d in range(count - 1, 0, -1)
    ]
    return before, planes


def arriving_state(low, before, planes):
    is_second = lax.axis_index("ep_2") == 1
    at = lax.axis_index("ep_0")
    total = None
    for k, part in enumerate(planes):
        part = masked(at >= len(planes) - k, pieces(part))
        total = part if total is None else link(total, part)
    state = link(total, before)[1]
    swapped = both_cores(state)
    entering = jnp.concatenate(
        [jnp.where(is_second, swapped, state), jnp.where(is_second, state, swapped)], axis=0
    )
    first_core = pieces(low)
    return jnp.where(is_second, jnp.exp(first_core[0]) * entering + first_core[1], entering)


def hidden_kernel(own_ref, near_ref, go_ref, uo_ref, gf_ref, uf_ref, out_ref, gate, up):
    step = pl.program_id(0)

    @pl.when(step == 0)
    def _():
        gate[...] = jnp.zeros_like(gate)
        up[...] = jnp.zeros_like(up)

    rows = jnp.concatenate([own_ref[...], near_ref[...]], axis=0)
    n = go_ref.shape[1]
    gate[:, :n] += mm(rows, go_ref[...])
    gate[:, n:] += mm(rows, gf_ref[...])
    up[:, :n] += mm(rows, uo_ref[...])
    up[:, n:] += mm(rows, uf_ref[...])

    @pl.when(step == pl.num_programs(0) - 1)
    def _():
        gated = jnp.minimum(gate[...], CLAMP_LIMIT)
        opened = jnp.clip(up[...], -CLAMP_LIMIT, CLAMP_LIMIT)
        out_ref[...] = (
            (opened + 1.0) * gated * jax.nn.sigmoid(SWISH_SLOPE * gated)
        ).astype(BF16)


def hidden_units(own, near, half, weights):
    count = own.shape[0]
    width, n = weights[0].shape
    kb = 1024
    weight = pl.BlockSpec((kb, n), lambda i: (i, 0))
    return pl.pallas_call(
        hidden_kernel,
        grid=(width // kb,),
        in_specs=[
            pl.BlockSpec((count, kb), lambda i: (0, i + half * (width // kb))),
            pl.BlockSpec((count, kb), lambda i: (0, i)),
            weight,
            weight,
            weight,
            weight,
        ],
        out_specs=pl.BlockSpec((2 * count, 2 * n), lambda i: (0, 0)),
        out_shape=jax.ShapeDtypeStruct((2 * count, 2 * n), BF16),
        scratch_shapes=[pltpu.VMEM((2 * count, 2 * n), F32)] * 2,
        compiler_params=params(),
        name="hidden",
    )(own, near, *weights)


def down_kernel(src, this, twin, down_ref, out_ref, *, first):
    k = pl.program_id(0)
    n = down_ref.shape[0] // 4
    rows = out_ref.shape[0]
    unit = lambda s: down_ref[pl.ds(pl.multiple_of(s * n, n), n), :]
    for step, (mine, other) in enumerate(((this, twin), (twin, this))):

        @pl.when(k == step)
        def _():
            s, t = src[first + step], src[first + 1 - step]
            total = mm(mine[:rows, :n], unit(s)) + mm(mine[:rows, n:], unit(3 - s))
            total += mm(other[rows:, :n], unit(t)) + mm(other[rows:, n:], unit(3 - t))
            out_ref[...] = total.astype(BF16)


def down_rows(src, this, twin, first, down):
    both, width = this.shape
    cols = down.shape[1]
    whole = lambda k, s: (0, 0)
    return pl.pallas_call(
        functools.partial(down_kernel, first=first),
        grid_spec=pltpu.PrefetchScalarGridSpec(
            num_scalar_prefetch=1,
            grid=(2,),
            in_specs=[pl.BlockSpec((both, width), whole)] * 2 + [pl.BlockSpec(down.shape, whole)],
            out_specs=pl.BlockSpec((both // 2, cols), lambda k, s: (0, k)),
        ),
        out_shape=jax.ShapeDtypeStruct((both // 2, 2 * cols), BF16),
        compiler_params=params(),
        name="down",
    )(src, this, twin, down)


def down4_kernel(src, h_own, h_near, h_far, h_opp, down_ref, out_ref):
    k = pl.program_id(0)
    n = down_ref.shape[0] // 4
    rows = out_ref.shape[0]
    unit = lambda s: down_ref[pl.ds(pl.multiple_of(s * n, n), n), :]
    for this, (mine, other, twin) in enumerate(
        ((h_own, h_near, 1), (h_near, h_own, 0), (h_far, h_opp, 3), (h_opp, h_far, 2))
    ):

        @pl.when(k == this)
        def _():
            s, t = src[this], src[twin]
            total = mm(mine[:rows, :n], unit(s)) + mm(mine[:rows, n:], unit(3 - s))
            total += mm(other[rows:, :n], unit(t)) + mm(other[rows:, n:], unit(3 - t))
            out_ref[...] = total.astype(BF16)


def down_rows4(src, parts, down):
    both, width = parts[0].shape
    cols = down.shape[1]
    whole = lambda k, s: (0, 0)
    return pl.pallas_call(
        down4_kernel,
        grid_spec=pltpu.PrefetchScalarGridSpec(
            num_scalar_prefetch=1,
            grid=(4,),
            in_specs=[pl.BlockSpec((both, width), whole)] * 4 + [pl.BlockSpec(down.shape, whole)],
            out_specs=pl.BlockSpec((both // 2, cols), lambda k, s: (0, k)),
        ),
        out_shape=jax.ShapeDtypeStruct((both // 2, 4 * cols), BF16),
        compiler_params=params(),
        name="down4",
    )(src, *parts, down)


def places_kernel(src, routes_ref, logits_ref, out_ref):
    experts = logits_ref.shape[1]
    first, second, count, before = chosen(routes_ref[0], experts)
    logits = logits_ref[0].astype(F32)
    l0 = jnp.sum(jnp.where(first, logits, 0.0), axis=0, keepdims=True)
    l1 = jnp.sum(jnp.where(second, logits, 0.0), axis=0, keepdims=True)
    w0 = 1.0 / (1.0 + jnp.exp(l1 - l0))
    w1 = 1.0 / (1.0 + jnp.exp(l0 - l1))
    weight = jnp.where(first, w0, 0.0) + jnp.where(second, w1, 0.0)
    both = [slot_matrix(weight, before, count, half) for half in range(2)]
    place = jnp.concatenate(both, axis=0).T
    out_ref[0] = jnp.concatenate(halves(place), axis=0)


def places(src, routes, logits):
    experts, toks = logits.shape[1:]
    return pl.pallas_call(
        places_kernel,
        grid_spec=pltpu.PrefetchScalarGridSpec(
            num_scalar_prefetch=1,
            grid=(4,),
            in_specs=[
                pl.BlockSpec((1, 2, toks), lambda k, s: (s[k], 0, 0)),
                pl.BlockSpec((1, experts, toks), lambda k, s: (k, 0, 0)),
            ],
            out_specs=pl.BlockSpec((1, 2 * toks, experts * CAP), lambda k, s: (k, 0, 0)),
        ),
        out_shape=jax.ShapeDtypeStruct((4, 2 * toks, experts * CAP), BF16),
        compiler_params=params(),
        name="places",
    )(src, routes, logits)


def combine_kernel(src, first_ref, second_ref, high_ref, place_ref, out_ref):
    k = pl.program_id(0)
    slots = high_ref.shape[0]
    toks = out_ref.shape[0]
    for pair, low_ref in enumerate((first_ref, second_ref)):

        @pl.when(k // 2 == pair)
        def _():
            total = mm(place_ref[0, :, :slots], low_ref[...])
            total += mm(place_ref[0, :, slots:], high_ref[...])
            out_ref[...] = (total[:toks] + total[toks:]).astype(BF16)


def combined(src, first, second, high, place):
    slots = high.shape[0]
    cols = high.shape[1] // 4
    toks = place.shape[1] // 2
    return pl.pallas_call(
        combine_kernel,
        grid_spec=pltpu.PrefetchScalarGridSpec(
            num_scalar_prefetch=1,
            grid=(4,),
            in_specs=[
                pl.BlockSpec((slots, cols), lambda k, s: (0, jnp.minimum(k, 1))),
                pl.BlockSpec((slots, cols), lambda k, s: (0, jnp.maximum(k - 2, 0))),
                pl.BlockSpec((slots, cols), lambda k, s: (0, k)),
                pl.BlockSpec((1,) + place.shape[1:], lambda k, s: (k, 0, 0)),
            ],
            out_specs=pl.BlockSpec((toks, cols), lambda k, s: (s[k], 0)),
        ),
        out_shape=jax.ShapeDtypeStruct((4 * toks, cols), BF16),
        compiler_params=params(),
        name="combine",
    )(src, first, second, high, place)


NEAR = [(i, i ^ 1) for i in range(4)]
FAR = [(i, 3 - i) for i in range(4)]
OPPOSITE = [(i, i ^ 2) for i in range(4)]


def to_near(a):
    return lax.ppermute(a, "tp", NEAR)


def to_far(a):
    return lax.ppermute(a, "tp", FAR)


def shared(a, direct=True):
    far = to_far(a)
    near = to_near(a)
    return a, near, far, (lax.ppermute(a, "tp", OPPOSITE) if direct else to_near(far))


def swap(a):
    experts = 32
    rows, cols = a.shape
    out = lax.all_to_all(
        a.reshape(experts, rows // experts, cols), EP, split_axis=0, concat_axis=0, tiled=True
    )
    return out.reshape(rows, cols)


def per_device(
    mix_input,
    moe_input,
    norm_mix,
    query_weight,
    forget_weight,
    value_weight,
    forget_gap,
    norm_out,
    norm_moe,
    router_weight,
    expert_gate,
    expert_up,
    expert_down,
    routes,
):
    toks = moe_input.shape[0]
    x = lax.axis_index("tp").astype(jnp.int32)
    src = jnp.stack([x, x ^ 1, 3 - x, x ^ 2])
    by_block = routes.reshape(4, toks, 2).transpose(0, 2, 1)
    router = router_weight.T

    rows_a = normed(mix_input, norm_mix).astype(BF16)
    group_a = shared(rows_a, direct=False)
    rows_b, own = front(src, moe_input, norm_moe.reshape(1, -1), by_block, router_weight.shape[1])
    own_rows = swap(own)
    rows_near = to_near(rows_b)
    gate_far = to_far(expert_gate[0])
    up_far = to_far(expert_up[0])
    logits, low, high = refill(src, rows_b, rows_near, router, by_block)
    low, own_rows = lax.optimization_barrier((low, own_rows))
    low_rows = swap(low)
    high, low_rows = lax.optimization_barrier((high, low_rows))
    high_rows = swap(high)
    logits = jnp.concatenate([logits, to_far(logits)])
    place = places(src, by_block, logits)

    inside, query, packed = mixer(
        src, group_a, query_weight, forget_weight, value_weight, forget_gap.reshape(1, -1)
    )
    first_core, chip, came = along_rows(packed)

    low_rows, packed = lax.optimization_barrier((low_rows, packed))
    weights = (expert_gate[0], expert_up[0], gate_far, up_far)
    h_low = hidden_units(own_rows, low_rows, 0, weights)
    h_low = shared(h_low)
    down_first = down_rows(src, h_low[0], h_low[1], 0, expert_down[0])
    back_first = swap(down_first)
    h_high = hidden_units(own_rows, high_rows, 1, weights)
    h_high = shared(h_high)
    far, high_own = lax.optimization_barrier((h_low[2], h_high[0]))
    h_high = (high_own,) + h_high[1:]
    down_second = down_rows(src, far, h_low[3], 2, expert_down[0])
    down_second, back_first = lax.optimization_barrier((down_second, back_first))
    back_second = swap(down_second)
    came, _ = lax.optimization_barrier((came, down_second))
    before, planes = along_planes(chip, came)
    down_high = down_rows4(src, h_high, expert_down[0])
    down_high, back_second = lax.optimization_barrier((down_high, back_second))
    back_high = swap(down_high)
    planes, _ = lax.optimization_barrier((planes, down_high))

    state = arriving_state(first_core, before, planes)
    mixer_out = readout(inside, query, state, norm_out.reshape(1, -1))
    expert_out = combined(src, back_first, back_second, back_high, place)
    return (mixer_out, expert_out)


def solution(mesh):
    finer = Mesh(mesh.devices.reshape(4, 4, 2, mesh.shape["tp"]), ("ep_0", "ep_1", "ep_2", "tp"))
    placed = (
        P(EP_TP, None),
        P(EP_TP, None),
        P(),
        P(None, "tp"),
        P(None, "tp"),
        P(None, "tp"),
        P("tp"),
        P("tp"),
        P(),
        P(),
        P(EP, None, "tp"),
        P(EP, None, "tp"),
        P(EP, None, "tp"),
        P(EP, None),
    )

    return jax.shard_map(
        per_device,
        mesh=finer,
        in_specs=placed,
        out_specs=(P(EP, "tp"), P(EP, "tp")),
        check_vma=False,
    )
```

```python
import functools

import jax
import jax.numpy as jnp
from jax import lax
from jax.experimental import pallas as pl
from jax.experimental.pallas import tpu as pltpu
from jax.sharding import Mesh
from jax.sharding import PartitionSpec as P

HEAD_DIM = 128

CAP = 16
HALF = 8
EP = ("ep_0", "ep_1", "ep_2")
EP_TP = ("ep_0", "ep_1", "ep_2", "tp")

EPSILON = 1e-06
CLAMP_LIMIT = 7.0
SWISH_SLOPE = 1.702
F32 = jnp.float32
BF16 = jnp.bfloat16


def mm(a, b, contract=((1,), (0,))):
    return lax.dot_general(a, b, (contract, ((), ())), preferred_element_type=F32)


def halves(a):
    high = a.astype(BF16)
    return high, (a - high.astype(F32)).astype(BF16)


def params(mib=56, axes=("arbitrary",)):
    return pltpu.CompilerParams(vmem_limit_bytes=mib << 20, dimension_semantics=axes)


def normed(row_data, gain_vec):
    as_float = row_data.astype(F32)
    scale = lax.rsqrt(jnp.mean(as_float * as_float, axis=-1, keepdims=True) + EPSILON)
    return as_float * scale * gain_vec


def chosen(routes, experts):
    toks = routes.shape[1]
    ids = lax.broadcasted_iota(jnp.int32, (experts, toks), 0)
    first = routes[0:1, :] == ids
    second = routes[1:2, :] == ids
    count = jnp.where(first | second, 1.0, 0.0)
    earlier = (
        lax.broadcasted_iota(jnp.int32, (toks, toks), 0)
        < lax.broadcasted_iota(jnp.int32, (toks, toks), 1)
    )
    before = mm(count.astype(BF16), jnp.where(earlier, 1.0, 0.0).astype(BF16))
    return first, second, count, before


def slot_matrix(weight, before, count, half):
    experts, toks = weight.shape
    place = lax.broadcasted_iota(jnp.int32, (experts, HALF, toks), 1) + half * HALF
    here = (before[:, None, :] == place.astype(F32)) & (count[:, None, :] > 0.5)
    return jnp.where(here, weight[:, None, :], 0.0).reshape(experts * HALF, toks)


def fill(routes, rows, experts, parts):
    _, _, count, before = chosen(routes, experts)
    pick = [slot_matrix(count, before, count, half) for half in range(parts)]
    out = mm(jnp.concatenate(pick, axis=0).astype(BF16), rows).astype(BF16)
    return [out[k * experts * HALF : (k + 1) * experts * HALF] for k in range(parts)]


def front_kernel(src, x_ref, gain_ref, routes_ref, rows_ref, buf_ref, *, group):
    step = pl.program_id(0)
    width = x_ref.shape[1]

    @pl.when(step == 0)
    def _():
        rows_ref[...] = normed(x_ref[...], gain_ref[...]).astype(BF16)

    low, high = fill(routes_ref[0] - step * group, rows_ref[...], group, 2)
    buf_ref[:, :width] = low
    buf_ref[:, width:] = high


def refill_kernel(src, own_ref, rows_ref, router_ref, routes_ref, logits_ref, low_ref, *, group):
    step = pl.program_id(0)

    @pl.when(step == 0)
    def _():
        for k, ref in enumerate((own_ref, rows_ref)):
            logits_ref[k] = mm(router_ref[...], ref[...], ((1,), (1,))).astype(BF16)

    (low_ref[...],) = fill(routes_ref[0] - step * group, rows_ref[...], group, 1)


def front(src, x, gain, routes, experts):
    toks, width = x.shape
    group = 16
    whole = lambda i, s: (0, 0)
    return pl.pallas_call(
        functools.partial(front_kernel, group=group),
        grid_spec=pltpu.PrefetchScalarGridSpec(
            num_scalar_prefetch=1,
            grid=(experts // group,),
            in_specs=[
                pl.BlockSpec((toks, width), whole),
                pl.BlockSpec((1, width), whole),
                pl.BlockSpec((1, 2, toks), lambda i, s: (s[0], 0, 0)),
            ],
            out_specs=[
                pl.BlockSpec((toks, width), whole),
                pl.BlockSpec((group * HALF, 2 * width), lambda i, s: (i, 0)),
            ],
        ),
        out_shape=[
            jax.ShapeDtypeStruct((toks, width), BF16),
            jax.ShapeDtypeStruct((experts * HALF, 2 * width), BF16),
        ],
        compiler_params=params(),
        name="front",
    )(src, x, gain, routes)


def refill(src, own, rows, router, routes):
    toks, width = rows.shape
    experts = router.shape[0]
    group = 16
    whole = lambda i, s: (0, 0)
    return pl.pallas_call(
        functools.partial(refill_kernel, group=group),
        grid_spec=pltpu.PrefetchScalarGridSpec(
            num_scalar_prefetch=1,
            grid=(experts // group,),
            in_specs=[
                pl.BlockSpec((toks, width), whole),
                pl.BlockSpec((toks, width), whole),
                pl.BlockSpec(router.shape, whole),
                pl.BlockSpec((1, 2, toks), lambda i, s: (s[1], 0, 0)),
            ],
            out_specs=[
                pl.BlockSpec((2, experts, toks), lambda i, s: (0, 0, 0)),
                pl.BlockSpec((group * HALF, width), lambda i, s: (i, 0)),
            ],
        ),
        out_shape=[
            jax.ShapeDtypeStruct((2, experts, toks), BF16),
            jax.ShapeDtypeStruct((experts * HALF, width), BF16),
        ],
        compiler_params=params(),
        name="refill",
    )(src, own, rows, router, routes)


def mixer_kernel(
    src, a0, a1, a2, a3, q_ref, f_ref, v_ref, gap_ref, inside_ref, query_ref, packed_ref, qa, fa, va, group
):
    step = pl.program_id(0)

    @pl.when(step == 0)
    def _():
        qa[...] = jnp.zeros_like(qa)
        fa[...] = jnp.zeros_like(fa)
        va[...] = jnp.zeros_like(va)

    toks = a0.shape[0]
    for k, part in enumerate((a0, a1, a2, a3)):
        group[pl.ds(pl.multiple_of(src[k] * toks, toks), toks), :] = part[...]
    a = group[...]
    qa[...] += mm(a, q_ref[...])
    fa[...] += mm(a, f_ref[...])
    va[...] += mm(a, v_ref[...])

    @pl.when(step == pl.num_programs(0) - 1)
    def _():
        rows = a.shape[0]
        causal = (
            lax.broadcasted_iota(jnp.int32, (rows, rows), 0)
            >= lax.broadcasted_iota(jnp.int32, (rows, rows), 1)
        )
        ones = jnp.where(causal[:toks, :toks], 1.0, 0.0).astype(BF16)
        shut = gap_ref[...] * jax.nn.sigmoid(-fa[...])
        fa[...] = jnp.log1p(-shut)
        cols = shut.shape[1]
        base = None
        for k in range(rows // toks):
            part = fa[k * toks : (k + 1) * toks, :]
            high = part.astype(BF16)
            rest = part - high.astype(F32)
            mid = rest.astype(BF16)
            low = (rest - mid.astype(F32)).astype(BF16)
            sums = mm(ones, jnp.concatenate([high, mid, low], axis=1))
            sums = sums[:, :cols] + sums[:, cols : 2 * cols] + sums[:, 2 * cols :]
            sums = sums if base is None else sums + base
            base = sums[toks - 1 :, :]
            fa[k * toks : (k + 1) * toks, :] = sums
        sums = fa[...]
        last = sums[rows - 1 :, :]
        query_ref[...] = qa[...] * jnp.exp(sums)
        keys = shut * jnp.exp(-sums)
        late = shut * jnp.exp(last - sums)
        half = rows // 2
        for h in range(packed_ref.shape[0]):
            at = slice(h * HEAD_DIM, (h + 1) * HEAD_DIM)
            q_high, q_low = halves(query_ref[:, at])
            k_high, k_low = halves(keys[:, at])
            v_high, v_low = halves(va[:, at])
            l_high, l_low = halves(late[:, at])
            left = jnp.concatenate([q_high, q_low, q_high], axis=1)
            right = jnp.concatenate([k_high, k_high, k_low], axis=1)
            values = jnp.concatenate([v_high, v_low], axis=1)
            for k in range(2):
                end = (k + 1) * half
                scores = mm(left[end - half : end], right[:end], ((1,), (1,)))
                s_high, s_low = halves(jnp.where(causal[end - half : end, :end], scores, 0.0))
                part = mm(s_high, values[:end])
                part = part[:, :HEAD_DIM] + part[:, HEAD_DIM:] + mm(s_low, v_high[:end])
                inside_ref[end - half : end, at] = part
            outer = mm(values, jnp.concatenate([l_high, l_low], axis=1), ((0,), (0,)))
            packed_ref[h, :HEAD_DIM, :] = (
                outer[:HEAD_DIM, :HEAD_DIM]
                + outer[:HEAD_DIM, HEAD_DIM:]
                + outer[HEAD_DIM:, :HEAD_DIM]
            )
            packed_ref[h, HEAD_DIM:, :] = jnp.broadcast_to(last[:, at], (8, HEAD_DIM))


def mixer(src, parts, wq, wf, wv, gap):
    toks, width = parts[0].shape
    rows = 4 * toks
    cols = wq.shape[1]
    heads = cols // HEAD_DIM
    kb = 512
    fixed = lambda i, s: (0, 0)
    weight = pl.BlockSpec((kb, cols), lambda i, s: (i, 0))
    return pl.pallas_call(
        mixer_kernel,
        grid_spec=pltpu.PrefetchScalarGridSpec(
            num_scalar_prefetch=1,
            grid=(width // kb,),
            in_specs=[pl.BlockSpec((toks, kb), lambda i, s: (0, i))] * 4
            + [weight, weight, weight, pl.BlockSpec((1, cols), fixed)],
            out_specs=[
                pl.BlockSpec((rows, cols), fixed),
                pl.BlockSpec((rows, cols), fixed),
                pl.BlockSpec((heads, HEAD_DIM + 8, HEAD_DIM), lambda i, s: (0, 0, 0)),
            ],
            scratch_shapes=[pltpu.VMEM((rows, cols), F32)] * 3 + [pltpu.VMEM((rows, kb), BF16)],
        ),
        out_shape=[
            jax.ShapeDtypeStruct((rows, cols), F32),
            jax.ShapeDtypeStruct((rows, cols), F32),
            jax.ShapeDtypeStruct((heads, HEAD_DIM + 8, HEAD_DIM), F32),
        ],
        compiler_params=params(),
        name="mixer",
    )(src, *parts, wq, wf, wv, gap)


def readout_kernel(inside_ref, query_ref, state_ref, gain_ref, out_ref):
    q_high, q_low = halves(query_ref[...])
    s_high, s_low = halves(state_ref[0])
    total = inside_ref[...] + mm(
        jnp.concatenate([q_high, q_low, q_high], axis=1),
        jnp.concatenate([s_high, s_high, s_low], axis=1),
        ((1,), (1,)),
    )
    out_ref[...] = normed(total, gain_ref[...]).astype(BF16)


def readout(inside, query, state, gain):
    rows, cols = inside.shape
    block = pl.BlockSpec((rows, HEAD_DIM), lambda h: (0, h))
    return pl.pallas_call(
        readout_kernel,
        grid=(cols // HEAD_DIM,),
        in_specs=[
            block,
            block,
            pl.BlockSpec((1, HEAD_DIM, HEAD_DIM), lambda h: (h, 0, 0)),
            pl.BlockSpec((1, HEAD_DIM), lambda h: (0, h)),
        ],
        out_specs=block,
        out_shape=jax.ShapeDtypeStruct((rows, cols), BF16),
        compiler_params=params(),
        name="readout",
    )(inside, query, state, gain)


def pieces(packed):
    return packed[:, HEAD_DIM : HEAD_DIM + 1, :], packed[:, :HEAD_DIM, :]


def link(earlier, later):
    return earlier[0] + later[0], jnp.exp(later[0]) * earlier[1] + later[1]


def pack(part):
    heads = part[1].shape[0]
    return jnp.concatenate(
        [part[1], jnp.broadcast_to(part[0], (heads, 8, HEAD_DIM))], axis=1
    )


def masked(flag, part):
    return jax.tree.map(lambda a: jnp.where(flag, a, 0.0), part)


def both_cores(a):
    return lax.ppermute(a, "ep_2", [(0, 1), (1, 0)])


def along_rows(packed):
    core = lax.axis_index("ep_2")
    other = both_cores(packed)
    is_second = core == 1
    low = jnp.where(is_second, other, packed)
    high = jnp.where(is_second, packed, other)
    half = packed.shape[0] // 2
    mine = lambda a: lax.dynamic_slice_in_dim(a, core * half, half, 0)
    chip = link(pieces(mine(low)), pieces(mine(high)))
    count = lax.axis_size("ep_1")
    sent = pack(chip)
    came = [
        lax.ppermute(sent, "ep_1", [(i, (i + d) % count) for i in range(count)])
        for d in range(count - 1, 0, -1)
    ]
    return low, chip, came


def along_planes(chip, came):
    row = lax.axis_index("ep_1")
    before = after = None
    for k, part in enumerate(came):
        d = len(came) - k
        early = masked(row >= d, pieces(part))
        late = masked(row < d, pieces(part))
        before = early if before is None else link(before, early)
        after = late if after is None else link(after, late)
    plane = pack(link(link(before, chip), after))
    count = lax.axis_size("ep_0")
    planes = [
        lax.ppermute(plane, "ep_0", [(i, (i + d) % count) for i in range(count)])
        for d in range(count - 1, 0, -1)
    ]
    return before, planes


def arriving_state(low, before, planes):
    is_second = lax.axis_index("ep_2") == 1
    at = lax.axis_index("ep_0")
    total = None
    for k, part in enumerate(planes):
        part = masked(at >= len(planes) - k, pieces(part))
        total = part if total is None else link(total, part)
    state = link(total, before)[1]
    swapped = both_cores(state)
    entering = jnp.concatenate(
        [jnp.where(is_second, swapped, state), jnp.where(is_second, state, swapped)], axis=0
    )
    first_core = pieces(low)
    return jnp.where(is_second, jnp.exp(first_core[0]) * entering + first_core[1], entering)


def hidden_kernel(own_ref, near_ref, go_ref, uo_ref, gf_ref, uf_ref, out_ref, gate, up):
    step = pl.program_id(0)

    @pl.when(step == 0)
    def _():
        gate[...] = jnp.zeros_like(gate)
        up[...] = jnp.zeros_like(up)

    rows = jnp.concatenate([own_ref[...], near_ref[...]], axis=0)
    n = go_ref.shape[1]
    gate[:, :n] += mm(rows, go_ref[...])
    gate[:, n:] += mm(rows, gf_ref[...])
    up[:, :n] += mm(rows, uo_ref[...])
    up[:, n:] += mm(rows, uf_ref[...])

    @pl.when(step == pl.num_programs(0) - 1)
    def _():
        gated = jnp.minimum(gate[...], CLAMP_LIMIT)
        opened = jnp.clip(up[...], -CLAMP_LIMIT, CLAMP_LIMIT)
        out_ref[...] = (
            (opened + 1.0) * gated * jax.nn.sigmoid(SWISH_SLOPE * gated)
        ).astype(BF16)


def hidden_units(own, near, half, weights):
    count = own.shape[0]
    width, n = weights[0].shape
    kb = 1024
    weight = pl.BlockSpec((kb, n), lambda i: (i, 0))
    return pl.pallas_call(
        hidden_kernel,
        grid=(width // kb,),
        in_specs=[
            pl.BlockSpec((count, kb), lambda i: (0, i + half * (width // kb))),
            pl.BlockSpec((count, kb), lambda i: (0, i)),
            weight,
            weight,
            weight,
            weight,
        ],
        out_specs=pl.BlockSpec((2 * count, 2 * n), lambda i: (0, 0)),
        out_shape=jax.ShapeDtypeStruct((2 * count, 2 * n), BF16),
        scratch_shapes=[pltpu.VMEM((2 * count, 2 * n), F32)] * 2,
        compiler_params=params(),
        name="hidden",
    )(own, near, *weights)


def down_kernel(src, h_own, h_near, h_far, h_opp, down_ref, out_ref):
    k = pl.program_id(0)
    n = down_ref.shape[0] // 4
    rows = out_ref.shape[0]
    unit = lambda s: down_ref[pl.ds(pl.multiple_of(s * n, n), n), :]
    for this, (mine, other, twin) in enumerate(
        ((h_own, h_near, 1), (h_near, h_own, 0), (h_far, h_opp, 3), (h_opp, h_far, 2))
    ):

        @pl.when(k == this)
        def _():
            s, t = src[this], src[twin]
            total = mm(mine[:rows, :n], unit(s)) + mm(mine[:rows, n:], unit(3 - s))
            total += mm(other[rows:, :n], unit(t)) + mm(other[rows:, n:], unit(3 - t))
            out_ref[...] = total.astype(BF16)


def down_rows(src, parts, down):
    both, width = parts[0].shape
    cols = down.shape[1]
    whole = lambda k, s: (0, 0)
    return pl.pallas_call(
        down_kernel,
        grid_spec=pltpu.PrefetchScalarGridSpec(
            num_scalar_prefetch=1,
            grid=(4,),
            in_specs=[pl.BlockSpec((both, width), whole)] * 4 + [pl.BlockSpec(down.shape, whole)],
            out_specs=pl.BlockSpec((both // 2, cols), lambda k, s: (0, k)),
        ),
        out_shape=jax.ShapeDtypeStruct((both // 2, 4 * cols), BF16),
        compiler_params=params(),
        name="down",
    )(src, *parts, down)


def places_kernel(src, routes_ref, logits_ref, out_ref):
    experts = logits_ref.shape[1]
    first, second, count, before = chosen(routes_ref[0], experts)
    logits = logits_ref[0].astype(F32)
    l0 = jnp.sum(jnp.where(first, logits, 0.0), axis=0, keepdims=True)
    l1 = jnp.sum(jnp.where(second, logits, 0.0), axis=0, keepdims=True)
    w0 = 1.0 / (1.0 + jnp.exp(l1 - l0))
    w1 = 1.0 / (1.0 + jnp.exp(l0 - l1))
    weight = jnp.where(first, w0, 0.0) + jnp.where(second, w1, 0.0)
    both = [slot_matrix(weight, before, count, half) for half in range(2)]
    place = jnp.concatenate(both, axis=0).T
    out_ref[0] = jnp.concatenate(halves(place), axis=0)


def places(src, routes, logits):
    experts, toks = logits.shape[1:]
    return pl.pallas_call(
        places_kernel,
        grid_spec=pltpu.PrefetchScalarGridSpec(
            num_scalar_prefetch=1,
            grid=(4,),
            in_specs=[
                pl.BlockSpec((1, 2, toks), lambda k, s: (s[k], 0, 0)),
                pl.BlockSpec((1, experts, toks), lambda k, s: (k, 0, 0)),
            ],
            out_specs=pl.BlockSpec((1, 2 * toks, experts * CAP), lambda k, s: (k, 0, 0)),
        ),
        out_shape=jax.ShapeDtypeStruct((4, 2 * toks, experts * CAP), BF16),
        compiler_params=params(),
        name="places",
    )(src, routes, logits)


def combine_kernel(src, low_ref, high_ref, place_ref, out_ref):
    slots = low_ref.shape[0]
    total = mm(place_ref[0, :, :slots], low_ref[...]) + mm(place_ref[0, :, slots:], high_ref[...])
    toks = out_ref.shape[0]
    out_ref[...] = (total[:toks] + total[toks:]).astype(BF16)


def combined(src, low, high, place):
    slots = low.shape[0]
    cols = low.shape[1] // 4
    toks = place.shape[1] // 2
    res = pl.BlockSpec((slots, cols), lambda k, s: (0, k))
    return pl.pallas_call(
        combine_kernel,
        grid_spec=pltpu.PrefetchScalarGridSpec(
            num_scalar_prefetch=1,
            grid=(4,),
            in_specs=[
                res,
                res,
                pl.BlockSpec((1,) + place.shape[1:], lambda k, s: (k, 0, 0)),
            ],
            out_specs=pl.BlockSpec((toks, cols), lambda k, s: (s[k], 0)),
        ),
        out_shape=jax.ShapeDtypeStruct((4 * toks, cols), BF16),
        compiler_params=params(),
        name="combine",
    )(src, low, high, place)


NEAR = [(i, i ^ 1) for i in range(4)]
FAR = [(i, 3 - i) for i in range(4)]
OPPOSITE = [(i, i ^ 2) for i in range(4)]


def to_near(a):
    return lax.ppermute(a, "tp", NEAR)


def to_far(a):
    return lax.ppermute(a, "tp", FAR)


def shared(a, direct=True):
    far = to_far(a)
    near = to_near(a)
    return a, near, far, (lax.ppermute(a, "tp", OPPOSITE) if direct else to_near(far))


def swap(a):
    experts = 32
    rows, cols = a.shape
    out = lax.all_to_all(
        a.reshape(experts, rows // experts, cols), EP, split_axis=0, concat_axis=0, tiled=True
    )
    return out.reshape(rows, cols)


def per_device(
    mix_input,
    moe_input,
    norm_mix,
    query_weight,
    forget_weight,
    value_weight,
    forget_gap,
    norm_out,
    norm_moe,
    router_weight,
    expert_gate,
    expert_up,
    expert_down,
    routes,
):
    toks = moe_input.shape[0]
    x = lax.axis_index("tp").astype(jnp.int32)
    src = jnp.stack([x, x ^ 1, 3 - x, x ^ 2])
    by_block = routes.reshape(4, toks, 2).transpose(0, 2, 1)
    router = router_weight.T

    width = moe_input.shape[1]
    gate_far = to_far(expert_gate[0])
    rows_b, own = front(src, moe_input, norm_moe.reshape(1, -1), by_block, router_weight.shape[1])
    own_rows = swap(own)
    rows_near = to_near(rows_b)
    mix_input, _ = lax.optimization_barrier((mix_input, rows_b))
    rows_a = normed(mix_input, norm_mix).astype(BF16)
    group_a = shared(rows_a, direct=False)
    up_far = to_far(expert_up[0])
    logits, low = refill(src, rows_b, rows_near, router, by_block)
    low, own_rows = lax.optimization_barrier((low, own_rows))
    low_rows = swap(low)
    high_rows = to_near(own_rows[:, width:])
    logits = jnp.concatenate([logits, to_far(logits)])
    place = places(src, by_block, logits)

    inside, query, packed = mixer(
        src, group_a, query_weight, forget_weight, value_weight, forget_gap.reshape(1, -1)
    )
    first_core, chip, came = along_rows(packed)

    low_rows, packed = lax.optimization_barrier((low_rows, packed))
    weights = (expert_gate[0], expert_up[0], gate_far, up_far)
    h_low = hidden_units(own_rows, low_rows, 0, weights)
    h_low = shared(h_low)
    high_rows, low_own = lax.optimization_barrier((high_rows, h_low[0]))
    h_high = hidden_units(own_rows, high_rows, 1, weights)
    h_high = shared(h_high)
    opp, high_own = lax.optimization_barrier((h_low[3], h_high[0]))
    down_low = down_rows(src, (low_own,) + h_low[1:3] + (opp,), expert_down[0])
    back_low = swap(down_low)
    came, _ = lax.optimization_barrier((came, down_low))
    before, planes = along_planes(chip, came)
    down_high = down_rows(src, (high_own,) + h_high[1:], expert_down[0])
    down_high, back_low = lax.optimization_barrier((down_high, back_low))
    back_high = swap(down_high)
    planes, _ = lax.optimization_barrier((planes, down_high))

    state = arriving_state(first_core, before, planes)
    mixer_out = readout(inside, query, state, norm_out.reshape(1, -1))
    expert_out = combined(src, back_low, back_high, place)
    return (mixer_out, expert_out)


def solution(mesh):
    finer = Mesh(mesh.devices.reshape(4, 4, 2, mesh.shape["tp"]), ("ep_0", "ep_1", "ep_2", "tp"))
    placed = (
        P(EP_TP, None),
        P(EP_TP, None),
        P(),
        P(None, "tp"),
        P(None, "tp"),
        P(None, "tp"),
        P("tp"),
        P("tp"),
        P(),
        P(),
        P(EP, None, "tp"),
        P(EP, None, "tp"),
        P(EP, None, "tp"),
        P(EP, None),
    )

    return jax.shard_map(
        per_device,
        mesh=finer,
        in_specs=placed,
        out_specs=(P(EP, "tp"), P(EP, "tp")),
        check_vma=False,
    )
```

```python
import functools

import jax
import jax.numpy as jnp
from jax import lax
from jax.experimental import pallas as pl
from jax.experimental.pallas import tpu as pltpu
from jax.sharding import Mesh
from jax.sharding import PartitionSpec as P

HEAD_DIM = 128

CAP = 16
HALF = 8
EP = ("ep_0", "ep_1", "ep_2")
EP_TP = ("ep_0", "ep_1", "ep_2", "tp")

EPSILON = 1e-06
CLAMP_LIMIT = 7.0
SWISH_SLOPE = 1.702
F32 = jnp.float32
BF16 = jnp.bfloat16


def mm(a, b, contract=((1,), (0,))):
    return lax.dot_general(a, b, (contract, ((), ())), preferred_element_type=F32)


def halves(a):
    high = a.astype(BF16)
    return high, (a - high.astype(F32)).astype(BF16)


def params(mib=56, axes=("arbitrary",)):
    return pltpu.CompilerParams(vmem_limit_bytes=mib << 20, dimension_semantics=axes)


def normed(row_data, gain_vec):
    as_float = row_data.astype(F32)
    scale = lax.rsqrt(jnp.mean(as_float * as_float, axis=-1, keepdims=True) + EPSILON)
    return as_float * scale * gain_vec


def chosen(routes, experts):
    toks = routes.shape[1]
    ids = lax.broadcasted_iota(jnp.int32, (experts, toks), 0)
    first = routes[0:1, :] == ids
    second = routes[1:2, :] == ids
    count = jnp.where(first | second, 1.0, 0.0)
    earlier = (
        lax.broadcasted_iota(jnp.int32, (toks, toks), 0)
        < lax.broadcasted_iota(jnp.int32, (toks, toks), 1)
    )
    before = mm(count.astype(BF16), jnp.where(earlier, 1.0, 0.0).astype(BF16))
    return first, second, count, before


def slot_matrix(weight, before, count, half):
    experts, toks = weight.shape
    place = lax.broadcasted_iota(jnp.int32, (experts, HALF, toks), 1) + half * HALF
    here = (before[:, None, :] == place.astype(F32)) & (count[:, None, :] > 0.5)
    return jnp.where(here, weight[:, None, :], 0.0).reshape(experts * HALF, toks)


def fill(routes, rows, experts):
    _, _, count, before = chosen(routes, experts)
    pick = [slot_matrix(count, before, count, half) for half in range(2)]
    both = mm(jnp.concatenate(pick, axis=0).astype(BF16), rows).astype(BF16)
    return both[: experts * HALF], both[experts * HALF :]


def front_kernel(src, x_ref, gain_ref, routes_ref, rows_ref, buf_ref, *, group):
    step = pl.program_id(0)
    width = x_ref.shape[1]

    @pl.when(step == 0)
    def _():
        rows_ref[...] = normed(x_ref[...], gain_ref[...]).astype(BF16)

    low, high = fill(routes_ref[0] - step * group, rows_ref[...], group)
    buf_ref[:, :width] = low
    buf_ref[:, width:] = high


def refill_kernel(src, own_ref, rows_ref, router_ref, routes_ref, logits_ref, low_ref, high_ref, *, group):
    step = pl.program_id(0)

    @pl.when(step == 0)
    def _():
        for k, ref in enumerate((own_ref, rows_ref)):
            logits_ref[k] = mm(router_ref[...], ref[...], ((1,), (1,))).astype(BF16)

    low_ref[...], high_ref[...] = fill(routes_ref[0] - step * group, rows_ref[...], group)


def front(src, x, gain, routes, experts):
    toks, width = x.shape
    group = 16
    whole = lambda i, s: (0, 0)
    return pl.pallas_call(
        functools.partial(front_kernel, group=group),
        grid_spec=pltpu.PrefetchScalarGridSpec(
            num_scalar_prefetch=1,
            grid=(experts // group,),
            in_specs=[
                pl.BlockSpec((toks, width), whole),
                pl.BlockSpec((1, width), whole),
                pl.BlockSpec((1, 2, toks), lambda i, s: (s[0], 0, 0)),
            ],
            out_specs=[
                pl.BlockSpec((toks, width), whole),
                pl.BlockSpec((group * HALF, 2 * width), lambda i, s: (i, 0)),
            ],
        ),
        out_shape=[
            jax.ShapeDtypeStruct((toks, width), BF16),
            jax.ShapeDtypeStruct((experts * HALF, 2 * width), BF16),
        ],
        compiler_params=params(),
        name="front",
    )(src, x, gain, routes)


def refill(src, own, rows, router, routes):
    toks, width = rows.shape
    experts = router.shape[0]
    group = 16
    whole = lambda i, s: (0, 0)
    return pl.pallas_call(
        functools.partial(refill_kernel, group=group),
        grid_spec=pltpu.PrefetchScalarGridSpec(
            num_scalar_prefetch=1,
            grid=(experts // group,),
            in_specs=[
                pl.BlockSpec((toks, width), whole),
                pl.BlockSpec((toks, width), whole),
                pl.BlockSpec(router.shape, whole),
                pl.BlockSpec((1, 2, toks), lambda i, s: (s[1], 0, 0)),
            ],
            out_specs=[
                pl.BlockSpec((2, experts, toks), lambda i, s: (0, 0, 0)),
                pl.BlockSpec((group * HALF, width), lambda i, s: (i, 0)),
                pl.BlockSpec((group * HALF, width), lambda i, s: (i, 0)),
            ],
        ),
        out_shape=[
            jax.ShapeDtypeStruct((2, experts, toks), BF16),
            jax.ShapeDtypeStruct((experts * HALF, width), BF16),
            jax.ShapeDtypeStruct((experts * HALF, width), BF16),
        ],
        compiler_params=params(),
        name="refill",
    )(src, own, rows, router, routes)


def mixer_kernel(
    src, a0, a1, a2, a3, q_ref, f_ref, v_ref, gap_ref, inside_ref, query_ref, packed_ref, qa, fa, va, group
):
    step = pl.program_id(0)

    @pl.when(step == 0)
    def _():
        qa[...] = jnp.zeros_like(qa)
        fa[...] = jnp.zeros_like(fa)
        va[...] = jnp.zeros_like(va)

    toks = a0.shape[0]
    for k, part in enumerate((a0, a1, a2, a3)):
        group[pl.ds(pl.multiple_of(src[k] * toks, toks), toks), :] = part[...]
    a = group[...]
    qa[...] += mm(a, q_ref[...])
    fa[...] += mm(a, f_ref[...])
    va[...] += mm(a, v_ref[...])

    @pl.when(step == pl.num_programs(0) - 1)
    def _():
        rows = a.shape[0]
        causal = (
            lax.broadcasted_iota(jnp.int32, (rows, rows), 0)
            >= lax.broadcasted_iota(jnp.int32, (rows, rows), 1)
        )
        ones = jnp.where(causal[:toks, :toks], 1.0, 0.0).astype(BF16)
        shut = gap_ref[...] * jax.nn.sigmoid(-fa[...])
        fa[...] = jnp.log1p(-shut)
        cols = shut.shape[1]
        base = None
        for k in range(rows // toks):
            part = fa[k * toks : (k + 1) * toks, :]
            high = part.astype(BF16)
            rest = part - high.astype(F32)
            mid = rest.astype(BF16)
            low = (rest - mid.astype(F32)).astype(BF16)
            sums = mm(ones, jnp.concatenate([high, mid, low], axis=1))
            sums = sums[:, :cols] + sums[:, cols : 2 * cols] + sums[:, 2 * cols :]
            sums = sums if base is None else sums + base
            base = sums[toks - 1 :, :]
            fa[k * toks : (k + 1) * toks, :] = sums
        sums = fa[...]
        last = sums[rows - 1 :, :]
        query_ref[...] = qa[...] * jnp.exp(sums)
        keys = shut * jnp.exp(-sums)
        late = shut * jnp.exp(last - sums)
        half = rows // 2
        for h in range(packed_ref.shape[0]):
            at = slice(h * HEAD_DIM, (h + 1) * HEAD_DIM)
            q_high, q_low = halves(query_ref[:, at])
            k_high, k_low = halves(keys[:, at])
            v_high, v_low = halves(va[:, at])
            l_high, l_low = halves(late[:, at])
            left = jnp.concatenate([q_high, q_low, q_high], axis=1)
            right = jnp.concatenate([k_high, k_high, k_low], axis=1)
            values = jnp.concatenate([v_high, v_low], axis=1)
            for k in range(2):
                end = (k + 1) * half
                scores = mm(left[end - half : end], right[:end], ((1,), (1,)))
                s_high, s_low = halves(jnp.where(causal[end - half : end, :end], scores, 0.0))
                part = mm(s_high, values[:end])
                part = part[:, :HEAD_DIM] + part[:, HEAD_DIM:] + mm(s_low, v_high[:end])
                inside_ref[end - half : end, at] = part
            outer = mm(values, jnp.concatenate([l_high, l_low], axis=1), ((0,), (0,)))
            packed_ref[h, :HEAD_DIM, :] = (
                outer[:HEAD_DIM, :HEAD_DIM]
                + outer[:HEAD_DIM, HEAD_DIM:]
                + outer[HEAD_DIM:, :HEAD_DIM]
            )
            packed_ref[h, HEAD_DIM:, :] = jnp.broadcast_to(last[:, at], (8, HEAD_DIM))


def mixer(src, parts, wq, wf, wv, gap):
    toks, width = parts[0].shape
    rows = 4 * toks
    cols = wq.shape[1]
    heads = cols // HEAD_DIM
    kb = 512
    fixed = lambda i, s: (0, 0)
    weight = pl.BlockSpec((kb, cols), lambda i, s: (i, 0))
    return pl.pallas_call(
        mixer_kernel,
        grid_spec=pltpu.PrefetchScalarGridSpec(
            num_scalar_prefetch=1,
            grid=(width // kb,),
            in_specs=[pl.BlockSpec((toks, kb), lambda i, s: (0, i))] * 4
            + [weight, weight, weight, pl.BlockSpec((1, cols), fixed)],
            out_specs=[
                pl.BlockSpec((rows, cols), fixed),
                pl.BlockSpec((rows, cols), fixed),
                pl.BlockSpec((heads, HEAD_DIM + 8, HEAD_DIM), lambda i, s: (0, 0, 0)),
            ],
            scratch_shapes=[pltpu.VMEM((rows, cols), F32)] * 3 + [pltpu.VMEM((rows, kb), BF16)],
        ),
        out_shape=[
            jax.ShapeDtypeStruct((rows, cols), F32),
            jax.ShapeDtypeStruct((rows, cols), F32),
            jax.ShapeDtypeStruct((heads, HEAD_DIM + 8, HEAD_DIM), F32),
        ],
        compiler_params=params(),
        name="mixer",
    )(src, *parts, wq, wf, wv, gap)


def readout_kernel(inside_ref, query_ref, state_ref, gain_ref, out_ref):
    q_high, q_low = halves(query_ref[...])
    s_high, s_low = halves(state_ref[0])
    total = inside_ref[...] + mm(
        jnp.concatenate([q_high, q_low, q_high], axis=1),
        jnp.concatenate([s_high, s_high, s_low], axis=1),
        ((1,), (1,)),
    )
    out_ref[...] = normed(total, gain_ref[...]).astype(BF16)


def readout(inside, query, state, gain):
    rows, cols = inside.shape
    block = pl.BlockSpec((rows, HEAD_DIM), lambda h: (0, h))
    return pl.pallas_call(
        readout_kernel,
        grid=(cols // HEAD_DIM,),
        in_specs=[
            block,
            block,
            pl.BlockSpec((1, HEAD_DIM, HEAD_DIM), lambda h: (h, 0, 0)),
            pl.BlockSpec((1, HEAD_DIM), lambda h: (0, h)),
        ],
        out_specs=block,
        out_shape=jax.ShapeDtypeStruct((rows, cols), BF16),
        compiler_params=params(),
        name="readout",
    )(inside, query, state, gain)


def pieces(packed):
    return packed[:, HEAD_DIM : HEAD_DIM + 1, :], packed[:, :HEAD_DIM, :]


def link(earlier, later):
    return earlier[0] + later[0], jnp.exp(later[0]) * earlier[1] + later[1]


def pack(part):
    heads = part[1].shape[0]
    return jnp.concatenate(
        [part[1], jnp.broadcast_to(part[0], (heads, 8, HEAD_DIM))], axis=1
    )


def masked(flag, part):
    return jax.tree.map(lambda a: jnp.where(flag, a, 0.0), part)


def both_cores(a):
    return lax.ppermute(a, "ep_2", [(0, 1), (1, 0)])


def along_rows(packed):
    core = lax.axis_index("ep_2")
    other = both_cores(packed)
    is_second = core == 1
    low = jnp.where(is_second, other, packed)
    high = jnp.where(is_second, packed, other)
    half = packed.shape[0] // 2
    mine = lambda a: lax.dynamic_slice_in_dim(a, core * half, half, 0)
    chip = link(pieces(mine(low)), pieces(mine(high)))
    count = lax.axis_size("ep_1")
    sent = pack(chip)
    came = [
        lax.ppermute(sent, "ep_1", [(i, (i + d) % count) for i in range(count)])
        for d in range(count - 1, 0, -1)
    ]
    return low, chip, came


def along_planes(chip, came):
    row = lax.axis_index("ep_1")
    before = after = None
    for k, part in enumerate(came):
        d = len(came) - k
        early = masked(row >= d, pieces(part))
        late = masked(row < d, pieces(part))
        before = early if before is None else link(before, early)
        after = late if after is None else link(after, late)
    plane = pack(link(link(before, chip), after))
    count = lax.axis_size("ep_0")
    planes = [
        lax.ppermute(plane, "ep_0", [(i, (i + d) % count) for i in range(count)])
        for d in range(count - 1, 0, -1)
    ]
    return before, planes


def arriving_state(low, before, planes):
    is_second = lax.axis_index("ep_2") == 1
    at = lax.axis_index("ep_0")
    total = None
    for k, part in enumerate(planes):
        part = masked(at >= len(planes) - k, pieces(part))
        total = part if total is None else link(total, part)
    state = link(total, before)[1]
    swapped = both_cores(state)
    entering = jnp.concatenate(
        [jnp.where(is_second, swapped, state), jnp.where(is_second, state, swapped)], axis=0
    )
    first_core = pieces(low)
    return jnp.where(is_second, jnp.exp(first_core[0]) * entering + first_core[1], entering)


def hidden_kernel(own_ref, near_ref, go_ref, uo_ref, gf_ref, uf_ref, out_ref, gate, up):
    step = pl.program_id(0)

    @pl.when(step == 0)
    def _():
        gate[...] = jnp.zeros_like(gate)
        up[...] = jnp.zeros_like(up)

    rows = jnp.concatenate([own_ref[...], near_ref[...]], axis=0)
    n = go_ref.shape[1]
    gate[:, :n] += mm(rows, go_ref[...])
    gate[:, n:] += mm(rows, gf_ref[...])
    up[:, :n] += mm(rows, uo_ref[...])
    up[:, n:] += mm(rows, uf_ref[...])

    @pl.when(step == pl.num_programs(0) - 1)
    def _():
        gated = jnp.minimum(gate[...], CLAMP_LIMIT)
        opened = jnp.clip(up[...], -CLAMP_LIMIT, CLAMP_LIMIT)
        out_ref[...] = (
            (opened + 1.0) * gated * jax.nn.sigmoid(SWISH_SLOPE * gated)
        ).astype(BF16)


def hidden_units(own, near, half, weights):
    count = own.shape[0]
    width, n = weights[0].shape
    kb = 1024
    weight = pl.BlockSpec((kb, n), lambda i: (i, 0))
    return pl.pallas_call(
        hidden_kernel,
        grid=(width // kb,),
        in_specs=[
            pl.BlockSpec((count, kb), lambda i: (0, i + half * (width // kb))),
            pl.BlockSpec((count, kb), lambda i: (0, i)),
            weight,
            weight,
            weight,
            weight,
        ],
        out_specs=pl.BlockSpec((2 * count, 2 * n), lambda i: (0, 0)),
        out_shape=jax.ShapeDtypeStruct((2 * count, 2 * n), BF16),
        scratch_shapes=[pltpu.VMEM((2 * count, 2 * n), F32)] * 2,
        compiler_params=params(),
        name="hidden",
    )(own, near, *weights)


def down_kernel(src, h_own, h_near, h_far, h_opp, down_ref, out_ref):
    k = pl.program_id(0)
    n = down_ref.shape[0] // 4
    rows = out_ref.shape[0]
    cols = down_ref.shape[1]
    unit = lambda s: down_ref[pl.ds(pl.multiple_of(s * n, n), n), :]
    for pair, refs in enumerate(((h_own, h_near), (h_far, h_opp))):

        @pl.when(k == pair)
        def _():
            both = []
            for j, ref in enumerate(refs):
                s = src[2 * pair + j]
                both.append(mm(ref[:, :n], unit(s)) + mm(ref[:, n:], unit(3 - s)))
            out_ref[:, :cols] = (both[0][:rows] + both[1][rows:]).astype(BF16)
            out_ref[:, cols:] = (both[0][rows:] + both[1][:rows]).astype(BF16)


def down_rows(src, parts, down):
    both, width = parts[0].shape
    cols = down.shape[1]
    whole = lambda k, s: (0, 0)
    return pl.pallas_call(
        down_kernel,
        grid_spec=pltpu.PrefetchScalarGridSpec(
            num_scalar_prefetch=1,
            grid=(2,),
            in_specs=[pl.BlockSpec((both, width), whole)] * 4 + [pl.BlockSpec(down.shape, whole)],
            out_specs=pl.BlockSpec((both // 2, 2 * cols), lambda k, s: (0, k)),
        ),
        out_shape=jax.ShapeDtypeStruct((both // 2, 4 * cols), BF16),
        compiler_params=params(),
        name="down",
    )(src, *parts, down)


def places_kernel(src, routes_ref, logits_ref, out_ref):
    experts = logits_ref.shape[1]
    first, second, count, before = chosen(routes_ref[0], experts)
    logits = logits_ref[0].astype(F32)
    l0 = jnp.sum(jnp.where(first, logits, 0.0), axis=0, keepdims=True)
    l1 = jnp.sum(jnp.where(second, logits, 0.0), axis=0, keepdims=True)
    w0 = 1.0 / (1.0 + jnp.exp(l1 - l0))
    w1 = 1.0 / (1.0 + jnp.exp(l0 - l1))
    weight = jnp.where(first, w0, 0.0) + jnp.where(second, w1, 0.0)
    both = [slot_matrix(weight, before, count, half) for half in range(2)]
    place = jnp.concatenate(both, axis=0).T
    out_ref[0] = jnp.concatenate(halves(place), axis=0)


def places(src, routes, logits):
    experts, toks = logits.shape[1:]
    return pl.pallas_call(
        places_kernel,
        grid_spec=pltpu.PrefetchScalarGridSpec(
            num_scalar_prefetch=1,
            grid=(4,),
            in_specs=[
                pl.BlockSpec((1, 2, toks), lambda k, s: (s[k], 0, 0)),
                pl.BlockSpec((1, experts, toks), lambda k, s: (k, 0, 0)),
            ],
            out_specs=pl.BlockSpec((1, 2 * toks, experts * CAP), lambda k, s: (k, 0, 0)),
        ),
        out_shape=jax.ShapeDtypeStruct((4, 2 * toks, experts * CAP), BF16),
        compiler_params=params(),
        name="places",
    )(src, routes, logits)


def combine_kernel(src, low_ref, high_ref, place_ref, out_ref):
    slots = low_ref.shape[0]
    total = mm(place_ref[0, :, :slots], low_ref[...]) + mm(place_ref[0, :, slots:], high_ref[...])
    toks = out_ref.shape[0]
    out_ref[...] = (total[:toks] + total[toks:]).astype(BF16)


def combined(src, low, high, place):
    slots = low.shape[0]
    cols = low.shape[1] // 4
    toks = place.shape[1] // 2
    res = pl.BlockSpec((slots, cols), lambda k, s: (0, k))
    return pl.pallas_call(
        combine_kernel,
        grid_spec=pltpu.PrefetchScalarGridSpec(
            num_scalar_prefetch=1,
            grid=(4,),
            in_specs=[
                res,
                res,
                pl.BlockSpec((1,) + place.shape[1:], lambda k, s: (k, 0, 0)),
            ],
            out_specs=pl.BlockSpec((toks, cols), lambda k, s: (s[k], 0)),
        ),
        out_shape=jax.ShapeDtypeStruct((4 * toks, cols), BF16),
        compiler_params=params(),
        name="combine",
    )(src, low, high, place)


NEAR = [(i, i ^ 1) for i in range(4)]
FAR = [(i, 3 - i) for i in range(4)]
OPPOSITE = [(i, i ^ 2) for i in range(4)]


def to_near(a):
    return lax.ppermute(a, "tp", NEAR)


def to_far(a):
    return lax.ppermute(a, "tp", FAR)


def shared(a, direct=True):
    far = to_far(a)
    near = to_near(a)
    return a, near, far, (lax.ppermute(a, "tp", OPPOSITE) if direct else to_near(far))


def swap(a):
    experts = 32
    rows, cols = a.shape
    out = lax.all_to_all(
        a.reshape(experts, rows // experts, cols), EP, split_axis=0, concat_axis=0, tiled=True
    )
    return out.reshape(rows, cols)


def per_device(
    mix_input,
    moe_input,
    norm_mix,
    query_weight,
    forget_weight,
    value_weight,
    forget_gap,
    norm_out,
    norm_moe,
    router_weight,
    expert_gate,
    expert_up,
    expert_down,
    routes,
):
    toks = moe_input.shape[0]
    x = lax.axis_index("tp").astype(jnp.int32)
    src = jnp.stack([x, x ^ 1, 3 - x, x ^ 2])
    by_block = routes.reshape(4, toks, 2).transpose(0, 2, 1)
    router = router_weight.T

    rows_a = normed(mix_input, norm_mix).astype(BF16)
    group_a = shared(rows_a, direct=False)
    rows_b, own = front(src, moe_input, norm_moe.reshape(1, -1), by_block, router_weight.shape[1])
    own_rows = swap(own)
    rows_near = to_near(rows_b)
    gate_far = to_far(expert_gate[0])
    up_far = to_far(expert_up[0])
    logits, low, high = refill(src, rows_b, rows_near, router, by_block)
    low_rows = swap(low)
    high_rows = swap(high)
    logits = jnp.concatenate([logits, to_far(logits)])
    place = places(src, by_block, logits)

    inside, query, packed = mixer(
        src, group_a, query_weight, forget_weight, value_weight, forget_gap.reshape(1, -1)
    )
    first_core, chip, came = along_rows(packed)

    low_rows, packed = lax.optimization_barrier((low_rows, packed))
    weights = (expert_gate[0], expert_up[0], gate_far, up_far)
    h_low = hidden_units(own_rows, low_rows, 0, weights)
    h_low = shared(h_low)
    high_rows, low_own = lax.optimization_barrier((high_rows, h_low[0]))
    h_high = hidden_units(own_rows, high_rows, 1, weights)
    h_high = shared(h_high)
    opp, high_own = lax.optimization_barrier((h_low[3], h_high[0]))
    down_low = down_rows(src, (low_own,) + h_low[1:3] + (opp,), expert_down[0])
    back_low = swap(down_low)
    came, _ = lax.optimization_barrier((came, down_low))
    before, planes = along_planes(chip, came)
    down_high = down_rows(src, (high_own,) + h_high[1:], expert_down[0])
    back_high = swap(down_high)
    planes, _ = lax.optimization_barrier((planes, down_high))

    state = arriving_state(first_core, before, planes)
    mixer_out = readout(inside, query, state, norm_out.reshape(1, -1))
    expert_out = combined(src, back_low, back_high, place)
    return (mixer_out, expert_out)


def solution(mesh):
    finer = Mesh(mesh.devices.reshape(4, 4, 2, mesh.shape["tp"]), ("ep_0", "ep_1", "ep_2", "tp"))
    placed = (
        P(EP_TP, None),
        P(EP_TP, None),
        P(),
        P(None, "tp"),
        P(None, "tp"),
        P(None, "tp"),
        P("tp"),
        P("tp"),
        P(),
        P(),
        P(EP, None, "tp"),
        P(EP, None, "tp"),
        P(EP, None, "tp"),
        P(EP, None),
    )

    return jax.shard_map(
        per_device,
        mesh=finer,
        in_specs=placed,
        out_specs=(P(EP, "tp"), P(EP, "tp")),
        check_vma=False,
    )
```

```python
import functools

import jax
import jax.numpy as jnp
from jax import lax
from jax.experimental import pallas as pl
from jax.experimental.pallas import tpu as pltpu
from jax.sharding import Mesh
from jax.sharding import PartitionSpec as P

HEAD_DIM = 128

CAP = 16
HALF = 8
EP = ("ep_0", "ep_1", "ep_2")
EP_TP = ("ep_0", "ep_1", "ep_2", "tp")

EPSILON = 1e-06
CLAMP_LIMIT = 7.0
SWISH_SLOPE = 1.702
F32 = jnp.float32
BF16 = jnp.bfloat16


def mm(a, b, contract=((1,), (0,))):
    return lax.dot_general(a, b, (contract, ((), ())), preferred_element_type=F32)


def halves(a):
    high = a.astype(BF16)
    return high, (a - high.astype(F32)).astype(BF16)


def params(mib=56, axes=("arbitrary",)):
    return pltpu.CompilerParams(vmem_limit_bytes=mib << 20, dimension_semantics=axes)


def normed(row_data, gain_vec):
    as_float = row_data.astype(F32)
    scale = lax.rsqrt(jnp.mean(as_float * as_float, axis=-1, keepdims=True) + EPSILON)
    return as_float * scale * gain_vec


def chosen(routes, experts):
    toks = routes.shape[1]
    ids = lax.broadcasted_iota(jnp.int32, (experts, toks), 0)
    first = routes[0:1, :] == ids
    second = routes[1:2, :] == ids
    count = jnp.where(first | second, 1.0, 0.0)
    earlier = (
        lax.broadcasted_iota(jnp.int32, (toks, toks), 0)
        < lax.broadcasted_iota(jnp.int32, (toks, toks), 1)
    )
    before = mm(count.astype(BF16), jnp.where(earlier, 1.0, 0.0).astype(BF16))
    return first, second, count, before


def slot_matrix(weight, before, count, half):
    experts, toks = weight.shape
    place = lax.broadcasted_iota(jnp.int32, (experts, HALF, toks), 1) + half * HALF
    here = (before[:, None, :] == place.astype(F32)) & (count[:, None, :] > 0.5)
    return jnp.where(here, weight[:, None, :], 0.0).reshape(experts * HALF, toks)


def fill(routes, rows, experts):
    _, _, count, before = chosen(routes, experts)
    pick = [slot_matrix(count, before, count, half) for half in range(2)]
    both = mm(jnp.concatenate(pick, axis=0).astype(BF16), rows).astype(BF16)
    return both[: experts * HALF], both[experts * HALF :]


def front_kernel(src, x_ref, gain_ref, routes_ref, rows_ref, buf_ref, *, group):
    step = pl.program_id(0)
    width = x_ref.shape[1]

    @pl.when(step == 0)
    def _():
        rows_ref[...] = normed(x_ref[...], gain_ref[...]).astype(BF16)

    low, high = fill(routes_ref[0] - step * group, rows_ref[...], group)
    buf_ref[:, :width] = low
    buf_ref[:, width:] = high


def refill_kernel(src, own_ref, rows_ref, router_ref, routes_ref, logits_ref, low_ref, high_ref, *, group):
    step = pl.program_id(0)

    @pl.when(step == 0)
    def _():
        for k, ref in enumerate((own_ref, rows_ref)):
            logits_ref[k] = mm(router_ref[...], ref[...], ((1,), (1,))).astype(BF16)

    low_ref[...], high_ref[...] = fill(routes_ref[0] - step * group, rows_ref[...], group)


def front(src, x, gain, routes, experts):
    toks, width = x.shape
    group = 16
    whole = lambda i, s: (0, 0)
    return pl.pallas_call(
        functools.partial(front_kernel, group=group),
        grid_spec=pltpu.PrefetchScalarGridSpec(
            num_scalar_prefetch=1,
            grid=(experts // group,),
            in_specs=[
                pl.BlockSpec((toks, width), whole),
                pl.BlockSpec((1, width), whole),
                pl.BlockSpec((1, 2, toks), lambda i, s: (s[0], 0, 0)),
            ],
            out_specs=[
                pl.BlockSpec((toks, width), whole),
                pl.BlockSpec((group * HALF, 2 * width), lambda i, s: (i, 0)),
            ],
        ),
        out_shape=[
            jax.ShapeDtypeStruct((toks, width), BF16),
            jax.ShapeDtypeStruct((experts * HALF, 2 * width), BF16),
        ],
        compiler_params=params(),
        name="front",
    )(src, x, gain, routes)


def refill(src, own, rows, router, routes):
    toks, width = rows.shape
    experts = router.shape[0]
    group = 16
    whole = lambda i, s: (0, 0)
    return pl.pallas_call(
        functools.partial(refill_kernel, group=group),
        grid_spec=pltpu.PrefetchScalarGridSpec(
            num_scalar_prefetch=1,
            grid=(experts // group,),
            in_specs=[
                pl.BlockSpec((toks, width), whole),
                pl.BlockSpec((toks, width), whole),
                pl.BlockSpec(router.shape, whole),
                pl.BlockSpec((1, 2, toks), lambda i, s: (s[1], 0, 0)),
            ],
            out_specs=[
                pl.BlockSpec((2, experts, toks), lambda i, s: (0, 0, 0)),
                pl.BlockSpec((group * HALF, width), lambda i, s: (i, 0)),
                pl.BlockSpec((group * HALF, width), lambda i, s: (i, 0)),
            ],
        ),
        out_shape=[
            jax.ShapeDtypeStruct((2, experts, toks), BF16),
            jax.ShapeDtypeStruct((experts * HALF, width), BF16),
            jax.ShapeDtypeStruct((experts * HALF, width), BF16),
        ],
        compiler_params=params(),
        name="refill",
    )(src, own, rows, router, routes)


def mixer_kernel(
    src, a0, a1, a2, a3, q_ref, f_ref, v_ref, gap_ref, inside_ref, query_ref, packed_ref, qa, fa, va, group
):
    step = pl.program_id(0)

    @pl.when(step == 0)
    def _():
        qa[...] = jnp.zeros_like(qa)
        fa[...] = jnp.zeros_like(fa)
        va[...] = jnp.zeros_like(va)

    toks = a0.shape[0]
    for k, part in enumerate((a0, a1, a2, a3)):
        group[pl.ds(pl.multiple_of(src[k] * toks, toks), toks), :] = part[...]
    a = group[...]
    qa[...] += mm(a, q_ref[...])
    fa[...] += mm(a, f_ref[...])
    va[...] += mm(a, v_ref[...])

    @pl.when(step == pl.num_programs(0) - 1)
    def _():
        rows = a.shape[0]
        causal = (
            lax.broadcasted_iota(jnp.int32, (rows, rows), 0)
            >= lax.broadcasted_iota(jnp.int32, (rows, rows), 1)
        )
        ones = jnp.where(causal[:toks, :toks], 1.0, 0.0).astype(BF16)
        shut = gap_ref[...] * jax.nn.sigmoid(-fa[...])
        fa[...] = jnp.log1p(-shut)
        cols = shut.shape[1]
        base = None
        for k in range(rows // toks):
            part = fa[k * toks : (k + 1) * toks, :]
            high = part.astype(BF16)
            rest = part - high.astype(F32)
            mid = rest.astype(BF16)
            low = (rest - mid.astype(F32)).astype(BF16)
            sums = mm(ones, jnp.concatenate([high, mid, low], axis=1))
            sums = sums[:, :cols] + sums[:, cols : 2 * cols] + sums[:, 2 * cols :]
            sums = sums if base is None else sums + base
            base = sums[toks - 1 :, :]
            fa[k * toks : (k + 1) * toks, :] = sums
        sums = fa[...]
        last = sums[rows - 1 :, :]
        query_ref[...] = qa[...] * jnp.exp(sums)
        keys = shut * jnp.exp(-sums)
        late = shut * jnp.exp(last - sums)
        half = rows // 2
        for h in range(packed_ref.shape[0]):
            at = slice(h * HEAD_DIM, (h + 1) * HEAD_DIM)
            q_high, q_low = halves(query_ref[:, at])
            k_high, k_low = halves(keys[:, at])
            v_high, v_low = halves(va[:, at])
            l_high, l_low = halves(late[:, at])
            left = jnp.concatenate([q_high, q_low, q_high], axis=1)
            right = jnp.concatenate([k_high, k_high, k_low], axis=1)
            values = jnp.concatenate([v_high, v_low], axis=1)
            for k in range(2):
                end = (k + 1) * half
                scores = mm(left[end - half : end], right[:end], ((1,), (1,)))
                s_high, s_low = halves(jnp.where(causal[end - half : end, :end], scores, 0.0))
                part = mm(s_high, values[:end])
                part = part[:, :HEAD_DIM] + part[:, HEAD_DIM:] + mm(s_low, v_high[:end])
                inside_ref[end - half : end, at] = part
            outer = mm(values, jnp.concatenate([l_high, l_low], axis=1), ((0,), (0,)))
            packed_ref[h, :HEAD_DIM, :] = (
                outer[:HEAD_DIM, :HEAD_DIM]
                + outer[:HEAD_DIM, HEAD_DIM:]
                + outer[HEAD_DIM:, :HEAD_DIM]
            )
            packed_ref[h, HEAD_DIM:, :] = jnp.broadcast_to(last[:, at], (8, HEAD_DIM))


def mixer(src, parts, wq, wf, wv, gap):
    toks, width = parts[0].shape
    rows = 4 * toks
    cols = wq.shape[1]
    heads = cols // HEAD_DIM
    kb = 512
    fixed = lambda i, s: (0, 0)
    weight = pl.BlockSpec((kb, cols), lambda i, s: (i, 0))
    return pl.pallas_call(
        mixer_kernel,
        grid_spec=pltpu.PrefetchScalarGridSpec(
            num_scalar_prefetch=1,
            grid=(width // kb,),
            in_specs=[pl.BlockSpec((toks, kb), lambda i, s: (0, i))] * 4
            + [weight, weight, weight, pl.BlockSpec((1, cols), fixed)],
            out_specs=[
                pl.BlockSpec((rows, cols), fixed),
                pl.BlockSpec((rows, cols), fixed),
                pl.BlockSpec((heads, HEAD_DIM + 8, HEAD_DIM), lambda i, s: (0, 0, 0)),
            ],
            scratch_shapes=[pltpu.VMEM((rows, cols), F32)] * 3 + [pltpu.VMEM((rows, kb), BF16)],
        ),
        out_shape=[
            jax.ShapeDtypeStruct((rows, cols), F32),
            jax.ShapeDtypeStruct((rows, cols), F32),
            jax.ShapeDtypeStruct((heads, HEAD_DIM + 8, HEAD_DIM), F32),
        ],
        compiler_params=params(28),
        name="mixer",
    )(src, *parts, wq, wf, wv, gap)


def readout_kernel(inside_ref, query_ref, state_ref, gain_ref, out_ref):
    q_high, q_low = halves(query_ref[...])
    s_high, s_low = halves(state_ref[0])
    total = inside_ref[...] + mm(
        jnp.concatenate([q_high, q_low, q_high], axis=1),
        jnp.concatenate([s_high, s_high, s_low], axis=1),
        ((1,), (1,)),
    )
    out_ref[...] = normed(total, gain_ref[...]).astype(BF16)


def readout(inside, query, state, gain):
    rows, cols = inside.shape
    block = pl.BlockSpec((rows, HEAD_DIM), lambda h: (0, h))
    return pl.pallas_call(
        readout_kernel,
        grid=(cols // HEAD_DIM,),
        in_specs=[
            block,
            block,
            pl.BlockSpec((1, HEAD_DIM, HEAD_DIM), lambda h: (h, 0, 0)),
            pl.BlockSpec((1, HEAD_DIM), lambda h: (0, h)),
        ],
        out_specs=block,
        out_shape=jax.ShapeDtypeStruct((rows, cols), BF16),
        compiler_params=params(8),
        name="readout",
    )(inside, query, state, gain)


def pieces(packed):
    return packed[:, HEAD_DIM : HEAD_DIM + 1, :], packed[:, :HEAD_DIM, :]


def link(earlier, later):
    return earlier[0] + later[0], jnp.exp(later[0]) * earlier[1] + later[1]


def pack(part):
    heads = part[1].shape[0]
    return jnp.concatenate(
        [part[1], jnp.broadcast_to(part[0], (heads, 8, HEAD_DIM))], axis=1
    )


def masked(flag, part):
    return jax.tree.map(lambda a: jnp.where(flag, a, 0.0), part)


def both_cores(a):
    return lax.ppermute(a, "ep_2", [(0, 1), (1, 0)])


def along_rows(packed):
    core = lax.axis_index("ep_2")
    other = both_cores(packed)
    is_second = core == 1
    low = jnp.where(is_second, other, packed)
    high = jnp.where(is_second, packed, other)
    half = packed.shape[0] // 2
    mine = lambda a: lax.dynamic_slice_in_dim(a, core * half, half, 0)
    chip = link(pieces(mine(low)), pieces(mine(high)))
    count = lax.axis_size("ep_1")
    sent = pack(chip)
    came = [
        lax.ppermute(sent, "ep_1", [(i, (i + d) % count) for i in range(count)])
        for d in range(count - 1, 0, -1)
    ]
    return low, chip, came


def along_planes(chip, came):
    row = lax.axis_index("ep_1")
    before = after = None
    for k, part in enumerate(came):
        d = len(came) - k
        early = masked(row >= d, pieces(part))
        late = masked(row < d, pieces(part))
        before = early if before is None else link(before, early)
        after = late if after is None else link(after, late)
    plane = pack(link(link(before, chip), after))
    count = lax.axis_size("ep_0")
    planes = [
        lax.ppermute(plane, "ep_0", [(i, (i + d) % count) for i in range(count)])
        for d in range(count - 1, 0, -1)
    ]
    return before, planes


def arriving_state(low, before, planes):
    is_second = lax.axis_index("ep_2") == 1
    at = lax.axis_index("ep_0")
    total = None
    for k, part in enumerate(planes):
        part = masked(at >= len(planes) - k, pieces(part))
        total = part if total is None else link(total, part)
    state = link(total, before)[1]
    swapped = both_cores(state)
    entering = jnp.concatenate(
        [jnp.where(is_second, swapped, state), jnp.where(is_second, state, swapped)], axis=0
    )
    first_core = pieces(low)
    return jnp.where(is_second, jnp.exp(first_core[0]) * entering + first_core[1], entering)


def hidden_kernel(own_ref, near_ref, go_ref, uo_ref, gf_ref, uf_ref, out_ref, gate, up):
    step = pl.program_id(0)

    @pl.when(step == 0)
    def _():
        gate[...] = jnp.zeros_like(gate)
        up[...] = jnp.zeros_like(up)

    rows = jnp.concatenate([own_ref[...], near_ref[...]], axis=0)
    n = go_ref.shape[1]
    gate[:, :n] += mm(rows, go_ref[...])
    gate[:, n:] += mm(rows, gf_ref[...])
    up[:, :n] += mm(rows, uo_ref[...])
    up[:, n:] += mm(rows, uf_ref[...])

    @pl.when(step == pl.num_programs(0) - 1)
    def _():
        gated = jnp.minimum(gate[...], CLAMP_LIMIT)
        opened = jnp.clip(up[...], -CLAMP_LIMIT, CLAMP_LIMIT)
        out_ref[...] = (
            (opened + 1.0) * gated * jax.nn.sigmoid(SWISH_SLOPE * gated)
        ).astype(BF16)


def hidden_units(own, near, half, weights):
    count = own.shape[0]
    width, n = weights[0].shape
    kb = 1024
    weight = pl.BlockSpec((kb, n), lambda i: (i, 0))
    return pl.pallas_call(
        hidden_kernel,
        grid=(width // kb,),
        in_specs=[
            pl.BlockSpec((count, kb), lambda i: (0, i + half * (width // kb))),
            pl.BlockSpec((count, kb), lambda i: (0, i)),
            weight,
            weight,
            weight,
            weight,
        ],
        out_specs=pl.BlockSpec((2 * count, 2 * n), lambda i: (0, 0)),
        out_shape=jax.ShapeDtypeStruct((2 * count, 2 * n), BF16),
        scratch_shapes=[pltpu.VMEM((2 * count, 2 * n), F32)] * 2,
        compiler_params=params(14),
        name="hidden",
    )(own, near, *weights)


def down_kernel(src, h_own, h_near, h_far, h_opp, down_ref, out_ref):
    k = pl.program_id(0)
    n = down_ref.shape[0] // 4
    rows = out_ref.shape[0]
    cols = down_ref.shape[1]
    unit = lambda s: down_ref[pl.ds(pl.multiple_of(s * n, n), n), :]
    for pair, refs in enumerate(((h_own, h_near), (h_far, h_opp))):

        @pl.when(k == pair)
        def _():
            both = []
            for j, ref in enumerate(refs):
                s = src[2 * pair + j]
                both.append(mm(ref[:, :n], unit(s)) + mm(ref[:, n:], unit(3 - s)))
            out_ref[:, :cols] = (both[0][:rows] + both[1][rows:]).astype(BF16)
            out_ref[:, cols:] = (both[0][rows:] + both[1][:rows]).astype(BF16)


def down_rows(src, parts, down):
    both, width = parts[0].shape
    cols = down.shape[1]
    whole = lambda k, s: (0, 0)
    return pl.pallas_call(
        down_kernel,
        grid_spec=pltpu.PrefetchScalarGridSpec(
            num_scalar_prefetch=1,
            grid=(2,),
            in_specs=[pl.BlockSpec((both, width), whole)] * 4 + [pl.BlockSpec(down.shape, whole)],
            out_specs=pl.BlockSpec((both // 2, 2 * cols), lambda k, s: (0, k)),
        ),
        out_shape=jax.ShapeDtypeStruct((both // 2, 4 * cols), BF16),
        compiler_params=params(20),
        name="down",
    )(src, *parts, down)


def places_kernel(src, routes_ref, logits_ref, out_ref):
    experts = logits_ref.shape[1]
    first, second, count, before = chosen(routes_ref[0], experts)
    logits = logits_ref[0].astype(F32)
    l0 = jnp.sum(jnp.where(first, logits, 0.0), axis=0, keepdims=True)
    l1 = jnp.sum(jnp.where(second, logits, 0.0), axis=0, keepdims=True)
    w0 = 1.0 / (1.0 + jnp.exp(l1 - l0))
    w1 = 1.0 / (1.0 + jnp.exp(l0 - l1))
    weight = jnp.where(first, w0, 0.0) + jnp.where(second, w1, 0.0)
    both = [slot_matrix(weight, before, count, half) for half in range(2)]
    place = jnp.concatenate(both, axis=0).T
    out_ref[0] = jnp.concatenate(halves(place), axis=0)


def places(src, routes, logits):
    experts, toks = logits.shape[1:]
    return pl.pallas_call(
        places_kernel,
        grid_spec=pltpu.PrefetchScalarGridSpec(
            num_scalar_prefetch=1,
            grid=(4,),
            in_specs=[
                pl.BlockSpec((1, 2, toks), lambda k, s: (s[k], 0, 0)),
                pl.BlockSpec((1, experts, toks), lambda k, s: (k, 0, 0)),
            ],
            out_specs=pl.BlockSpec((1, 2 * toks, experts * CAP), lambda k, s: (k, 0, 0)),
        ),
        out_shape=jax.ShapeDtypeStruct((4, 2 * toks, experts * CAP), BF16),
        compiler_params=params(8),
        name="places",
    )(src, routes, logits)


def combine_kernel(src, low_ref, high_ref, place_ref, out_ref):
    slots = low_ref.shape[0]
    total = mm(place_ref[0, :, :slots], low_ref[...]) + mm(place_ref[0, :, slots:], high_ref[...])
    toks = out_ref.shape[0]
    out_ref[...] = (total[:toks] + total[toks:]).astype(BF16)


def combined(src, low, high, place):
    slots = low.shape[0]
    cols = low.shape[1] // 4
    toks = place.shape[1] // 2
    res = pl.BlockSpec((slots, cols), lambda k, s: (0, k))
    return pl.pallas_call(
        combine_kernel,
        grid_spec=pltpu.PrefetchScalarGridSpec(
            num_scalar_prefetch=1,
            grid=(4,),
            in_specs=[
                res,
                res,
                pl.BlockSpec((1,) + place.shape[1:], lambda k, s: (k, 0, 0)),
            ],
            out_specs=pl.BlockSpec((toks, cols), lambda k, s: (s[k], 0)),
        ),
        out_shape=jax.ShapeDtypeStruct((4 * toks, cols), BF16),
        compiler_params=params(10),
        name="combine",
    )(src, low, high, place)


NEAR = [(i, i ^ 1) for i in range(4)]
FAR = [(i, 3 - i) for i in range(4)]
OPPOSITE = [(i, i ^ 2) for i in range(4)]


def to_near(a):
    return lax.ppermute(a, "tp", NEAR)


def to_far(a):
    return lax.ppermute(a, "tp", FAR)


def shared(a, direct=True):
    far = to_far(a)
    near = to_near(a)
    return a, near, far, (lax.ppermute(a, "tp", OPPOSITE) if direct else to_near(far))


def swap(a):
    experts = 32
    rows, cols = a.shape
    out = lax.all_to_all(
        a.reshape(experts, rows // experts, cols), EP, split_axis=0, concat_axis=0, tiled=True
    )
    return out.reshape(rows, cols)


def per_device(
    mix_input,
    moe_input,
    norm_mix,
    query_weight,
    forget_weight,
    value_weight,
    forget_gap,
    norm_out,
    norm_moe,
    router_weight,
    expert_gate,
    expert_up,
    expert_down,
    routes,
):
    toks = moe_input.shape[0]
    x = lax.axis_index("tp").astype(jnp.int32)
    src = jnp.stack([x, x ^ 1, 3 - x, x ^ 2])
    by_block = routes.reshape(4, toks, 2).transpose(0, 2, 1)
    router = router_weight.T

    rows_a = normed(mix_input, norm_mix).astype(BF16)
    group_a = shared(rows_a, direct=False)
    rows_b, own = front(src, moe_input, norm_moe.reshape(1, -1), by_block, router_weight.shape[1])
    own_rows = swap(own)
    rows_near = to_near(rows_b)
    gate_far = to_far(expert_gate[0])
    up_far = to_far(expert_up[0])
    logits, low, high = refill(src, rows_b, rows_near, router, by_block)
    low_rows = swap(low)
    high_rows = swap(high)
    logits = jnp.concatenate([logits, to_far(logits)])
    place = places(src, by_block, logits)

    inside, query, packed = mixer(
        src, group_a, query_weight, forget_weight, value_weight, forget_gap.reshape(1, -1)
    )
    first_core, chip, came = along_rows(packed)

    low_rows, packed = lax.optimization_barrier((low_rows, packed))
    weights = (expert_gate[0], expert_up[0], gate_far, up_far)
    h_low = hidden_units(own_rows, low_rows, 0, weights)
    h_low = shared(h_low)
    high_rows, low_own = lax.optimization_barrier((high_rows, h_low[0]))
    h_high = hidden_units(own_rows, high_rows, 1, weights)
    h_high = shared(h_high)
    opp, high_own = lax.optimization_barrier((h_low[3], h_high[0]))
    down_low = down_rows(src, (low_own,) + h_low[1:3] + (opp,), expert_down[0])
    back_low = swap(down_low)
    came, _ = lax.optimization_barrier((came, down_low))
    before, planes = along_planes(chip, came)
    down_high = down_rows(src, (high_own,) + h_high[1:], expert_down[0])
    back_high = swap(down_high)
    planes, _ = lax.optimization_barrier((planes, down_high))

    state = arriving_state(first_core, before, planes)
    mixer_out = readout(inside, query, state, norm_out.reshape(1, -1))
    expert_out = combined(src, back_low, back_high, place)
    return (mixer_out, expert_out)


def solution(mesh):
    finer = Mesh(mesh.devices.reshape(4, 4, 2, mesh.shape["tp"]), ("ep_0", "ep_1", "ep_2", "tp"))
    placed = (
        P(EP_TP, None),
        P(EP_TP, None),
        P(),
        P(None, "tp"),
        P(None, "tp"),
        P(None, "tp"),
        P("tp"),
        P("tp"),
        P(),
        P(),
        P(EP, None, "tp"),
        P(EP, None, "tp"),
        P(EP, None, "tp"),
        P(EP, None),
    )

    return jax.shard_map(
        per_device,
        mesh=finer,
        in_specs=placed,
        out_specs=(P(EP, "tp"), P(EP, "tp")),
        check_vma=False,
    )
```

```python
import functools

import jax
import jax.numpy as jnp
from jax import lax
from jax.experimental import pallas as pl
from jax.experimental.pallas import tpu as pltpu
from jax.sharding import Mesh
from jax.sharding import PartitionSpec as P

HEAD_DIM = 128

CAP = 16
HALF = 8
EP = ("ep_0", "ep_1", "ep_2")
EP_TP = ("ep_0", "ep_1", "ep_2", "tp")

EPSILON = 1e-06
CLAMP_LIMIT = 7.0
SWISH_SLOPE = 1.702
F32 = jnp.float32
BF16 = jnp.bfloat16


def mm(a, b, contract=((1,), (0,))):
    return lax.dot_general(a, b, (contract, ((), ())), preferred_element_type=F32)


def halves(a):
    high = a.astype(BF16)
    return high, (a - high.astype(F32)).astype(BF16)


def params(mib=56, axes=("arbitrary",)):
    return pltpu.CompilerParams(vmem_limit_bytes=mib << 20, dimension_semantics=axes)


def normed(row_data, gain_vec):
    as_float = row_data.astype(F32)
    scale = lax.rsqrt(jnp.mean(as_float * as_float, axis=-1, keepdims=True) + EPSILON)
    return as_float * scale * gain_vec


def chosen(routes, experts):
    toks = routes.shape[1]
    ids = lax.broadcasted_iota(jnp.int32, (experts, toks), 0)
    first = routes[0:1, :] == ids
    second = routes[1:2, :] == ids
    count = jnp.where(first | second, 1.0, 0.0)
    earlier = (
        lax.broadcasted_iota(jnp.int32, (toks, toks), 0)
        < lax.broadcasted_iota(jnp.int32, (toks, toks), 1)
    )
    before = mm(count.astype(BF16), jnp.where(earlier, 1.0, 0.0).astype(BF16))
    return first, second, count, before


def slot_matrix(weight, before, count, half):
    experts, toks = weight.shape
    place = lax.broadcasted_iota(jnp.int32, (experts, HALF, toks), 1) + half * HALF
    here = (before[:, None, :] == place.astype(F32)) & (count[:, None, :] > 0.5)
    return jnp.where(here, weight[:, None, :], 0.0).reshape(experts * HALF, toks)


def fill(routes, rows, experts):
    _, _, count, before = chosen(routes, experts)
    pick = [slot_matrix(count, before, count, half) for half in range(2)]
    both = mm(jnp.concatenate(pick, axis=0).astype(BF16), rows).astype(BF16)
    return both[: experts * HALF], both[experts * HALF :]


def norm_kernel(x_ref, gain_ref, out_ref):
    out_ref[...] = normed(x_ref[...], gain_ref[...]).astype(BF16)


def norm_rows(x, gain):
    toks, width = x.shape
    block = pl.BlockSpec((toks // 4, width), lambda i: (i, 0))
    return pl.pallas_call(
        norm_kernel,
        grid=(4,),
        in_specs=[block, pl.BlockSpec((1, width), lambda i: (0, 0))],
        out_specs=block,
        out_shape=jax.ShapeDtypeStruct((toks, width), BF16),
        compiler_params=params(),
        name="norm",
    )(x, gain)


def front_kernel(src, x_ref, gain_ref, routes_ref, rows_ref, buf_ref, *, group):
    step = pl.program_id(0)
    width = x_ref.shape[1]

    @pl.when(step == 0)
    def _():
        rows_ref[...] = normed(x_ref[...], gain_ref[...]).astype(BF16)

    low, high = fill(routes_ref[0] - step * group, rows_ref[...], group)
    buf_ref[:, :width] = low
    buf_ref[:, width:] = high


def refill_kernel(src, own_ref, rows_ref, router_ref, routes_ref, logits_ref, low_ref, high_ref, *, group):
    step = pl.program_id(0)

    @pl.when(step == 0)
    def _():
        for k, ref in enumerate((own_ref, rows_ref)):
            logits_ref[k] = mm(router_ref[...], ref[...], ((1,), (1,))).astype(BF16)

    low_ref[...], high_ref[...] = fill(routes_ref[0] - step * group, rows_ref[...], group)


def front(src, x, gain, routes, experts):
    toks, width = x.shape
    group = 16
    whole = lambda i, s: (0, 0)
    return pl.pallas_call(
        functools.partial(front_kernel, group=group),
        grid_spec=pltpu.PrefetchScalarGridSpec(
            num_scalar_prefetch=1,
            grid=(experts // group,),
            in_specs=[
                pl.BlockSpec((toks, width), whole),
                pl.BlockSpec((1, width), whole),
                pl.BlockSpec((1, 2, toks), lambda i, s: (s[0], 0, 0)),
            ],
            out_specs=[
                pl.BlockSpec((toks, width), whole),
                pl.BlockSpec((group * HALF, 2 * width), lambda i, s: (i, 0)),
            ],
        ),
        out_shape=[
            jax.ShapeDtypeStruct((toks, width), BF16),
            jax.ShapeDtypeStruct((experts * HALF, 2 * width), BF16),
        ],
        compiler_params=params(),
        name="front",
    )(src, x, gain, routes)


def refill(src, own, rows, router, routes):
    toks, width = rows.shape
    experts = router.shape[0]
    group = 16
    whole = lambda i, s: (0, 0)
    return pl.pallas_call(
        functools.partial(refill_kernel, group=group),
        grid_spec=pltpu.PrefetchScalarGridSpec(
            num_scalar_prefetch=1,
            grid=(experts // group,),
            in_specs=[
                pl.BlockSpec((toks, width), whole),
                pl.BlockSpec((toks, width), whole),
                pl.BlockSpec(router.shape, whole),
                pl.BlockSpec((1, 2, toks), lambda i, s: (s[1], 0, 0)),
            ],
            out_specs=[
                pl.BlockSpec((2, experts, toks), lambda i, s: (0, 0, 0)),
                pl.BlockSpec((group * HALF, width), lambda i, s: (i, 0)),
                pl.BlockSpec((group * HALF, width), lambda i, s: (i, 0)),
            ],
        ),
        out_shape=[
            jax.ShapeDtypeStruct((2, experts, toks), BF16),
            jax.ShapeDtypeStruct((experts * HALF, width), BF16),
            jax.ShapeDtypeStruct((experts * HALF, width), BF16),
        ],
        compiler_params=params(),
        name="refill",
    )(src, own, rows, router, routes)


def mixer_kernel(
    src, a0, a1, a2, a3, q_ref, f_ref, v_ref, gap_ref, inside_ref, query_ref, packed_ref, qa, fa, va, group
):
    step = pl.program_id(0)

    @pl.when(step == 0)
    def _():
        qa[...] = jnp.zeros_like(qa)
        fa[...] = jnp.zeros_like(fa)
        va[...] = jnp.zeros_like(va)

    toks = a0.shape[0]
    for k, part in enumerate((a0, a1, a2, a3)):
        group[pl.ds(pl.multiple_of(src[k] * toks, toks), toks), :] = part[...]
    a = group[...]
    qa[...] += mm(a, q_ref[...])
    fa[...] += mm(a, f_ref[...])
    va[...] += mm(a, v_ref[...])

    @pl.when(step == pl.num_programs(0) - 1)
    def _():
        rows = a.shape[0]
        causal = (
            lax.broadcasted_iota(jnp.int32, (rows, rows), 0)
            >= lax.broadcasted_iota(jnp.int32, (rows, rows), 1)
        )
        ones = jnp.where(causal[:toks, :toks], 1.0, 0.0).astype(BF16)
        shut = gap_ref[...] * jax.nn.sigmoid(-fa[...])
        fa[...] = jnp.log1p(-shut)
        cols = shut.shape[1]
        base = None
        for k in range(rows // toks):
            part = fa[k * toks : (k + 1) * toks, :]
            high = part.astype(BF16)
            rest = part - high.astype(F32)
            mid = rest.astype(BF16)
            low = (rest - mid.astype(F32)).astype(BF16)
            sums = mm(ones, jnp.concatenate([high, mid, low], axis=1))
            sums = sums[:, :cols] + sums[:, cols : 2 * cols] + sums[:, 2 * cols :]
            sums = sums if base is None else sums + base
            base = sums[toks - 1 :, :]
            fa[k * toks : (k + 1) * toks, :] = sums
        sums = fa[...]
        last = sums[rows - 1 :, :]
        query_ref[...] = qa[...] * jnp.exp(sums)
        keys = shut * jnp.exp(-sums)
        late = shut * jnp.exp(last - sums)
        half = rows // 2
        for h in range(packed_ref.shape[0]):
            at = slice(h * HEAD_DIM, (h + 1) * HEAD_DIM)
            q_high, q_low = halves(query_ref[:, at])
            k_high, k_low = halves(keys[:, at])
            v_high, v_low = halves(va[:, at])
            l_high, l_low = halves(late[:, at])
            left = jnp.concatenate([q_high, q_low, q_high], axis=1)
            right = jnp.concatenate([k_high, k_high, k_low], axis=1)
            values = jnp.concatenate([v_high, v_low], axis=1)
            for k in range(2):
                end = (k + 1) * half
                scores = mm(left[end - half : end], right[:end], ((1,), (1,)))
                s_high, s_low = halves(jnp.where(causal[end - half : end, :end], scores, 0.0))
                part = mm(s_high, values[:end])
                part = part[:, :HEAD_DIM] + part[:, HEAD_DIM:] + mm(s_low, v_high[:end])
                inside_ref[end - half : end, at] = part
            outer = mm(values, jnp.concatenate([l_high, l_low], axis=1), ((0,), (0,)))
            packed_ref[h, :HEAD_DIM, :] = (
                outer[:HEAD_DIM, :HEAD_DIM]
                + outer[:HEAD_DIM, HEAD_DIM:]
                + outer[HEAD_DIM:, :HEAD_DIM]
            )
            packed_ref[h, HEAD_DIM:, :] = jnp.broadcast_to(last[:, at], (8, HEAD_DIM))


def mixer(src, parts, wq, wf, wv, gap):
    toks, width = parts[0].shape
    rows = 4 * toks
    cols = wq.shape[1]
    heads = cols // HEAD_DIM
    kb = 512
    fixed = lambda i, s: (0, 0)
    weight = pl.BlockSpec((kb, cols), lambda i, s: (i, 0))
    return pl.pallas_call(
        mixer_kernel,
        grid_spec=pltpu.PrefetchScalarGridSpec(
            num_scalar_prefetch=1,
            grid=(width // kb,),
            in_specs=[pl.BlockSpec((toks, kb), lambda i, s: (0, i))] * 4
            + [weight, weight, weight, pl.BlockSpec((1, cols), fixed)],
            out_specs=[
                pl.BlockSpec((rows, cols), fixed),
                pl.BlockSpec((rows, cols), fixed),
                pl.BlockSpec((heads, HEAD_DIM + 8, HEAD_DIM), lambda i, s: (0, 0, 0)),
            ],
            scratch_shapes=[pltpu.VMEM((rows, cols), F32)] * 3 + [pltpu.VMEM((rows, kb), BF16)],
        ),
        out_shape=[
            jax.ShapeDtypeStruct((rows, cols), F32),
            jax.ShapeDtypeStruct((rows, cols), F32),
            jax.ShapeDtypeStruct((heads, HEAD_DIM + 8, HEAD_DIM), F32),
        ],
        compiler_params=params(),
        name="mixer",
    )(src, *parts, wq, wf, wv, gap)


def readout_kernel(inside_ref, query_ref, state_ref, gain_ref, out_ref):
    q_high, q_low = halves(query_ref[...])
    s_high, s_low = halves(state_ref[0])
    total = inside_ref[...] + mm(
        jnp.concatenate([q_high, q_low, q_high], axis=1),
        jnp.concatenate([s_high, s_high, s_low], axis=1),
        ((1,), (1,)),
    )
    out_ref[...] = normed(total, gain_ref[...]).astype(BF16)


def readout(inside, query, state, gain):
    rows, cols = inside.shape
    block = pl.BlockSpec((rows, HEAD_DIM), lambda h: (0, h))
    return pl.pallas_call(
        readout_kernel,
        grid=(cols // HEAD_DIM,),
        in_specs=[
            block,
            block,
            pl.BlockSpec((1, HEAD_DIM, HEAD_DIM), lambda h: (h, 0, 0)),
            pl.BlockSpec((1, HEAD_DIM), lambda h: (0, h)),
        ],
        out_specs=block,
        out_shape=jax.ShapeDtypeStruct((rows, cols), BF16),
        compiler_params=params(8),
        name="readout",
    )(inside, query, state, gain)


def pieces(packed):
    return packed[:, HEAD_DIM : HEAD_DIM + 1, :], packed[:, :HEAD_DIM, :]


def link(earlier, later):
    return earlier[0] + later[0], jnp.exp(later[0]) * earlier[1] + later[1]


def pack(part):
    heads = part[1].shape[0]
    return jnp.concatenate(
        [part[1], jnp.broadcast_to(part[0], (heads, 8, HEAD_DIM))], axis=1
    )


def masked(flag, part):
    return jax.tree.map(lambda a: jnp.where(flag, a, 0.0), part)


def both_cores(a):
    return lax.ppermute(a, "ep_2", [(0, 1), (1, 0)])


def along_rows(packed):
    core = lax.axis_index("ep_2")
    other = both_cores(packed)
    is_second = core == 1
    low = jnp.where(is_second, other, packed)
    high = jnp.where(is_second, packed, other)
    half = packed.shape[0] // 2
    mine = lambda a: lax.dynamic_slice_in_dim(a, core * half, half, 0)
    chip = link(pieces(mine(low)), pieces(mine(high)))
    count = lax.axis_size("ep_1")
    sent = pack(chip)
    came = [
        lax.ppermute(sent, "ep_1", [(i, (i + d) % count) for i in range(count)])
        for d in range(count - 1, 0, -1)
    ]
    return low, chip, came


def along_planes(chip, came):
    row = lax.axis_index("ep_1")
    before = after = None
    for k, part in enumerate(came):
        d = len(came) - k
        early = masked(row >= d, pieces(part))
        late = masked(row < d, pieces(part))
        before = early if before is None else link(before, early)
        after = late if after is None else link(after, late)
    plane = pack(link(link(before, chip), after))
    count = lax.axis_size("ep_0")
    planes = [
        lax.ppermute(plane, "ep_0", [(i, (i + d) % count) for i in range(count)])
        for d in range(count - 1, 0, -1)
    ]
    return before, planes


def arriving_state(low, before, planes):
    is_second = lax.axis_index("ep_2") == 1
    at = lax.axis_index("ep_0")
    total = None
    for k, part in enumerate(planes):
        part = masked(at >= len(planes) - k, pieces(part))
        total = part if total is None else link(total, part)
    state = link(total, before)[1]
    swapped = both_cores(state)
    entering = jnp.concatenate(
        [jnp.where(is_second, swapped, state), jnp.where(is_second, state, swapped)], axis=0
    )
    first_core = pieces(low)
    return jnp.where(is_second, jnp.exp(first_core[0]) * entering + first_core[1], entering)


def hidden_kernel(own_ref, near_ref, go_ref, uo_ref, gf_ref, uf_ref, out_ref, gate, up):
    step = pl.program_id(0)

    @pl.when(step == 0)
    def _():
        gate[...] = jnp.zeros_like(gate)
        up[...] = jnp.zeros_like(up)

    rows = jnp.concatenate([own_ref[...], near_ref[...]], axis=0)
    n = go_ref.shape[1]
    gate[:, :n] += mm(rows, go_ref[...])
    gate[:, n:] += mm(rows, gf_ref[...])
    up[:, :n] += mm(rows, uo_ref[...])
    up[:, n:] += mm(rows, uf_ref[...])

    @pl.when(step == pl.num_programs(0) - 1)
    def _():
        gated = jnp.minimum(gate[...], CLAMP_LIMIT)
        opened = jnp.clip(up[...], -CLAMP_LIMIT, CLAMP_LIMIT)
        out_ref[...] = (
            (opened + 1.0) * gated * jax.nn.sigmoid(SWISH_SLOPE * gated)
        ).astype(BF16)


def hidden_units(own, near, half, weights):
    count = own.shape[0]
    width, n = weights[0].shape
    kb = 1024
    weight = pl.BlockSpec((kb, n), lambda i: (i, 0))
    return pl.pallas_call(
        hidden_kernel,
        grid=(width // kb,),
        in_specs=[
            pl.BlockSpec((count, kb), lambda i: (0, i + half * (width // kb))),
            pl.BlockSpec((count, kb), lambda i: (0, i)),
            weight,
            weight,
            weight,
            weight,
        ],
        out_specs=pl.BlockSpec((2 * count, 2 * n), lambda i: (0, 0)),
        out_shape=jax.ShapeDtypeStruct((2 * count, 2 * n), BF16),
        scratch_shapes=[pltpu.VMEM((2 * count, 2 * n), F32)] * 2,
        compiler_params=params(),
        name="hidden",
    )(own, near, *weights)


def down_kernel(src, h_own, h_near, h_far, h_opp, down_ref, out_ref):
    k = pl.program_id(0)
    n = down_ref.shape[0] // 4
    rows = out_ref.shape[0]
    cols = down_ref.shape[1]
    unit = lambda s: down_ref[pl.ds(pl.multiple_of(s * n, n), n), :]
    for pair, refs in enumerate(((h_own, h_near), (h_far, h_opp))):

        @pl.when(k == pair)
        def _():
            both = []
            for j, ref in enumerate(refs):
                s = src[2 * pair + j]
                both.append(mm(ref[:, :n], unit(s)) + mm(ref[:, n:], unit(3 - s)))
            out_ref[:, :cols] = (both[0][:rows] + both[1][rows:]).astype(BF16)
            out_ref[:, cols:] = (both[0][rows:] + both[1][:rows]).astype(BF16)


def down_rows(src, parts, down):
    both, width = parts[0].shape
    cols = down.shape[1]
    whole = lambda k, s: (0, 0)
    return pl.pallas_call(
        down_kernel,
        grid_spec=pltpu.PrefetchScalarGridSpec(
            num_scalar_prefetch=1,
            grid=(2,),
            in_specs=[pl.BlockSpec((both, width), whole)] * 4 + [pl.BlockSpec(down.shape, whole)],
            out_specs=pl.BlockSpec((both // 2, 2 * cols), lambda k, s: (0, k)),
        ),
        out_shape=jax.ShapeDtypeStruct((both // 2, 4 * cols), BF16),
        compiler_params=params(20),
        name="down",
    )(src, *parts, down)


def places_kernel(src, routes_ref, logits_ref, out_ref):
    experts = logits_ref.shape[1]
    first, second, count, before = chosen(routes_ref[0], experts)
    logits = logits_ref[0].astype(F32)
    l0 = jnp.sum(jnp.where(first, logits, 0.0), axis=0, keepdims=True)
    l1 = jnp.sum(jnp.where(second, logits, 0.0), axis=0, keepdims=True)
    w0 = 1.0 / (1.0 + jnp.exp(l1 - l0))
    w1 = 1.0 / (1.0 + jnp.exp(l0 - l1))
    weight = jnp.where(first, w0, 0.0) + jnp.where(second, w1, 0.0)
    both = [slot_matrix(weight, before, count, half) for half in range(2)]
    place = jnp.concatenate(both, axis=0).T
    out_ref[0] = jnp.concatenate(halves(place), axis=0)


def places(src, routes, logits):
    experts, toks = logits.shape[1:]
    return pl.pallas_call(
        places_kernel,
        grid_spec=pltpu.PrefetchScalarGridSpec(
            num_scalar_prefetch=1,
            grid=(4,),
            in_specs=[
                pl.BlockSpec((1, 2, toks), lambda k, s: (s[k], 0, 0)),
                pl.BlockSpec((1, experts, toks), lambda k, s: (k, 0, 0)),
            ],
            out_specs=pl.BlockSpec((1, 2 * toks, experts * CAP), lambda k, s: (k, 0, 0)),
        ),
        out_shape=jax.ShapeDtypeStruct((4, 2 * toks, experts * CAP), BF16),
        compiler_params=params(8),
        name="places",
    )(src, routes, logits)


def combine_kernel(src, low_ref, high_ref, place_ref, out_ref):
    slots = low_ref.shape[0]
    total = mm(place_ref[0, :, :slots], low_ref[...]) + mm(place_ref[0, :, slots:], high_ref[...])
    toks = out_ref.shape[0]
    out_ref[...] = (total[:toks] + total[toks:]).astype(BF16)


def combined(src, low, high, place):
    slots = low.shape[0]
    cols = low.shape[1] // 4
    toks = place.shape[1] // 2
    res = pl.BlockSpec((slots, cols), lambda k, s: (0, k))
    return pl.pallas_call(
        combine_kernel,
        grid_spec=pltpu.PrefetchScalarGridSpec(
            num_scalar_prefetch=1,
            grid=(4,),
            in_specs=[
                res,
                res,
                pl.BlockSpec((1,) + place.shape[1:], lambda k, s: (k, 0, 0)),
            ],
            out_specs=pl.BlockSpec((toks, cols), lambda k, s: (s[k], 0)),
        ),
        out_shape=jax.ShapeDtypeStruct((4 * toks, cols), BF16),
        compiler_params=params(10),
        name="combine",
    )(src, low, high, place)


NEAR = [(i, i ^ 1) for i in range(4)]
FAR = [(i, 3 - i) for i in range(4)]
OPPOSITE = [(i, i ^ 2) for i in range(4)]


def to_near(a):
    return lax.ppermute(a, "tp", NEAR)


def to_far(a):
    return lax.ppermute(a, "tp", FAR)


def shared(a, direct=True):
    far = to_far(a)
    near = to_near(a)
    return a, near, far, (lax.ppermute(a, "tp", OPPOSITE) if direct else to_near(far))


def swap(a):
    experts = 32
    rows, cols = a.shape
    out = lax.all_to_all(
        a.reshape(experts, rows // experts, cols), EP, split_axis=0, concat_axis=0, tiled=True
    )
    return out.reshape(rows, cols)


def per_device(
    mix_input,
    moe_input,
    norm_mix,
    query_weight,
    forget_weight,
    value_weight,
    forget_gap,
    norm_out,
    norm_moe,
    router_weight,
    expert_gate,
    expert_up,
    expert_down,
    routes,
):
    toks = moe_input.shape[0]
    x = lax.axis_index("tp").astype(jnp.int32)
    src = jnp.stack([x, x ^ 1, 3 - x, x ^ 2])
    by_block = routes.reshape(4, toks, 2).transpose(0, 2, 1)
    router = router_weight.T

    rows_a = norm_rows(mix_input, norm_mix.reshape(1, -1))
    group_a = shared(rows_a, direct=False)
    rows_b, own = front(src, moe_input, norm_moe.reshape(1, -1), by_block, router_weight.shape[1])
    own_rows = swap(own)
    rows_near = to_near(rows_b)
    gate_far = to_far(expert_gate[0])
    up_far = to_far(expert_up[0])
    logits, low, high = refill(src, rows_b, rows_near, router, by_block)
    low_rows = swap(low)
    high_rows = swap(high)
    logits = jnp.concatenate([logits, to_far(logits)])
    place = places(src, by_block, logits)

    inside, query, packed = mixer(
        src, group_a, query_weight, forget_weight, value_weight, forget_gap.reshape(1, -1)
    )
    first_core, chip, came = along_rows(packed)

    low_rows, packed = lax.optimization_barrier((low_rows, packed))
    weights = (expert_gate[0], expert_up[0], gate_far, up_far)
    h_low = hidden_units(own_rows, low_rows, 0, weights)
    h_low = shared(h_low)
    high_rows, low_own = lax.optimization_barrier((high_rows, h_low[0]))
    h_high = hidden_units(own_rows, high_rows, 1, weights)
    h_high = shared(h_high)
    opp, high_own = lax.optimization_barrier((h_low[3], h_high[0]))
    down_low = down_rows(src, (low_own,) + h_low[1:3] + (opp,), expert_down[0])
    back_low = swap(down_low)
    came, _ = lax.optimization_barrier((came, down_low))
    before, planes = along_planes(chip, came)
    down_high = down_rows(src, (high_own,) + h_high[1:], expert_down[0])
    back_high = swap(down_high)
    planes, _ = lax.optimization_barrier((planes, down_high))

    state = arriving_state(first_core, before, planes)
    mixer_out = readout(inside, query, state, norm_out.reshape(1, -1))
    expert_out = combined(src, back_low, back_high, place)
    return (mixer_out, expert_out)


def solution(mesh):
    finer = Mesh(mesh.devices.reshape(4, 4, 2, mesh.shape["tp"]), ("ep_0", "ep_1", "ep_2", "tp"))
    placed = (
        P(EP_TP, None),
        P(EP_TP, None),
        P(),
        P(None, "tp"),
        P(None, "tp"),
        P(None, "tp"),
        P("tp"),
        P("tp"),
        P(),
        P(),
        P(EP, None, "tp"),
        P(EP, None, "tp"),
        P(EP, None, "tp"),
        P(EP, None),
    )

    return jax.shard_map(
        per_device,
        mesh=finer,
        in_specs=placed,
        out_specs=(P(EP, "tp"), P(EP, "tp")),
        check_vma=False,
    )
```

```python
import functools

import jax
import jax.numpy as jnp
from jax import lax
from jax.experimental import pallas as pl
from jax.experimental.pallas import tpu as pltpu
from jax.sharding import Mesh
from jax.sharding import PartitionSpec as P

HEAD_DIM = 128

CAP = 16
HALF = 8
EP = ("ep_0", "ep_1", "ep_2")
EP_TP = ("ep_0", "ep_1", "ep_2", "tp")

EPSILON = 1e-06
CLAMP_LIMIT = 7.0
SWISH_SLOPE = 1.702
F32 = jnp.float32
BF16 = jnp.bfloat16


def mm(a, b, contract=((1,), (0,))):
    return lax.dot_general(a, b, (contract, ((), ())), preferred_element_type=F32)


def halves(a):
    high = a.astype(BF16)
    return high, (a - high.astype(F32)).astype(BF16)


def params(mib=56, axes=("arbitrary",)):
    return pltpu.CompilerParams(vmem_limit_bytes=mib << 20, dimension_semantics=axes)


def normed(row_data, gain_vec):
    as_float = row_data.astype(F32)
    scale = lax.rsqrt(jnp.mean(as_float * as_float, axis=-1, keepdims=True) + EPSILON)
    return as_float * scale * gain_vec


def chosen(routes, experts):
    toks = routes.shape[1]
    ids = lax.broadcasted_iota(jnp.int32, (experts, toks), 0)
    first = routes[0:1, :] == ids
    second = routes[1:2, :] == ids
    count = jnp.where(first | second, 1.0, 0.0)
    earlier = (
        lax.broadcasted_iota(jnp.int32, (toks, toks), 0)
        < lax.broadcasted_iota(jnp.int32, (toks, toks), 1)
    )
    before = mm(count.astype(BF16), jnp.where(earlier, 1.0, 0.0).astype(BF16))
    return first, second, count, before


def slot_matrix(weight, before, count, half):
    experts, toks = weight.shape
    place = lax.broadcasted_iota(jnp.int32, (experts, HALF, toks), 1) + half * HALF
    here = (before[:, None, :] == place.astype(F32)) & (count[:, None, :] > 0.5)
    return jnp.where(here, weight[:, None, :], 0.0).reshape(experts * HALF, toks)


def fill(routes, rows, experts):
    _, _, count, before = chosen(routes, experts)
    pick = [slot_matrix(count, before, count, half) for half in range(2)]
    both = mm(jnp.concatenate(pick, axis=0).astype(BF16), rows).astype(BF16)
    return both[: experts * HALF], both[experts * HALF :]


def front_kernel(src, x_ref, gain_ref, routes_ref, rows_ref, buf_ref, *, group):
    step = pl.program_id(0)
    width = x_ref.shape[1]

    @pl.when(step == 0)
    def _():
        rows_ref[...] = normed(x_ref[...], gain_ref[...]).astype(BF16)

    low, high = fill(routes_ref[0] - step * group, rows_ref[...], group)
    buf_ref[:, :width] = low
    buf_ref[:, width:] = high


def refill_kernel(src, own_ref, rows_ref, router_ref, routes_ref, logits_ref, low_ref, high_ref, *, group):
    step = pl.program_id(0)

    @pl.when(step == 0)
    def _():
        for k, ref in enumerate((own_ref, rows_ref)):
            logits_ref[k] = mm(router_ref[...], ref[...], ((1,), (1,))).astype(BF16)

    low_ref[...], high_ref[...] = fill(routes_ref[0] - step * group, rows_ref[...], group)


def front(src, x, gain, routes, experts):
    toks, width = x.shape
    group = 16
    whole = lambda i, s: (0, 0)
    return pl.pallas_call(
        functools.partial(front_kernel, group=group),
        grid_spec=pltpu.PrefetchScalarGridSpec(
            num_scalar_prefetch=1,
            grid=(experts // group,),
            in_specs=[
                pl.BlockSpec((toks, width), whole),
                pl.BlockSpec((1, width), whole),
                pl.BlockSpec((1, 2, toks), lambda i, s: (s[0], 0, 0)),
            ],
            out_specs=[
                pl.BlockSpec((toks, width), whole),
                pl.BlockSpec((group * HALF, 2 * width), lambda i, s: (i, 0)),
            ],
        ),
        out_shape=[
            jax.ShapeDtypeStruct((toks, width), BF16),
            jax.ShapeDtypeStruct((experts * HALF, 2 * width), BF16),
        ],
        compiler_params=params(),
        name="front",
    )(src, x, gain, routes)


def refill(src, own, rows, router, routes):
    toks, width = rows.shape
    experts = router.shape[0]
    group = 16
    whole = lambda i, s: (0, 0)
    return pl.pallas_call(
        functools.partial(refill_kernel, group=group),
        grid_spec=pltpu.PrefetchScalarGridSpec(
            num_scalar_prefetch=1,
            grid=(experts // group,),
            in_specs=[
                pl.BlockSpec((toks, width), whole),
                pl.BlockSpec((toks, width), whole),
                pl.BlockSpec(router.shape, whole),
                pl.BlockSpec((1, 2, toks), lambda i, s: (s[1], 0, 0)),
            ],
            out_specs=[
                pl.BlockSpec((2, experts, toks), lambda i, s: (0, 0, 0)),
                pl.BlockSpec((group * HALF, width), lambda i, s: (i, 0)),
                pl.BlockSpec((group * HALF, width), lambda i, s: (i, 0)),
            ],
        ),
        out_shape=[
            jax.ShapeDtypeStruct((2, experts, toks), BF16),
            jax.ShapeDtypeStruct((experts * HALF, width), BF16),
            jax.ShapeDtypeStruct((experts * HALF, width), BF16),
        ],
        compiler_params=params(),
        name="refill",
    )(src, own, rows, router, routes)


def mixer_kernel(
    src, a0, a1, a2, a3, q_ref, f_ref, v_ref, gap_ref, inside_ref, query_ref, packed_ref, qa, fa, va, group
):
    step = pl.program_id(0)

    @pl.when(step == 0)
    def _():
        qa[...] = jnp.zeros_like(qa)
        fa[...] = jnp.zeros_like(fa)
        va[...] = jnp.zeros_like(va)

    toks = a0.shape[0]
    for k, part in enumerate((a0, a1, a2, a3)):
        group[pl.ds(pl.multiple_of(src[k] * toks, toks), toks), :] = part[...]
    a = group[...]
    qa[...] += mm(a, q_ref[...])
    fa[...] += mm(a, f_ref[...])
    va[...] += mm(a, v_ref[...])

    @pl.when(step == pl.num_programs(0) - 1)
    def _():
        rows = a.shape[0]
        causal = (
            lax.broadcasted_iota(jnp.int32, (rows, rows), 0)
            >= lax.broadcasted_iota(jnp.int32, (rows, rows), 1)
        )
        ones = jnp.where(causal[:toks, :toks], 1.0, 0.0).astype(BF16)
        shut = gap_ref[...] * jax.nn.sigmoid(-fa[...])
        fa[...] = jnp.log1p(-shut)
        cols = shut.shape[1]
        base = None
        for k in range(rows // toks):
            part = fa[k * toks : (k + 1) * toks, :]
            high = part.astype(BF16)
            rest = part - high.astype(F32)
            mid = rest.astype(BF16)
            low = (rest - mid.astype(F32)).astype(BF16)
            sums = mm(ones, jnp.concatenate([high, mid, low], axis=1))
            sums = sums[:, :cols] + sums[:, cols : 2 * cols] + sums[:, 2 * cols :]
            sums = sums if base is None else sums + base
            base = sums[toks - 1 :, :]
            fa[k * toks : (k + 1) * toks, :] = sums
        sums = fa[...]
        last = sums[rows - 1 :, :]
        query_ref[...] = qa[...] * jnp.exp(sums)
        keys = shut * jnp.exp(-sums)
        late = shut * jnp.exp(last - sums)
        half = rows // 2
        for h in range(packed_ref.shape[0]):
            at = slice(h * HEAD_DIM, (h + 1) * HEAD_DIM)
            q_high, q_low = halves(query_ref[:, at])
            k_high, k_low = halves(keys[:, at])
            v_high, v_low = halves(va[:, at])
            l_high, l_low = halves(late[:, at])
            left = jnp.concatenate([q_high, q_low, q_high], axis=1)
            right = jnp.concatenate([k_high, k_high, k_low], axis=1)
            values = jnp.concatenate([v_high, v_low], axis=1)
            for k in range(2):
                end = (k + 1) * half
                scores = mm(left[end - half : end], right[:end], ((1,), (1,)))
                s_high, s_low = halves(jnp.where(causal[end - half : end, :end], scores, 0.0))
                part = mm(s_high, values[:end])
                part = part[:, :HEAD_DIM] + part[:, HEAD_DIM:] + mm(s_low, v_high[:end])
                inside_ref[end - half : end, at] = part
            outer = mm(values, jnp.concatenate([l_high, l_low], axis=1), ((0,), (0,)))
            packed_ref[h, :HEAD_DIM, :] = (
                outer[:HEAD_DIM, :HEAD_DIM]
                + outer[:HEAD_DIM, HEAD_DIM:]
                + outer[HEAD_DIM:, :HEAD_DIM]
            )
            packed_ref[h, HEAD_DIM:, :] = jnp.broadcast_to(last[:, at], (8, HEAD_DIM))


def mixer(src, parts, wq, wf, wv, gap):
    toks, width = parts[0].shape
    rows = 4 * toks
    cols = wq.shape[1]
    heads = cols // HEAD_DIM
    kb = 1024
    fixed = lambda i, s: (0, 0)
    weight = pl.BlockSpec((kb, cols), lambda i, s: (i, 0))
    return pl.pallas_call(
        mixer_kernel,
        grid_spec=pltpu.PrefetchScalarGridSpec(
            num_scalar_prefetch=1,
            grid=(width // kb,),
            in_specs=[pl.BlockSpec((toks, kb), lambda i, s: (0, i))] * 4
            + [weight, weight, weight, pl.BlockSpec((1, cols), fixed)],
            out_specs=[
                pl.BlockSpec((rows, cols), fixed),
                pl.BlockSpec((rows, cols), fixed),
                pl.BlockSpec((heads, HEAD_DIM + 8, HEAD_DIM), lambda i, s: (0, 0, 0)),
            ],
            scratch_shapes=[pltpu.VMEM((rows, cols), F32)] * 3 + [pltpu.VMEM((rows, kb), BF16)],
        ),
        out_shape=[
            jax.ShapeDtypeStruct((rows, cols), F32),
            jax.ShapeDtypeStruct((rows, cols), F32),
            jax.ShapeDtypeStruct((heads, HEAD_DIM + 8, HEAD_DIM), F32),
        ],
        compiler_params=params(),
        name="mixer",
    )(src, *parts, wq, wf, wv, gap)


def readout_kernel(inside_ref, query_ref, state_ref, gain_ref, out_ref):
    q_high, q_low = halves(query_ref[...])
    s_high, s_low = halves(state_ref[0])
    total = inside_ref[...] + mm(
        jnp.concatenate([q_high, q_low, q_high], axis=1),
        jnp.concatenate([s_high, s_high, s_low], axis=1),
        ((1,), (1,)),
    )
    out_ref[...] = normed(total, gain_ref[...]).astype(BF16)


def readout(inside, query, state, gain):
    rows, cols = inside.shape
    block = pl.BlockSpec((rows, HEAD_DIM), lambda h: (0, h))
    return pl.pallas_call(
        readout_kernel,
        grid=(cols // HEAD_DIM,),
        in_specs=[
            block,
            block,
            pl.BlockSpec((1, HEAD_DIM, HEAD_DIM), lambda h: (h, 0, 0)),
            pl.BlockSpec((1, HEAD_DIM), lambda h: (0, h)),
        ],
        out_specs=block,
        out_shape=jax.ShapeDtypeStruct((rows, cols), BF16),
        compiler_params=params(8),
        name="readout",
    )(inside, query, state, gain)


def pieces(packed):
    return packed[:, HEAD_DIM : HEAD_DIM + 1, :], packed[:, :HEAD_DIM, :]


def link(earlier, later):
    return earlier[0] + later[0], jnp.exp(later[0]) * earlier[1] + later[1]


def pack(part):
    heads = part[1].shape[0]
    return jnp.concatenate(
        [part[1], jnp.broadcast_to(part[0], (heads, 8, HEAD_DIM))], axis=1
    )


def masked(flag, part):
    return jax.tree.map(lambda a: jnp.where(flag, a, 0.0), part)


def both_cores(a):
    return lax.ppermute(a, "ep_2", [(0, 1), (1, 0)])


def along_rows(packed):
    core = lax.axis_index("ep_2")
    other = both_cores(packed)
    is_second = core == 1
    low = jnp.where(is_second, other, packed)
    high = jnp.where(is_second, packed, other)
    half = packed.shape[0] // 2
    mine = lambda a: lax.dynamic_slice_in_dim(a, core * half, half, 0)
    chip = link(pieces(mine(low)), pieces(mine(high)))
    count = lax.axis_size("ep_1")
    sent = pack(chip)
    came = [
        lax.ppermute(sent, "ep_1", [(i, (i + d) % count) for i in range(count)])
        for d in range(count - 1, 0, -1)
    ]
    return low, chip, came


def along_planes(chip, came):
    row = lax.axis_index("ep_1")
    before = after = None
    for k, part in enumerate(came):
        d = len(came) - k
        early = masked(row >= d, pieces(part))
        late = masked(row < d, pieces(part))
        before = early if before is None else link(before, early)
        after = late if after is None else link(after, late)
    plane = pack(link(link(before, chip), after))
    count = lax.axis_size("ep_0")
    planes = [
        lax.ppermute(plane, "ep_0", [(i, (i + d) % count) for i in range(count)])
        for d in range(count - 1, 0, -1)
    ]
    return before, planes


def arriving_state(low, before, planes):
    is_second = lax.axis_index("ep_2") == 1
    at = lax.axis_index("ep_0")
    total = None
    for k, part in enumerate(planes):
        part = masked(at >= len(planes) - k, pieces(part))
        total = part if total is None else link(total, part)
    state = link(total, before)[1]
    swapped = both_cores(state)
    entering = jnp.concatenate(
        [jnp.where(is_second, swapped, state), jnp.where(is_second, state, swapped)], axis=0
    )
    first_core = pieces(low)
    return jnp.where(is_second, jnp.exp(first_core[0]) * entering + first_core[1], entering)


def hidden_kernel(own_ref, near_ref, go_ref, uo_ref, gf_ref, uf_ref, out_ref, gate, up):
    step = pl.program_id(0)

    @pl.when(step == 0)
    def _():
        gate[...] = jnp.zeros_like(gate)
        up[...] = jnp.zeros_like(up)

    rows = jnp.concatenate([own_ref[...], near_ref[...]], axis=0)
    n = go_ref.shape[1]
    gate[:, :n] += mm(rows, go_ref[...])
    gate[:, n:] += mm(rows, gf_ref[...])
    up[:, :n] += mm(rows, uo_ref[...])
    up[:, n:] += mm(rows, uf_ref[...])

    @pl.when(step == pl.num_programs(0) - 1)
    def _():
        gated = jnp.minimum(gate[...], CLAMP_LIMIT)
        opened = jnp.clip(up[...], -CLAMP_LIMIT, CLAMP_LIMIT)
        out_ref[...] = (
            (opened + 1.0) * gated * jax.nn.sigmoid(SWISH_SLOPE * gated)
        ).astype(BF16)


def hidden_units(own, near, half, weights):
    count = own.shape[0]
    width, n = weights[0].shape
    kb = 1024
    weight = pl.BlockSpec((kb, n), lambda i: (i, 0))
    return pl.pallas_call(
        hidden_kernel,
        grid=(width // kb,),
        in_specs=[
            pl.BlockSpec((count, kb), lambda i: (0, i + half * (width // kb))),
            pl.BlockSpec((count, kb), lambda i: (0, i)),
            weight,
            weight,
            weight,
            weight,
        ],
        out_specs=pl.BlockSpec((2 * count, 2 * n), lambda i: (0, 0)),
        out_shape=jax.ShapeDtypeStruct((2 * count, 2 * n), BF16),
        scratch_shapes=[pltpu.VMEM((2 * count, 2 * n), F32)] * 2,
        compiler_params=params(),
        name="hidden",
    )(own, near, *weights)


def down_kernel(src, h_own, h_near, h_far, h_opp, down_ref, out_ref):
    k = pl.program_id(0)
    n = down_ref.shape[0] // 4
    rows = out_ref.shape[0]
    cols = down_ref.shape[1]
    unit = lambda s: down_ref[pl.ds(pl.multiple_of(s * n, n), n), :]
    for pair, refs in enumerate(((h_own, h_near), (h_far, h_opp))):

        @pl.when(k == pair)
        def _():
            both = []
            for j, ref in enumerate(refs):
                s = src[2 * pair + j]
                both.append(mm(ref[:, :n], unit(s)) + mm(ref[:, n:], unit(3 - s)))
            out_ref[:, :cols] = (both[0][:rows] + both[1][rows:]).astype(BF16)
            out_ref[:, cols:] = (both[0][rows:] + both[1][:rows]).astype(BF16)


def down_rows(src, parts, down):
    both, width = parts[0].shape
    cols = down.shape[1]
    whole = lambda k, s: (0, 0)
    return pl.pallas_call(
        down_kernel,
        grid_spec=pltpu.PrefetchScalarGridSpec(
            num_scalar_prefetch=1,
            grid=(2,),
            in_specs=[pl.BlockSpec((both, width), whole)] * 4 + [pl.BlockSpec(down.shape, whole)],
            out_specs=pl.BlockSpec((both // 2, 2 * cols), lambda k, s: (0, k)),
        ),
        out_shape=jax.ShapeDtypeStruct((both // 2, 4 * cols), BF16),
        compiler_params=params(20),
        name="down",
    )(src, *parts, down)


def places_kernel(src, routes_ref, logits_ref, out_ref):
    experts = logits_ref.shape[1]
    first, second, count, before = chosen(routes_ref[0], experts)
    logits = logits_ref[0].astype(F32)
    l0 = jnp.sum(jnp.where(first, logits, 0.0), axis=0, keepdims=True)
    l1 = jnp.sum(jnp.where(second, logits, 0.0), axis=0, keepdims=True)
    w0 = 1.0 / (1.0 + jnp.exp(l1 - l0))
    w1 = 1.0 / (1.0 + jnp.exp(l0 - l1))
    weight = jnp.where(first, w0, 0.0) + jnp.where(second, w1, 0.0)
    both = [slot_matrix(weight, before, count, half) for half in range(2)]
    place = jnp.concatenate(both, axis=0).T
    out_ref[0] = jnp.concatenate(halves(place), axis=0)


def places(src, routes, logits):
    experts, toks = logits.shape[1:]
    return pl.pallas_call(
        places_kernel,
        grid_spec=pltpu.PrefetchScalarGridSpec(
            num_scalar_prefetch=1,
            grid=(4,),
            in_specs=[
                pl.BlockSpec((1, 2, toks), lambda k, s: (s[k], 0, 0)),
                pl.BlockSpec((1, experts, toks), lambda k, s: (k, 0, 0)),
            ],
            out_specs=pl.BlockSpec((1, 2 * toks, experts * CAP), lambda k, s: (k, 0, 0)),
        ),
        out_shape=jax.ShapeDtypeStruct((4, 2 * toks, experts * CAP), BF16),
        compiler_params=params(8),
        name="places",
    )(src, routes, logits)


def combine_kernel(src, low_ref, high_ref, place_ref, out_ref):
    slots = low_ref.shape[0]
    total = mm(place_ref[0, :, :slots], low_ref[...]) + mm(place_ref[0, :, slots:], high_ref[...])
    toks = out_ref.shape[0]
    out_ref[...] = (total[:toks] + total[toks:]).astype(BF16)


def combined(src, low, high, place):
    slots = low.shape[0]
    cols = low.shape[1] // 4
    toks = place.shape[1] // 2
    res = pl.BlockSpec((slots, cols), lambda k, s: (0, k))
    return pl.pallas_call(
        combine_kernel,
        grid_spec=pltpu.PrefetchScalarGridSpec(
            num_scalar_prefetch=1,
            grid=(4,),
            in_specs=[
                res,
                res,
                pl.BlockSpec((1,) + place.shape[1:], lambda k, s: (k, 0, 0)),
            ],
            out_specs=pl.BlockSpec((toks, cols), lambda k, s: (s[k], 0)),
        ),
        out_shape=jax.ShapeDtypeStruct((4 * toks, cols), BF16),
        compiler_params=params(10),
        name="combine",
    )(src, low, high, place)


NEAR = [(i, i ^ 1) for i in range(4)]
FAR = [(i, 3 - i) for i in range(4)]
OPPOSITE = [(i, i ^ 2) for i in range(4)]


def to_near(a):
    return lax.ppermute(a, "tp", NEAR)


def to_far(a):
    return lax.ppermute(a, "tp", FAR)


def shared(a, direct=True):
    far = to_far(a)
    near = to_near(a)
    return a, near, far, (lax.ppermute(a, "tp", OPPOSITE) if direct else to_near(far))


def swap(a):
    experts = 32
    rows, cols = a.shape
    out = lax.all_to_all(
        a.reshape(experts, rows // experts, cols), EP, split_axis=0, concat_axis=0, tiled=True
    )
    return out.reshape(rows, cols)


def per_device(
    mix_input,
    moe_input,
    norm_mix,
    query_weight,
    forget_weight,
    value_weight,
    forget_gap,
    norm_out,
    norm_moe,
    router_weight,
    expert_gate,
    expert_up,
    expert_down,
    routes,
):
    toks = moe_input.shape[0]
    x = lax.axis_index("tp").astype(jnp.int32)
    src = jnp.stack([x, x ^ 1, 3 - x, x ^ 2])
    by_block = routes.reshape(4, toks, 2).transpose(0, 2, 1)
    router = router_weight.T

    rows_a = normed(mix_input, norm_mix).astype(BF16)
    group_a = shared(rows_a, direct=False)
    rows_b, own = front(src, moe_input, norm_moe.reshape(1, -1), by_block, router_weight.shape[1])
    own_rows = swap(own)
    rows_near = to_near(rows_b)
    gate_far = to_far(expert_gate[0])
    up_far = to_far(expert_up[0])
    logits, low, high = refill(src, rows_b, rows_near, router, by_block)
    low_rows = swap(low)
    high_rows = swap(high)
    logits = jnp.concatenate([logits, to_far(logits)])
    place = places(src, by_block, logits)

    inside, query, packed = mixer(
        src, group_a, query_weight, forget_weight, value_weight, forget_gap.reshape(1, -1)
    )
    first_core, chip, came = along_rows(packed)

    low_rows, packed = lax.optimization_barrier((low_rows, packed))
    weights = (expert_gate[0], expert_up[0], gate_far, up_far)
    h_low = hidden_units(own_rows, low_rows, 0, weights)
    h_low = shared(h_low)
    high_rows, low_own = lax.optimization_barrier((high_rows, h_low[0]))
    h_high = hidden_units(own_rows, high_rows, 1, weights)
    h_high = shared(h_high)
    opp, high_own = lax.optimization_barrier((h_low[3], h_high[0]))
    down_low = down_rows(src, (low_own,) + h_low[1:3] + (opp,), expert_down[0])
    back_low = swap(down_low)
    came, _ = lax.optimization_barrier((came, down_low))
    before, planes = along_planes(chip, came)
    down_high = down_rows(src, (high_own,) + h_high[1:], expert_down[0])
    back_high = swap(down_high)
    planes, _ = lax.optimization_barrier((planes, down_high))

    state = arriving_state(first_core, before, planes)
    mixer_out = readout(inside, query, state, norm_out.reshape(1, -1))
    expert_out = combined(src, back_low, back_high, place)
    return (mixer_out, expert_out)


def solution(mesh):
    finer = Mesh(mesh.devices.reshape(4, 4, 2, mesh.shape["tp"]), ("ep_0", "ep_1", "ep_2", "tp"))
    placed = (
        P(EP_TP, None),
        P(EP_TP, None),
        P(),
        P(None, "tp"),
        P(None, "tp"),
        P(None, "tp"),
        P("tp"),
        P("tp"),
        P(),
        P(),
        P(EP, None, "tp"),
        P(EP, None, "tp"),
        P(EP, None, "tp"),
        P(EP, None),
    )

    return jax.shard_map(
        per_device,
        mesh=finer,
        in_specs=placed,
        out_specs=(P(EP, "tp"), P(EP, "tp")),
        check_vma=False,
    )
```
